32 devices in a mesh: fs: 16 (over z, y, x), tp: 2 (over core).
Axes of the slice: x: 2, y: 2, z: 4, core: 2. Of those that a mesh axis runs over, the one named last changes fastest.
Arguments:
- tokens: bfloat16 [8192, 2048], P('fs', 'tp'), may hold values from -6 to 6
- norm_gain: bfloat16 [2048], P('tp'), may hold values from 0.099609375 to 1.8984375
- proj_u: bfloat16 [2048, 2048], P('fs', 'tp'), may hold values from -0.125 to 0.125
- proj_v: bfloat16 [2048, 2048], P('fs', 'tp'), may hold values from -0.125 to 0.125
- layer_gain: bfloat16 [2048], P('tp'), may hold values from 0.099609375 to 1.8984375
- layer_shift: bfloat16 [2048], P('tp'), may hold values from -3 to 3
- mix_weight: bfloat16 [16, 128, 128], P('tp'), may hold values from -0.5 to 0.5
- mix_bias: bfloat16 [16, 128], P('tp'), may hold values from 0.099609375 to 1.8984375
- proj_out: bfloat16 [2048, 2048], P('tp', 'fs'), may hold values from -0.1875 to 0.1875
- ffn_gain: bfloat16 [2048], P('tp'), may hold values from 0.099609375 to 1.8984375
- ffn_gate: bfloat16 [2048, 4096], P('fs', 'tp'), may hold values from -0.125 to 0.125
- ffn_value: bfloat16 [2048, 4096], P('fs', 'tp'), may hold values from -0.125 to 0.125
- conv_gate: bfloat16 [3, 4096], P(None, 'tp'), may hold values from -3 to 3
- conv_value: bfloat16 [3, 4096], P(None, 'tp'), may hold values from -3 to 3
- proj_down: bfloat16 [4096, 2048], P('tp', 'fs'), may hold values from -0.125 to 0.125
Outputs:
- result: bfloat16 [8192, 2048], P('fs', 'tp')
The draws below stay inside these ranges and needn't reach their ends.
All inputs are finite; a program needn't handle non-finite values.
Results may differ from the reference program's by a relative error of at most 0.017.
Values may be sent and summed in bfloat16 or wider, within the bound.
A program may use at most 64 MiB of HBM per device.

```python
import jax
import jax.numpy as jnp
from jax import lax

D = 2048
GROUPS = 16
GROUP_DIM = 128
DA = 2048
FF = 4096
BLOCK = 128
SEGMENT = 64
KERNEL = 3
SEQ_LEN = 256
TOK_DEV = 512
TOKENS = 8192
N_FS = 16
N_TP = 2


def draw_tokens(key, part):
    column = jnp.arange(D).astype(jnp.float32)
    col_scale = 0.6 * 3.0 ** (column / D)
    values = jax.random.normal(key, (TOKENS, D), jnp.float32) * col_scale
    return jnp.clip(values, -6.0, 6.0).astype(jnp.bfloat16)


def strengthened(drawn, stream_key, source, target, blocks, factor):
    owner, partner = [(jnp.arange(drawn.shape[dim]) // (drawn.shape[dim] // blocks)).reshape([-1 if axis == dim else 1 for axis in range(drawn.ndim)]) for dim in (source, target)]
    chosen = jax.random.permutation(stream_key, blocks)[partner]
    strong = (owner == chosen) | (owner == (partner + blocks // 2) % blocks)
    return jnp.where(strong, factor * drawn, drawn)


def levels(own_key, shape, shards, least, high):
    factor_of, own = 1.0, jax.random.fold_in(own_key, 6)
    for position, blocks in shards:
        draws = jnp.exp(jax.random.uniform(jax.random.fold_in(own, position), (blocks,), jnp.float32, least / len(shards), high / len(shards)))
        factor_of = factor_of * jnp.repeat(draws, shape[position] // blocks).reshape([-1 if axis == position else 1 for axis in range(len(shape))])
    return factor_of


def bell_draw(key, extent, scale, most, cuts=(), dtype=jnp.bfloat16):
    loudness = levels(key, extent, cuts, -0.22, 0.18) if cuts else 1.0
    values = jax.random.normal(key, extent, jnp.float32) * scale * loudness
    return jnp.minimum(jnp.maximum(values, -most), most).astype(dtype)


def bell_draw_with(own_key, dims, scale, most, cuts, heavy, dtype=jnp.bfloat16):
    array = scale * jax.random.normal(own_key, dims, jnp.float32)
    if cuts:
        array = array * levels(own_key, dims, cuts, -0.22, 0.18)
    return jnp.clip(strengthened(array, jax.random.fold_in(own_key, 3), *heavy), -most, most).astype(dtype)


def setup_inputs(seed: int = 0) -> dict:
    keys = jax.random.split(jax.random.key(seed), 16)
    tokens = draw_tokens(jax.random.fold_in(keys[15], 71), 0)
    norm_gain = jnp.clip(1.0 + 0.18 * jax.random.normal(keys[1], (D,), jnp.float32), 0.099609375, 1.8984375).astype(jnp.bfloat16)
    proj_u = bell_draw(keys[2], (D, DA), D ** -0.5, 0.125, ((0, 16), (1, 2)))
    proj_v = bell_draw(keys[3], (D, DA), D ** -0.5, 0.125, ((0, 16), (1, 2)))
    layer_gain = jnp.clip(1.0 + 0.18 * jax.random.normal(keys[4], (DA,), jnp.float32), 0.099609375, 1.8984375).astype(jnp.bfloat16)
    layer_shift = bell_draw(keys[5], (DA,), 0.5, 3.0, ((0, 2),))
    mix_weight = bell_draw(keys[6], (GROUPS, BLOCK, BLOCK), BLOCK ** -0.5, 0.5, ((0, 2),))
    mix_bias = jnp.clip(1.0 + 0.18 * jax.random.normal(keys[7], (GROUPS, BLOCK), jnp.float32), 0.099609375, 1.8984375).astype(jnp.bfloat16)
    proj_out = bell_draw_with(keys[8], (DA, D), DA ** -0.5, 0.1875, ((0, 2), (1, 16)), (0, 1, 16, 2.0))
    ffn_gain = jnp.clip(1.0 + 0.18 * jax.random.normal(keys[9], (D,), jnp.float32), 0.099609375, 1.8984375).astype(jnp.bfloat16)
    ffn_gate = bell_draw(keys[10], (D, FF), D ** -0.5, 0.125, ((0, 16), (1, 2)))
    ffn_value = bell_draw(keys[11], (D, FF), D ** -0.5, 0.125, ((0, 16), (1, 2)))
    conv_gate = bell_draw(keys[12], (KERNEL, FF), 0.6, 3.0, ((1, 2),))
    conv_value = bell_draw(keys[13], (KERNEL, FF), 0.6, 3.0, ((1, 2),))
    proj_down = bell_draw_with(keys[14], (FF, D), FF ** -0.5, 0.125, ((0, 2), (1, 16)), (0, 1, 16, 2.0))
    return dict(tokens=tokens, norm_gain=norm_gain, proj_u=proj_u, proj_v=proj_v, layer_gain=layer_gain, layer_shift=layer_shift, mix_weight=mix_weight, mix_bias=mix_bias, proj_out=proj_out, ffn_gain=ffn_gain, ffn_gate=ffn_gate, ffn_value=ffn_value, conv_gate=conv_gate, conv_value=conv_value, proj_down=proj_down)


EPS = 1e-06

def matmul(operand, matrix):
    return jnp.dot(operand, matrix, preferred_element_type=jnp.float32)

def share_sum(operand, matrix, share_width):
    summed = jnp.zeros((operand.shape[0], matrix.shape[1]), jnp.float32)
    for index in range(N_TP):
        lower = index * share_width
        product = matmul(operand[:, lower:lower + share_width], matrix[lower:lower + share_width, :])
        rounded = lax.optimization_barrier(product.astype(jnp.bfloat16))
        summed = summed + rounded.astype(jnp.float32)
    return summed

def rms_rows(values_in, gain_row):
    values = values_in.astype(jnp.float32)
    scale_row = lax.rsqrt(lax.optimization_barrier(jnp.mean(values * values, axis=1, keepdims=True)) + EPS)
    return (values * scale_row * gain_row.astype(jnp.float32)).astype(jnp.bfloat16)

def causal_taps(values, weights):
    seq_count = values.shape[0] // SEQ_LEN
    shaped = values.reshape(seq_count, SEQ_LEN, values.shape[1])
    padded = jnp.pad(shaped, ((0, 0), (KERNEL - 1, 0), (0, 0)))
    summed = jnp.zeros(shaped.shape, jnp.float32)
    for tap_index in range(KERNEL):
        summed = summed + padded[:, tap_index:tap_index + SEQ_LEN].astype(jnp.float32) * weights[tap_index].astype(jnp.float32)
    return summed.reshape(values.shape[0], values.shape[1])

def reference(tokens, norm_gain, proj_u, proj_v, layer_gain, layer_shift, mix_weight, mix_bias, proj_out, ffn_gain, ffn_gate, ffn_value, conv_gate, conv_value, proj_down):
    segment = jnp.arange(BLOCK) // SEGMENT
    visible = segment[None, :] <= segment[:, None]
    masked = jnp.where(visible[None], mix_weight, jnp.zeros_like(mix_weight)).astype(jnp.float32)

    def one_block(token_rows):
        row_count = token_rows.shape[0]
        normed = rms_rows(token_rows, norm_gain)
        act_u = jax.nn.gelu(matmul(normed, proj_u), approximate=False)
        act_v = jax.nn.gelu(matmul(normed, proj_v), approximate=False)
        center = lax.optimization_barrier(jnp.mean(act_v, axis=1, keepdims=True))
        spread = lax.optimization_barrier(jnp.mean(act_v * act_v, axis=1, keepdims=True)) - center * center
        mixed_in = ((act_v - center) * lax.rsqrt(spread + EPS) * layer_gain.astype(jnp.float32) + layer_shift.astype(jnp.float32)).astype(jnp.bfloat16)
        blocks = mixed_in.reshape(row_count // BLOCK, BLOCK, GROUPS, GROUP_DIM).astype(jnp.float32)
        spatial = jnp.einsum('gij,njgc->nigc', masked, blocks) + mix_bias.astype(jnp.float32).T[None, :, :, None]
        gated = (act_u * spatial.reshape(row_count, DA)).astype(jnp.bfloat16)
        stream = (token_rows.astype(jnp.float32) + share_sum(gated, proj_out, DA // N_TP)).astype(jnp.bfloat16)
        normed_two = rms_rows(stream, ffn_gain)
        up_gate = matmul(normed_two, ffn_gate).astype(jnp.bfloat16)
        up_value = matmul(normed_two, ffn_value).astype(jnp.bfloat16)
        conv_g = causal_taps(up_gate, conv_gate)
        conv_v = causal_taps(up_value, conv_value)
        hidden = (jax.nn.silu(conv_g) * conv_v).astype(jnp.bfloat16)
        return (stream.astype(jnp.float32) + share_sum(hidden, proj_down, FF // N_TP)).astype(jnp.bfloat16)
    grouped = tokens.reshape(N_FS, TOK_DEV, D)
    return lax.map(one_block, grouped).reshape(TOKENS, D)
```

```python
import functools

import jax
import jax.numpy as jnp
from jax import lax
from jax.experimental import pallas as pl
from jax.experimental.pallas import tpu as pltpu
from jax.sharding import PartitionSpec as P

MESH = pl.DeviceIdType.MESH
LANES = 128

GROUP_DIM = 128
BLOCK = 128
SEGMENT = 64
KERNEL = 3
SEQ_LEN = 256


EPS = 1e-06


def matmul(operand, matrix):
    return jnp.dot(operand, matrix, preferred_element_type=jnp.float32)


def local_rms(values_in, gain_row):
    values = values_in.astype(jnp.float32)
    scale_row = lax.rsqrt(jnp.mean(values * values, axis=1, keepdims=True) + EPS)
    return (values * scale_row * gain_row.astype(jnp.float32)).astype(jnp.bfloat16)


def causal_taps(values, weights):
    seq_count = values.shape[0] // SEQ_LEN
    shaped = values.reshape(seq_count, SEQ_LEN, values.shape[1])
    padded = jnp.pad(shaped, ((0, 0), (KERNEL - 1, 0), (0, 0)))
    summed = jnp.zeros(shaped.shape, jnp.float32)
    for tap_index in range(KERNEL):
        summed = summed + padded[:, tap_index : tap_index + SEQ_LEN].astype(jnp.float32) * weights[
            tap_index
        ].astype(jnp.float32)
    return summed.reshape(values.shape[0], values.shape[1])


def on_device(
    tokens,
    norm_gain,
    proj_u,
    proj_v,
    layer_gain,
    layer_shift,
    mix_weight,
    mix_bias,
    proj_out,
    ffn_gain,
    ffn_gate,
    ffn_value,
    conv_gate,
    conv_value,
    proj_down,
):
    own_width = tokens.shape[1]
    whole_tokens, whole_gain, whole_ffn_gain = (
        lax.all_gather(tokens, "tp", axis=1, tiled=True),
        lax.all_gather(norm_gain, "tp", axis=0, tiled=True),
        lax.all_gather(ffn_gain, "tp", axis=0, tiled=True),
    )
    normed = local_rms(whole_tokens, whole_gain)
    row_count = normed.shape[0]
    whole_u, whole_v = (
        lax.all_gather(proj_u, "fs", axis=0, tiled=True),
        lax.all_gather(proj_v, "fs", axis=0, tiled=True),
    )
    pre_u = matmul(normed, whole_u)
    pre_v = matmul(normed, whole_v)
    act_u = jax.nn.gelu(pre_u, approximate=False)
    act_v = jax.nn.gelu(pre_v, approximate=False)
    full_width = act_v.shape[1] * lax.axis_size("tp")
    total_sum, second = lax.psum((jnp.sum(act_v, axis=1), jnp.sum(act_v * act_v, axis=1)), "tp")
    center = total_sum / full_width
    spread = second / full_width - center * center
    mixed_in = (
        (act_v - center[:, None])
        * lax.rsqrt(spread + EPS)[:, None]
        * layer_gain.astype(jnp.float32)
        + layer_shift.astype(jnp.float32)
    ).astype(jnp.bfloat16)
    groups = mixed_in.shape[1] // GROUP_DIM
    blocks = mixed_in.reshape(row_count // BLOCK, BLOCK, groups, GROUP_DIM)
    segment = jnp.arange(BLOCK) // SEGMENT
    visible = segment[None, :] <= segment[:, None]
    masked = jnp.where(visible[None], mix_weight, jnp.zeros_like(mix_weight))
    spatial = (
        jnp.einsum("gij,njgc->nigc", masked, blocks, preferred_element_type=jnp.float32)
        + mix_bias.astype(jnp.float32).T[None, :, :, None]
    )
    gated_rows = (act_u * spatial.reshape(row_count, mixed_in.shape[1])).astype(jnp.bfloat16)
    whole_out = lax.all_gather(proj_out, "fs", axis=1, tiled=True)
    partial_value = matmul(gated_rows, whole_out)
    summed = lax.psum(partial_value.astype(jnp.bfloat16), "tp").astype(jnp.float32)
    stream_rows = (whole_tokens.astype(jnp.float32) + summed).astype(jnp.bfloat16)
    normed_two = local_rms(stream_rows, whole_ffn_gain)
    stream = lax.dynamic_slice_in_dim(stream_rows, lax.axis_index("tp") * own_width, own_width, 1)
    whole_gate, whole_value = (
        lax.all_gather(ffn_gate, "fs", axis=0, tiled=True),
        lax.all_gather(ffn_value, "fs", axis=0, tiled=True),
    )
    pre_gate = matmul(normed_two, whole_gate)
    pre_value = matmul(normed_two, whole_value)
    conv_g = causal_taps(pre_gate.astype(jnp.bfloat16), conv_gate)
    conv_v = causal_taps(pre_value.astype(jnp.bfloat16), conv_value)
    hidden = (jax.nn.silu(conv_g) * conv_v).astype(jnp.bfloat16)
    whole_down = lax.all_gather(proj_down, "fs", axis=1, tiled=True)
    partial_two = matmul(hidden, whole_down)
    return (
        stream.astype(jnp.float32)
        + lax.psum_scatter(
            partial_two.astype(jnp.bfloat16), "tp", scatter_dimension=1, tiled=True
        ).astype(jnp.float32)
    ).astype(jnp.bfloat16)


V, U, O, G, E, W = range(6)
BY_ROWS = (V, U, G, E)
VMEM_BYTES = 67043328


def gelu(values):
    return 0.5 * values * (1.0 + lax.erf(values * (0.5**0.5)))


def aligned(index, size):
    return pl.multiple_of(index * size, size)


def layer_kernel(
    fs_size,
    tokens,
    vectors,
    mix_weight,
    mix_bias,
    conv_gate,
    conv_value,
    proj_u,
    proj_v,
    proj_out,
    ffn_gate,
    ffn_value,
    proj_down,
    result,
    whole_v,
    whole_u,
    whole_out,
    whole_gate,
    whole_value,
    whole_down,
    rows_in,
    normed,
    gains,
    act_v,
    act_u,
    stat_cols,
    stat_own,
    stat_chip,
    stat_near,
    stat_far,
    masked,
    bias_cols,
    gated,
    partial,
    from_core,
    chip_sum,
    from_side,
    stream,
    pre_gate,
    hidden,
    total,
    near_down,
    far_down,
    local_sem,
    pool_send,
    pool_recv,
    ring_send,
    ring_recv,
    token_send,
    token_recv,
    stat_send,
    stat_recv,
    core_send,
    core_recv,
    side_send,
    side_recv,
    half_send,
    half_recv,
    near_send,
    near_recv,
    far_send,
    far_recv,
):
    pairs = fs_size // 2
    depth = pairs // 2
    last = 2 * (depth - 1)
    steps = last + 1
    index, core = lax.axis_index("fs"), lax.axis_index("tp")
    side, pair = index % 2, index // 2
    level, column = pair // 2, pair % 2
    spot = level * (1 - column) + (pairs - 1 - level) * column

    def pair_at(place):
        far = place // depth
        return 2 * (place * (1 - far) + (pairs - 1 - place) * far) + far

    def turned(shift):
        return pair_at((spot + shift + pairs) % pairs)

    right = (2 * turned(1) + side, core)
    left = (2 * turned(-1) + side, core)
    across = (2 * pair + 1 - side, core)
    partner = (index, 1 - core)

    own_rows, own_width = tokens.shape
    row_count, full = rows_in.shape
    tile = SEQ_LEN
    tiles = row_count // tile
    half_tiles = tiles // 2
    quarter = whole_v.shape[1]
    units = whole_gate.shape[1]
    groups = quarter // GROUP_DIM
    spread_width = 2 * 2 * quarter
    block_width = whole_out.shape[2]
    half_blocks = pairs // 2

    sources = (proj_v, proj_u, proj_out, ffn_gate, ffn_value, proj_down)
    wholes = (whole_v, whole_u, whole_out, whole_gate, whole_value, whole_down)

    def chunk(which, owner, part):
        whole = wholes[which]
        if which in BY_ROWS:
            depth_rows = sources[which].shape[0]
            return whole.at[pl.ds(aligned(2 * owner + part, depth_rows), depth_rows), :]
        width = sources[which].shape[1]
        return whole.at[owner, :, pl.ds(aligned(part, width), width)]

    def shard(which, part):
        source = sources[which]
        if which in BY_ROWS:
            width = source.shape[1] // 2
            return source.at[:, pl.ds(aligned(part, width), width)]
        height = source.shape[0] // 2
        return source.at[pl.ds(aligned(part, height), height), :]

    def remote(source, target, send, recv, device):
        return pltpu.make_async_remote_copy(
            src_ref=source,
            dst_ref=target,
            send_sem=send,
            recv_sem=recv,
            device_id=device,
            device_id_type=MESH,
        )

    def own_copy(which):
        return pltpu.make_async_copy(
            shard(which, side), chunk(which, pair, side), local_sem.at[which]
        )

    def pool_copy(which):
        return remote(
            shard(which, 1 - side),
            chunk(which, pair, side),
            pool_send.at[which],
            pool_recv.at[which],
            across,
        )

    def pool_arrived(which):
        here = chunk(which, pair, 1 - side)
        remote(here, here, pool_send.at[which], pool_recv.at[which], across).wait_recv()

    def relative(which_part):
        return side + which_part * (1 - 2 * side)

    def ring_copy(which, step, way, shift):
        part = step % 2 if way == 0 else step % 2 + step // last
        sign = 1 - 2 * way
        piece = chunk(which, turned(-sign * shift), relative(part))
        slot = (which * 2 + way) * steps + step
        return remote(
            piece, piece, ring_send.at[slot], ring_recv.at[slot], right if way == 0 else left
        )

    def ring_arrived(which, step, way):
        ring_copy(which, step, way, step // 2 + 1).wait_recv()

    def pump(which, step):
        if isinstance(step, int) and step == 0:
            own_copy(which).wait()
        elif isinstance(step, int) and step == 1:
            pool_arrived(which)
        else:
            ring_arrived(which, step - 2, 0)
            ring_arrived(which, step - 2 + step // last, 1)
        ring_copy(which, step, 0, step // 2).start()
        ring_copy(which, step, 1, step // 2).start()

    def drain(which):
        for step, way in ((last - 1, 0), (last, 0), (last - 2, 1), (last, 1)):
            ring_arrived(which, step, way)

    def token_region(which_side, which_core):
        return rows_in.at[
            pl.ds(aligned(which_side, own_rows), own_rows),
            pl.ds(aligned(which_core, own_width), own_width),
        ]

    def gain_region(which_core):
        return gains.at[:, pl.ds(aligned(which_core, own_width), own_width)]

    def token_copy(which, region, device):
        return remote(region, region, token_send.at[which], token_recv.at[which], device)

    def rows_of(place, height=tile):
        return pl.ds(aligned(place, height), height)

    barrier = pltpu.get_barrier_semaphore()
    for device in (right, left, across, partner):
        pl.semaphore_signal(barrier, inc=1, device_id=device, device_id_type=MESH)
    for which in (V, U):
        own_copy(which).start()
    tokens_in = pltpu.make_async_copy(tokens, token_region(side, core), local_sem.at[6])
    tokens_in.start()
    vectors_in = pltpu.make_async_copy(vectors, gain_region(core), local_sem.at[7])
    vectors_in.start()
    for which in (O, G, E, W):
        own_copy(which).start()
    pl.semaphore_wait(barrier, 4)

    for which in (V, U):
        pool_copy(which).start()
    for which in (V, U):
        pump(which, 0)
    tokens_in.wait()
    own_tokens = token_region(side, core)
    token_copy(0, own_tokens, across).start()
    token_copy(1, own_tokens, partner).start()
    vectors_in.wait()
    token_copy(3, gain_region(core), partner).start()
    for which in (O, G, E, W):
        pool_copy(which).start()
    for which in (V, U):
        pump(which, 1)

    head = side * groups
    above = lax.broadcasted_iota(jnp.int32, (BLOCK, BLOCK), 1)
    below = lax.broadcasted_iota(jnp.int32, (BLOCK, BLOCK), 0)
    visible = lax.div(above, SEGMENT) <= lax.div(below, SEGMENT)
    bias_rows = mix_bias[...].astype(jnp.float32)
    for group in range(groups):
        weight = mix_weight[head + group].astype(jnp.float32)
        masked[group] = jnp.where(visible, weight, 0.0).astype(jnp.bfloat16)
        lower, upper = bias_rows[group : group + 1], bias_rows[group + groups : group + groups + 1]
        row = jnp.where(side == 0, lower, upper)
        bias_cols[group] = jnp.broadcast_to(row, (LANES, BLOCK)).T

    def rms_tile(source, place, gain_index):
        step_rows = 32

        def one(part, carry):
            rows = pl.ds(aligned(place * (tile // step_rows) + part, step_rows), step_rows)
            values = source[rows, :].astype(jnp.float32)
            scale = lax.rsqrt(jnp.mean(values * values, axis=1, keepdims=True) + EPS)
            normed[rows, :] = (values * scale * gains[gain_index : gain_index + 1, :]).astype(
                jnp.bfloat16
            )
            return carry

        lax.fori_loop(0, tile // step_rows, one, 0)

    def product(target, rows, weights, width, finish):
        def one(part, carry):
            columns = pl.ds(aligned(part, width), width)
            value = jnp.dot(
                normed[rows, :], weights[:, columns], preferred_element_type=jnp.float32
            )
            target[rows, columns] = finish(value)
            return carry

        lax.fori_loop(0, weights.shape[1] // width, one, 0)

    token_copy(1, token_region(side, 1 - core), partner).wait_recv()
    token_copy(3, gain_region(1 - core), partner).wait_recv()
    for step in range(2, last):
        for which in (V, U):
            pump(which, step)
        if step - 2 < half_tiles:
            rms_tile(rows_in, side * half_tiles + step - 2, 0)
    token_copy(0, token_region(1 - side, core), across).wait_recv()
    token_copy(2, token_region(1 - side, core), partner).start()
    for which in (V, U):
        pump(which, last)
    pump(O, 0)
    pump(O, 1)
    pump(G, 0)
    token_copy(2, token_region(1 - side, 1 - core), partner).wait_recv()
    for place in range(half_tiles):
        rms_tile(rows_in, (1 - side) * half_tiles + place, 0)

    lane = lax.broadcasted_iota(jnp.int32, (64, LANES), 1)

    def act_tile(place, weights, target, with_stats):
        rows = rows_of(place)
        product(target, rows, weights, 256, lambda value: value)

        def one(part, carry):
            some = pl.ds(aligned(place * (tile // 64) + part, 64), 64)
            value = gelu(target[some, :])
            target[some, :] = value
            if with_stats:
                sums = jnp.sum(value, axis=1, keepdims=True)
                squares = jnp.sum(value * value, axis=1, keepdims=True)
                stat_cols[some, :] = jnp.where(lane == 0, sums, jnp.where(lane == 1, squares, 0.0))
            return carry

        lax.fori_loop(0, tile // 64, one, 0)
        if with_stats:
            for part in range(tile // LANES):
                some = pl.ds(aligned(place * (tile // LANES) + part, LANES), LANES)
                stat_own[:, some] = stat_cols[some, :].T[0:8, :]

    drain(V)

    def v_tile(place, carry):
        act_tile(place, whole_v, act_v, True)
        return carry

    lax.fori_loop(0, tiles, v_tile, 0)
    near_stats = remote(stat_own, stat_near, stat_send.at[0], stat_recv.at[0], partner)
    near_stats.start()
    for which, step in ((O, 2), (O, 3), (G, 1)):
        pump(which, step)
    near_stats.wait_recv()
    stat_chip[...] = stat_own[...] + stat_near[...]
    far_stats = remote(stat_chip, stat_far, stat_send.at[1], stat_recv.at[1], across)
    far_stats.start()
    drain(U)

    def u_tile(place, carry):
        act_tile(place, whole_u, act_u, False)
        return carry

    lax.fori_loop(0, tiles, u_tile, 0)
    for which, step in ((O, 4), (O, 5), (E, 0)):
        pump(which, step)
    far_stats.wait_recv()

    def mix_block(block, carry):
        rows = pl.ds(aligned(block, BLOCK), BLOCK)
        sums = stat_chip[0:2, rows] + stat_far[0:2, rows]
        center_row = sums[0:1] / spread_width
        spread_row = sums[1:2] / spread_width - center_row * center_row
        scale_row = lax.rsqrt(spread_row + EPS)
        center = jnp.broadcast_to(center_row, (LANES, BLOCK)).T
        scale = jnp.broadcast_to(scale_row, (LANES, BLOCK)).T
        for group in range(groups):
            columns = slice(group * GROUP_DIM, (group + 1) * GROUP_DIM)
            own = pl.ds(aligned(side * groups + group, GROUP_DIM), GROUP_DIM)
            mixed = (
                (act_v[rows, columns] - center) * scale * vectors[2:3, own] + vectors[3:4, own]
            ).astype(jnp.bfloat16)
            spatial = (
                jnp.dot(masked[group], mixed, preferred_element_type=jnp.float32)
                + bias_cols[group]
            )
            gated[rows, columns] = (act_u[rows, columns] * spatial).astype(jnp.bfloat16)
        return carry

    lax.fori_loop(0, row_count // BLOCK, mix_block, 0)
    pump(O, last)
    pump(E, 1)
    pump(G, 2)
    pump(G, 3)
    drain(O)

    own_columns = pl.ds(aligned(core, own_width), own_width)
    other_columns = pl.ds(aligned(1 - core, own_width), own_width)

    def core_copy(place):
        rows = rows_of(place)
        return remote(
            partial.at[rows, other_columns],
            from_core.at[rows, :],
            core_send.at[place],
            core_recv.at[place],
            partner,
        )

    def side_copy(place):
        rows = rows_of(place)
        return remote(
            chip_sum.at[rows, :],
            from_side.at[rows, :],
            side_send.at[place],
            side_recv.at[place],
            across,
        )

    def half_copy(place, columns):
        region = stream.at[rows_of(place), columns]
        return remote(region, region, half_send.at[place], half_recv.at[place], partner)

    def out_tile(place, carry):
        rows = rows_of(place)

        def one(block, inner):
            columns = pl.ds(aligned(block, block_width), block_width)
            value = jnp.dot(gated[rows, :], whole_out[block], preferred_element_type=jnp.float32)
            partial[rows, columns] = value.astype(jnp.bfloat16)
            return inner

        lax.fori_loop(0, pairs, one, 0)
        core_copy(place).start()
        return carry

    lax.fori_loop(0, tiles, out_tile, 0)

    def chip_tile(place, carry):
        core_copy(place).wait_recv()
        rows = rows_of(place)
        chip_sum[rows, :] = (
            partial[rows, own_columns].astype(jnp.float32)
            + from_core[rows, :].astype(jnp.float32)
        ).astype(jnp.bfloat16)
        side_copy(place).start()
        return carry

    lax.fori_loop(0, tiles, chip_tile, 0)

    def stream_tile(place):
        side_copy(place).wait_recv()
        rows = rows_of(place)
        stream[rows, own_columns] = (
            rows_in[rows, own_columns].astype(jnp.float32)
            + chip_sum[rows, :].astype(jnp.float32)
            + from_side[rows, :].astype(jnp.float32)
        ).astype(jnp.bfloat16)
        half_copy(place, own_columns).start()

    def to_bfloat(value):
        return value.astype(jnp.bfloat16)

    def gate_tile(place):
        half_copy(place, other_columns).wait_recv()
        rms_tile(stream, place, 1)
        product(pre_gate, rows_of(place), whole_gate, 256, to_bfloat)

    for which, step in ((G, 4), (G, 5), (G, 6)):
        pump(which, step)
    after_tiles = (((E, 2), (E, 3)), ((E, 4), (E, 5)), ((E, 6), (W, 0)), ((W, 1),))
    for place in range(tiles):
        stream_tile(place)
        for which, step in after_tiles[place]:
            pump(which, step)
        if place == 0:
            drain(G)
        gate_tile(place)

    drain(E)
    shifted = lax.broadcasted_iota(jnp.int32, (tile, 256), 0)

    def taps(values, weights):
        before = jnp.where(shifted >= 1, pltpu.roll(values, 1, 0), 0.0)
        earlier = jnp.where(shifted >= 2, pltpu.roll(values, 2, 0), 0.0)
        return earlier * weights[0:1] + before * weights[1:2] + values * weights[2:3]

    def value_tile(place):
        rows = rows_of(place)

        def one(part, carry):
            columns = pl.ds(aligned(part, 256), 256)
            own = pl.ds(aligned(side * (units // 256) + part, 256), 256)
            value = jnp.dot(
                normed[rows, :], whole_value[:, columns], preferred_element_type=jnp.float32
            )
            value = value.astype(jnp.bfloat16).astype(jnp.float32)
            gate = pre_gate[rows, columns].astype(jnp.float32)
            conv_g = taps(gate, conv_gate[:, own].astype(jnp.float32))
            conv_v = taps(value, conv_value[:, own].astype(jnp.float32))
            hidden[rows, columns] = (jax.nn.silu(conv_g) * conv_v).astype(jnp.bfloat16)
            return carry

        lax.fori_loop(0, units // 256, one, 0)

    def value_tiles(turn, carry):
        def one(place, inner):
            value_tile(2 * turn + place)
            return inner

        lax.fori_loop(0, 2, one, 0)
        pump(W, 2 + turn)
        return carry

    lax.fori_loop(0, tiles // 2, value_tiles, 0)

    given, kept = (1 - side), side

    def near_copy(order, block, which_side, which):
        rows = rows_of(which_side, own_rows)
        quarter_block = block % half_blocks
        return remote(
            partial.at[rows, pl.ds(aligned(block, block_width), block_width)],
            near_down.at[rows, pl.ds(aligned(quarter_block, block_width), block_width)],
            near_send.at[2 * order + which],
            near_recv.at[2 * order + which],
            partner,
        )

    def far_copy(order, block):
        columns = pl.ds(aligned(block % half_blocks, block_width), block_width)
        return remote(
            chip_sum.at[pl.ds(0, own_rows), columns],
            far_down.at[:, columns],
            far_send.at[order],
            far_recv.at[order],
            across,
        )

    def down_block(order, block):
        columns = pl.ds(aligned(block, block_width), block_width)
        for which, which_side in enumerate((given, kept)):

            def one(part, carry):
                rows = rows_of(which_side * half_tiles + part)
                value = jnp.dot(
                    hidden[rows, :], whole_down[block], preferred_element_type=jnp.float32
                )
                partial[rows, columns] = value.astype(jnp.bfloat16)
                return carry

            lax.fori_loop(0, half_tiles, one, 0)

            @pl.when(block // half_blocks != core)
            def _():
                near_copy(order, block, which_side, which).start()

    def down_sum(order, block):
        columns = pl.ds(aligned(block, block_width), block_width)
        quarter_columns = pl.ds(aligned(block % half_blocks, block_width), block_width)

        @pl.when(block // half_blocks == core)
        def _():
            near_copy(order, block, given, 0).wait_recv()
            rows = rows_of(given, own_rows)
            chip_sum[pl.ds(0, own_rows), quarter_columns] = (
                partial[rows, columns].astype(jnp.float32)
                + near_down[rows, quarter_columns].astype(jnp.float32)
            ).astype(jnp.bfloat16)
            far_copy(order, block).start()
            near_copy(order, block, kept, 1).wait_recv()
            rows = rows_of(kept, own_rows)
            total[:, quarter_columns] = (
                stream[rows, columns].astype(jnp.float32)
                + partial[rows, columns].astype(jnp.float32)
                + near_down[rows, quarter_columns].astype(jnp.float32)
            )

    def down_end(order, block):
        quarter_columns = pl.ds(aligned(block % half_blocks, block_width), block_width)

        @pl.when(block // half_blocks == core)
        def _():
            far_copy(order, block).wait_recv()
            result[:, quarter_columns] = (
                total[:, quarter_columns] + far_down[:, quarter_columns].astype(jnp.float32)
            ).astype(jnp.bfloat16)

    def sent(place, carry):
        core_copy(place).wait_send()
        side_copy(place).wait_send()
        half_copy(place, own_columns).wait_send()
        return carry

    lax.fori_loop(0, tiles, sent, 0)

    blocks = [turned(0)]
    down_block(0, blocks[0])
    down_sum(0, blocks[0])
    for hop in range(1, depth + 1):
        here = [turned(-hop), turned(hop)] if hop < depth else [turned(depth)]
        if hop < depth:
            ready = {0: (2 * hop - 2, 2 * hop - 1), 1: (2 * hop - 2, 2 * hop - 1)}
        else:
            ready = {0: (last,), 1: (last,)}
        forwarded = 2 + tiles // 2
        for step in range(2 * hop, min(2 * hop + 2, last + 1)):
            if step >= forwarded:
                pump(W, step)
        if hop == depth - 1:
            ring_arrived(W, last - 1, 0)
            ring_arrived(W, last - 2, 1)
        if hop == depth:
            ring_arrived(W, last, 0)
            ring_arrived(W, last, 1)
        for block in here:
            down_block(len(blocks), block)
            blocks.append(block)
        for order in range(len(blocks) - len(here), len(blocks)):
            down_sum(order, blocks[order])
    for order, block in enumerate(blocks):
        down_end(order, block)

    for which in range(6):
        for step in range(steps):
            for way in range(2):
                ring_copy(which, step, way, step // 2).wait_send()
        pool_copy(which).wait_send()
    for order, block in enumerate(blocks):

        @pl.when(block // half_blocks != core)
        def _():
            near_copy(order, block, given, 0).wait_send()
            near_copy(order, block, kept, 1).wait_send()

        @pl.when(block // half_blocks == core)
        def _():
            far_copy(order, block).wait_send()

    token_copy(0, own_tokens, across).wait_send()
    token_copy(1, own_tokens, partner).wait_send()
    token_copy(2, token_region(1 - side, core), partner).wait_send()
    token_copy(3, gain_region(core), partner).wait_send()
    near_stats.wait_send()
    far_stats.wait_send()


def on_ring(
    fs_size,
    tokens,
    norm_gain,
    proj_u,
    proj_v,
    layer_gain,
    layer_shift,
    mix_weight,
    mix_bias,
    proj_out,
    ffn_gain,
    ffn_gate,
    ffn_value,
    conv_gate,
    conv_value,
    proj_down,
):
    own_rows, own_width = tokens.shape
    row_count, full = 2 * own_rows, 2 * own_width
    pairs = fs_size // 2
    steps = 2 * (pairs // 2) - 1
    quarter, units = proj_u.shape[1] // 2, ffn_gate.shape[1] // 2
    groups = quarter // GROUP_DIM
    tiles = row_count // SEQ_LEN
    bf16, f32 = jnp.bfloat16, jnp.float32
    pack = jnp.stack([norm_gain, ffn_gain, layer_gain, layer_shift]).astype(f32)
    vectors = jnp.concatenate([pack, jnp.zeros_like(pack)], axis=0)
    vmem, hbm = pl.BlockSpec(memory_space=pltpu.VMEM), pl.BlockSpec(memory_space=pl.ANY)
    dma = pltpu.SemaphoreType.DMA
    scratch = [
        pltpu.VMEM((full, quarter), bf16),
        pltpu.VMEM((full, quarter), bf16),
        pltpu.VMEM((pairs, quarter, 2 * proj_out.shape[1]), bf16),
        pltpu.VMEM((full, units), bf16),
        pltpu.VMEM((full, units), bf16),
        pltpu.VMEM((pairs, units, 2 * proj_down.shape[1]), bf16),
        pltpu.VMEM((row_count, full), bf16),
        pltpu.VMEM((row_count, full), bf16),
        pltpu.VMEM((8, full), f32),
        pltpu.VMEM((row_count, quarter), f32),
        pltpu.VMEM((row_count, quarter), f32),
        pltpu.VMEM((row_count, LANES), f32),
        pltpu.VMEM((8, row_count), f32),
        pltpu.VMEM((8, row_count), f32),
        pltpu.VMEM((8, row_count), f32),
        pltpu.VMEM((8, row_count), f32),
        pltpu.VMEM((groups, BLOCK, BLOCK), bf16),
        pltpu.VMEM((groups, BLOCK, LANES), f32),
        pltpu.VMEM((row_count, quarter), bf16),
        pltpu.VMEM((row_count, full), bf16),
        pltpu.VMEM((row_count, own_width), bf16),
        pltpu.VMEM((row_count, own_width), bf16),
        pltpu.VMEM((row_count, own_width), bf16),
        pltpu.VMEM((row_count, full), bf16),
        pltpu.VMEM((row_count, units), bf16),
        pltpu.VMEM((row_count, units), bf16),
        pltpu.VMEM((own_rows, own_width), f32),
        pltpu.VMEM((row_count, own_width), bf16),
        pltpu.VMEM((own_rows, own_width), bf16),
        dma((8,)),
        dma((6,)),
        dma((6,)),
        dma((12 * steps,)),
        dma((12 * steps,)),
        dma((4,)),
        dma((4,)),
        dma((2,)),
        dma((2,)),
        dma((tiles,)),
        dma((tiles,)),
        dma((tiles,)),
        dma((tiles,)),
        dma((tiles,)),
        dma((tiles,)),
        dma((2 * pairs,)),
        dma((2 * pairs,)),
        dma((pairs,)),
        dma((pairs,)),
    ]
    return pl.pallas_call(
        functools.partial(layer_kernel, fs_size),
        out_shape=jax.ShapeDtypeStruct((own_rows, own_width), bf16),
        in_specs=[hbm, vmem, vmem, vmem, vmem, vmem] + [hbm] * 6,
        out_specs=vmem,
        scratch_shapes=scratch,
        compiler_params=pltpu.CompilerParams(
            collective_id=0, has_side_effects=True, vmem_limit_bytes=VMEM_BYTES
        ),
        name="layer",
    )(
        tokens,
        vectors,
        mix_weight,
        mix_bias,
        conv_gate,
        conv_value,
        proj_u,
        proj_v,
        proj_out,
        ffn_gate,
        ffn_value,
        proj_down,
    )


def solution(mesh):
    fs_size, tp_size = mesh.shape["fs"], mesh.shape["tp"]
    ringed = tp_size == 2 and fs_size == 16
    in_specs = (
        P("fs", "tp"),
        P("tp"),
        P("fs", "tp"),
        P("fs", "tp"),
        P("tp"),
        P("tp"),
        P("tp", None, None),
        P("tp", None),
        P("tp", "fs"),
        P("tp"),
        P("fs", "tp"),
        P("fs", "tp"),
        P(None, "tp"),
        P(None, "tp"),
        P("tp", "fs"),
    )
    return jax.shard_map(
        functools.partial(on_ring, fs_size) if ringed else on_device,
        mesh=mesh,
        in_specs=in_specs,
        out_specs=P("fs", "tp"),
        check_vma=False,
    )
```

```python
import functools

import jax
import jax.numpy as jnp
from jax import lax
from jax.experimental import pallas as pl
from jax.experimental.pallas import tpu as pltpu
from jax.sharding import PartitionSpec as P

MESH = pl.DeviceIdType.MESH
LANES = 128

GROUP_DIM = 128
BLOCK = 128
SEGMENT = 64
KERNEL = 3
SEQ_LEN = 256


EPS = 1e-06


def matmul(operand, matrix):
    return jnp.dot(operand, matrix, preferred_element_type=jnp.float32)


def local_rms(values_in, gain_row):
    values = values_in.astype(jnp.float32)
    scale_row = lax.rsqrt(jnp.mean(values * values, axis=1, keepdims=True) + EPS)
    return (values * scale_row * gain_row.astype(jnp.float32)).astype(jnp.bfloat16)


def causal_taps(values, weights):
    seq_count = values.shape[0] // SEQ_LEN
    shaped = values.reshape(seq_count, SEQ_LEN, values.shape[1])
    padded = jnp.pad(shaped, ((0, 0), (KERNEL - 1, 0), (0, 0)))
    summed = jnp.zeros(shaped.shape, jnp.float32)
    for tap_index in range(KERNEL):
        summed = summed + padded[:, tap_index : tap_index + SEQ_LEN].astype(jnp.float32) * weights[
            tap_index
        ].astype(jnp.float32)
    return summed.reshape(values.shape[0], values.shape[1])


def on_device(
    tokens,
    norm_gain,
    proj_u,
    proj_v,
    layer_gain,
    layer_shift,
    mix_weight,
    mix_bias,
    proj_out,
    ffn_gain,
    ffn_gate,
    ffn_value,
    conv_gate,
    conv_value,
    proj_down,
):
    own_width = tokens.shape[1]
    whole_tokens, whole_gain, whole_ffn_gain = (
        lax.all_gather(tokens, "tp", axis=1, tiled=True),
        lax.all_gather(norm_gain, "tp", axis=0, tiled=True),
        lax.all_gather(ffn_gain, "tp", axis=0, tiled=True),
    )
    normed = local_rms(whole_tokens, whole_gain)
    row_count = normed.shape[0]
    whole_u, whole_v = (
        lax.all_gather(proj_u, "fs", axis=0, tiled=True),
        lax.all_gather(proj_v, "fs", axis=0, tiled=True),
    )
    pre_u = matmul(normed, whole_u)
    pre_v = matmul(normed, whole_v)
    act_u = jax.nn.gelu(pre_u, approximate=False)
    act_v = jax.nn.gelu(pre_v, approximate=False)
    full_width = act_v.shape[1] * lax.axis_size("tp")
    total_sum, second = lax.psum((jnp.sum(act_v, axis=1), jnp.sum(act_v * act_v, axis=1)), "tp")
    center = total_sum / full_width
    spread = second / full_width - center * center
    mixed_in = (
        (act_v - center[:, None])
        * lax.rsqrt(spread + EPS)[:, None]
        * layer_gain.astype(jnp.float32)
        + layer_shift.astype(jnp.float32)
    ).astype(jnp.bfloat16)
    groups = mixed_in.shape[1] // GROUP_DIM
    blocks = mixed_in.reshape(row_count // BLOCK, BLOCK, groups, GROUP_DIM)
    segment = jnp.arange(BLOCK) // SEGMENT
    visible = segment[None, :] <= segment[:, None]
    masked = jnp.where(visible[None], mix_weight, jnp.zeros_like(mix_weight))
    spatial = (
        jnp.einsum("gij,njgc->nigc", masked, blocks, preferred_element_type=jnp.float32)
        + mix_bias.astype(jnp.float32).T[None, :, :, None]
    )
    gated_rows = (act_u * spatial.reshape(row_count, mixed_in.shape[1])).astype(jnp.bfloat16)
    whole_out = lax.all_gather(proj_out, "fs", axis=1, tiled=True)
    partial_value = matmul(gated_rows, whole_out)
    summed = lax.psum(partial_value.astype(jnp.bfloat16), "tp").astype(jnp.float32)
    stream_rows = (whole_tokens.astype(jnp.float32) + summed).astype(jnp.bfloat16)
    normed_two = local_rms(stream_rows, whole_ffn_gain)
    stream = lax.dynamic_slice_in_dim(stream_rows, lax.axis_index("tp") * own_width, own_width, 1)
    whole_gate, whole_value = (
        lax.all_gather(ffn_gate, "fs", axis=0, tiled=True),
        lax.all_gather(ffn_value, "fs", axis=0, tiled=True),
    )
    pre_gate = matmul(normed_two, whole_gate)
    pre_value = matmul(normed_two, whole_value)
    conv_g = causal_taps(pre_gate.astype(jnp.bfloat16), conv_gate)
    conv_v = causal_taps(pre_value.astype(jnp.bfloat16), conv_value)
    hidden = (jax.nn.silu(conv_g) * conv_v).astype(jnp.bfloat16)
    whole_down = lax.all_gather(proj_down, "fs", axis=1, tiled=True)
    partial_two = matmul(hidden, whole_down)
    return (
        stream.astype(jnp.float32)
        + lax.psum_scatter(
            partial_two.astype(jnp.bfloat16), "tp", scatter_dimension=1, tiled=True
        ).astype(jnp.float32)
    ).astype(jnp.bfloat16)


V, U, O, G, E, W = range(6)
BY_ROWS = (V, U, G, E)
GATING = (V, U, O)
VMEM_BYTES = 67043328


def gelu(values):
    return 0.5 * values * (1.0 + lax.erf(values * (0.5**0.5)))


def aligned(index, size):
    return pl.multiple_of(index * size, size)


def layer_kernel(
    fs_size,
    tokens,
    vectors,
    mix_weight,
    mix_bias,
    conv_gate,
    conv_value,
    proj_u,
    proj_v,
    proj_out,
    ffn_gate,
    ffn_value,
    proj_down,
    result,
    whole_v,
    whole_u,
    whole_out,
    whole_gate,
    whole_value,
    whole_down,
    rows_in,
    normed,
    gains,
    act_v,
    act_u,
    stat_cols,
    stat_own,
    stat_chip,
    stat_near,
    stat_far,
    masked,
    bias_cols,
    gated,
    partial,
    from_core,
    chip_sum,
    from_side,
    stream,
    pre_gate,
    hidden,
    total,
    near_down,
    far_down,
    local_sem,
    pool_send,
    pool_recv,
    ring_send,
    ring_recv,
    flow_send,
    flow_recv,
    token_send,
    token_recv,
    stat_send,
    stat_recv,
    core_send,
    core_recv,
    side_send,
    side_recv,
    half_send,
    half_recv,
    depth_send,
    depth_recv,
    near_send,
    near_recv,
    far_send,
    far_recv,
):
    pairs = fs_size // 2
    depth = pairs // 2
    last = 2 * (depth - 1)
    steps = last + 1
    index, core = lax.axis_index("fs"), lax.axis_index("tp")
    side, pair = index % 2, index // 2
    level, column = pair // 2, pair % 2
    spot = level * (1 - column) + (pairs - 1 - level) * column

    def pair_at(place):
        far = place // depth
        return 2 * (place * (1 - far) + (pairs - 1 - place) * far) + far

    def turned(shift):
        return pair_at((spot + shift + pairs) % pairs)

    right = (2 * turned(1) + side, core)
    left = (2 * turned(-1) + side, core)
    across = (2 * pair + 1 - side, core)
    partner = (index, 1 - core)
    plane = fs_size // 4
    cell = index % plane
    low, half = level % 2, level // 2
    slot = (low + half) % 2
    over = (index + 2 * (1 - 2 * column), core)
    mate = (index + plane * (1 - 2 * low), core)
    mirror = ((3 - level) * plane + cell, core)

    own_rows, own_width = tokens.shape
    row_count, full = rows_in.shape
    tile = SEQ_LEN
    tiles = row_count // tile
    half_tiles = tiles // 2
    quarter = whole_v.shape[1]
    units = whole_gate.shape[1]
    groups = quarter // GROUP_DIM
    spread_width = 2 * 2 * quarter
    block_width = whole_out.shape[2]
    half_blocks = pairs // 2

    sources = (proj_v, proj_u, proj_out, ffn_gate, ffn_value, proj_down)
    wholes = (whole_v, whole_u, whole_out, whole_gate, whole_value, whole_down)

    def chunk(which, owner, part):
        whole = wholes[which]
        if which in BY_ROWS:
            depth_rows = sources[which].shape[0]
            return whole.at[pl.ds(aligned(2 * owner + part, depth_rows), depth_rows), :]
        width = sources[which].shape[1]
        return whole.at[owner, :, pl.ds(aligned(part, width), width)]

    def shard(which, part):
        source = sources[which]
        if which in BY_ROWS:
            width = source.shape[1] // 2
            return source.at[:, pl.ds(aligned(part, width), width)]
        height = source.shape[0] // 2
        return source.at[pl.ds(aligned(part, height), height), :]

    def piece(which, at_level, at_cell):
        whole = wholes[which]
        if which in BY_ROWS:
            depth_rows = sources[which].shape[0]
            return whole.at[pl.ds(aligned(at_level * plane + at_cell, depth_rows), depth_rows), :]
        width = sources[which].shape[1]
        block = (at_level // 2) * plane + at_cell
        return whole.at[block, :, pl.ds(aligned(at_level % 2, width), width)]

    def remote(source, target, send, recv, device):
        return pltpu.make_async_remote_copy(
            src_ref=source,
            dst_ref=target,
            send_sem=send,
            recv_sem=recv,
            device_id=device,
            device_id_type=MESH,
        )

    def own_copy(which):
        if which in GATING:
            source, target = shard(which, side), chunk(which, pair, side)
        else:
            source, target = shard(which, slot), piece(which, level, cell)
        return pltpu.make_async_copy(source, target, local_sem.at[which])

    def pool_copy(which):
        if which in GATING:
            source, target, device = shard(which, 1 - side), chunk(which, pair, side), across
        else:
            source, target, device = shard(which, 1 - slot), piece(which, level, cell), mate
        return remote(source, target, pool_send.at[which], pool_recv.at[which], device)

    def pool_arrived(which):
        if which in GATING:
            here, device = chunk(which, pair, 1 - side), across
        else:
            here, device = piece(which, level + 1 - 2 * low, cell), mate
        remote(here, here, pool_send.at[which], pool_recv.at[which], device).wait_recv()

    facing = 3 - level
    levels = (level, level + 1 - 2 * low, facing, facing + 1 - 2 * (facing % 2))
    beside, beyond = cell + 1 - 2 * side, cell + 2 - 4 * column
    across_diagonal = beside + 2 - 4 * column

    def send_on(which, way, step):
        if step < 4:
            here = piece(which, levels[step], cell)
        else:
            here = piece(which, levels[2 * (step - 4) + way], (beyond, beside)[way])
        place = (which - G) * 14 + way * 6 + step
        return remote(
            here, here, flow_send.at[place], flow_recv.at[place], (across, over)[way]
        )

    def come_in(which, way, step):
        if step < 4:
            here = piece(which, levels[step], (beside, beyond)[way])
        else:
            here = piece(which, levels[2 * (step - 4) + way], across_diagonal)
        place = (which - G) * 14 + way * 6 + step
        remote(
            here, here, flow_send.at[place], flow_recv.at[place], (across, over)[way]
        ).wait_recv()

    def reflect(which, part):
        here = piece(which, levels[part], cell)
        place = (which - G) * 14 + 12 + part
        return remote(here, here, flow_send.at[place], flow_recv.at[place], mirror)

    def reflected(which, part):
        here = piece(which, levels[2 + part], cell)
        place = (which - G) * 14 + 12 + part
        remote(here, here, flow_send.at[place], flow_recv.at[place], mirror).wait_recv()

    def by_x(which, step):
        send_on(which, 0, step).start()

    def by_y(which, step):
        send_on(which, 1, step).start()

    def relative(which_part):
        return side + which_part * (1 - 2 * side)

    def ring_copy(which, step, way, shift):
        part = step % 2 if way == 0 else step % 2 + step // last
        sign = 1 - 2 * way
        piece = chunk(which, turned(-sign * shift), relative(part))
        slot = (which * 2 + way) * steps + step
        return remote(
            piece, piece, ring_send.at[slot], ring_recv.at[slot], right if way == 0 else left
        )

    def ring_arrived(which, step, way):
        ring_copy(which, step, way, step // 2 + 1).wait_recv()

    def pump(which, step):
        if isinstance(step, int) and step == 0:
            own_copy(which).wait()
        elif isinstance(step, int) and step == 1:
            pool_arrived(which)
        else:
            ring_arrived(which, step - 2, 0)
            ring_arrived(which, step - 2 + step // last, 1)
        ring_copy(which, step, 0, step // 2).start()
        ring_copy(which, step, 1, step // 2).start()

    def drain(which):
        for step, way in ((last - 1, 0), (last, 0), (last - 2, 1), (last, 1)):
            ring_arrived(which, step, way)

    def token_region(which_side, which_core):
        return rows_in.at[
            pl.ds(aligned(which_side, own_rows), own_rows),
            pl.ds(aligned(which_core, own_width), own_width),
        ]

    def gain_region(which_core):
        return gains.at[:, pl.ds(aligned(which_core, own_width), own_width)]

    def token_copy(which, region, device):
        return remote(region, region, token_send.at[which], token_recv.at[which], device)

    def rows_of(place, height=tile):
        return pl.ds(aligned(place, height), height)

    barrier = pltpu.get_barrier_semaphore()
    for device in (right, left, across, over, mate, mirror, partner):
        pl.semaphore_signal(barrier, inc=1, device_id=device, device_id_type=MESH)
    for which in (V, U):
        own_copy(which).start()
    tokens_in = pltpu.make_async_copy(tokens, token_region(side, core), local_sem.at[6])
    tokens_in.start()
    vectors_in = pltpu.make_async_copy(vectors, gain_region(core), local_sem.at[7])
    vectors_in.start()
    for which in (O, G, E, W):
        own_copy(which).start()
    pl.semaphore_wait(barrier, 7)

    for which in (V, U):
        pool_copy(which).start()
    for which in (V, U):
        pump(which, 0)
    tokens_in.wait()
    own_tokens = token_region(side, core)
    token_copy(0, own_tokens, across).start()
    token_copy(1, own_tokens, partner).start()
    vectors_in.wait()
    token_copy(3, gain_region(core), partner).start()
    pool_copy(O).start()
    for which in (G, E, W):
        own_copy(which).wait()
        by_x(which, 0)
    for which in (V, U):
        pump(which, 1)

    head = side * groups
    above = lax.broadcasted_iota(jnp.int32, (BLOCK, BLOCK), 1)
    below = lax.broadcasted_iota(jnp.int32, (BLOCK, BLOCK), 0)
    visible = lax.div(above, SEGMENT) <= lax.div(below, SEGMENT)
    bias_rows = mix_bias[...].astype(jnp.float32)
    for group in range(groups):
        weight = mix_weight[head + group].astype(jnp.float32)
        masked[group] = jnp.where(visible, weight, 0.0).astype(jnp.bfloat16)
        lower, upper = bias_rows[group : group + 1], bias_rows[group + groups : group + groups + 1]
        row = jnp.where(side == 0, lower, upper)
        bias_cols[group] = jnp.broadcast_to(row, (LANES, BLOCK)).T

    def rms_tile(source, place, gain_index):
        step_rows = 32

        def one(part, carry):
            rows = pl.ds(aligned(place * (tile // step_rows) + part, step_rows), step_rows)
            values = source[rows, :].astype(jnp.float32)
            scale = lax.rsqrt(jnp.mean(values * values, axis=1, keepdims=True) + EPS)
            normed[rows, :] = (values * scale * gains[gain_index : gain_index + 1, :]).astype(
                jnp.bfloat16
            )
            return carry

        lax.fori_loop(0, tile // step_rows, one, 0)

    def product(target, rows, weights, width, finish):
        def one(part, carry):
            columns = pl.ds(aligned(part, width), width)
            value = jnp.dot(
                normed[rows, :], weights[:, columns], preferred_element_type=jnp.float32
            )
            target[rows, columns] = finish(value)
            return carry

        lax.fori_loop(0, weights.shape[1] // width, one, 0)

    token_copy(1, token_region(side, 1 - core), partner).wait_recv()
    token_copy(3, gain_region(1 - core), partner).wait_recv()
    for step in range(2, last):
        for which in (V, U):
            pump(which, step)
        if step - 2 < half_tiles:
            rms_tile(rows_in, side * half_tiles + step - 2, 0)
    token_copy(0, token_region(1 - side, core), across).wait_recv()
    token_copy(2, token_region(1 - side, core), partner).start()
    for which in (V, U):
        pump(which, last)
    pump(O, 0)
    pump(O, 1)
    pool_copy(G).start()
    reflect(G, 0).start()
    by_y(G, 0)
    token_copy(2, token_region(1 - side, 1 - core), partner).wait_recv()
    for place in range(half_tiles):
        rms_tile(rows_in, (1 - side) * half_tiles + place, 0)

    lane = lax.broadcasted_iota(jnp.int32, (64, LANES), 1)

    def act_tile(place, weights, target, with_stats):
        rows = rows_of(place)
        product(target, rows, weights, 256, lambda value: value)

        def one(part, carry):
            some = pl.ds(aligned(place * (tile // 64) + part, 64), 64)
            value = gelu(target[some, :])
            target[some, :] = value
            if with_stats:
                sums = jnp.sum(value, axis=1, keepdims=True)
                squares = jnp.sum(value * value, axis=1, keepdims=True)
                stat_cols[some, :] = jnp.where(lane == 0, sums, jnp.where(lane == 1, squares, 0.0))
            return carry

        lax.fori_loop(0, tile // 64, one, 0)
        if with_stats:
            for part in range(tile // LANES):
                some = pl.ds(aligned(place * (tile // LANES) + part, LANES), LANES)
                stat_own[:, some] = stat_cols[some, :].T[0:8, :]

    drain(V)

    def v_tile(place, carry):
        act_tile(place, whole_v, act_v, True)
        return carry

    lax.fori_loop(0, tiles, v_tile, 0)
    near_stats = remote(stat_own, stat_near, stat_send.at[0], stat_recv.at[0], partner)
    near_stats.start()
    pump(O, 2)
    pump(O, 3)
    pool_arrived(G)
    reflect(G, 1).start()
    by_x(G, 1)
    near_stats.wait_recv()
    stat_chip[...] = stat_own[...] + stat_near[...]
    far_stats = remote(stat_chip, stat_far, stat_send.at[1], stat_recv.at[1], across)
    far_stats.start()
    drain(U)

    def u_tile(place, carry):
        act_tile(place, whole_u, act_u, False)
        return carry

    lax.fori_loop(0, tiles, u_tile, 0)
    pump(O, 4)
    pump(O, 5)
    by_y(G, 1)
    reflected(G, 0)
    by_x(G, 2)
    far_stats.wait_recv()

    def mix_block(block, carry):
        rows = pl.ds(aligned(block, BLOCK), BLOCK)
        sums = stat_chip[0:2, rows] + stat_far[0:2, rows]
        center_row = sums[0:1] / spread_width
        spread_row = sums[1:2] / spread_width - center_row * center_row
        scale_row = lax.rsqrt(spread_row + EPS)
        center = jnp.broadcast_to(center_row, (LANES, BLOCK)).T
        scale = jnp.broadcast_to(scale_row, (LANES, BLOCK)).T
        for group in range(groups):
            columns = slice(group * GROUP_DIM, (group + 1) * GROUP_DIM)
            own = pl.ds(aligned(side * groups + group, GROUP_DIM), GROUP_DIM)
            mixed = (
                (act_v[rows, columns] - center) * scale * vectors[2:3, own] + vectors[3:4, own]
            ).astype(jnp.bfloat16)
            spatial = (
                jnp.dot(masked[group], mixed, preferred_element_type=jnp.float32)
                + bias_cols[group]
            )
            gated[rows, columns] = (act_u[rows, columns] * spatial).astype(jnp.bfloat16)
        return carry

    lax.fori_loop(0, row_count // BLOCK, mix_block, 0)
    pump(O, last)
    by_y(G, 2)
    pool_copy(E).start()
    reflect(E, 0).start()
    reflected(G, 1)
    by_y(G, 3)
    drain(O)

    own_columns = pl.ds(aligned(core, own_width), own_width)
    other_columns = pl.ds(aligned(1 - core, own_width), own_width)

    def core_copy(place):
        rows = rows_of(place)
        return remote(
            partial.at[rows, other_columns],
            from_core.at[rows, :],
            core_send.at[place],
            core_recv.at[place],
            partner,
        )

    def side_copy(place):
        return remote(
            chip_sum.at[rows_of((1 - side) * half_tiles + place), :],
            from_side.at[rows_of(place), :],
            side_send.at[place],
            side_recv.at[place],
            across,
        )

    def stream_rows(which_slot, place):
        return rows_of(which_slot * half_tiles + place)

    def half_copy(which_slot, place, columns, order):
        region = stream.at[stream_rows(which_slot, place), columns]
        return remote(region, region, half_send.at[order], half_recv.at[order], partner)

    def depth_copy(which_slot, place):
        region = stream.at[stream_rows(which_slot, place), own_columns]
        return remote(region, region, depth_send.at[place], depth_recv.at[place], mate)

    def out_tile(place, carry):
        rows = rows_of(place)

        def one(block, inner):
            columns = pl.ds(aligned(block, block_width), block_width)
            value = jnp.dot(gated[rows, :], whole_out[block], preferred_element_type=jnp.float32)
            partial[rows, columns] = value.astype(jnp.bfloat16)
            return inner

        lax.fori_loop(0, pairs, one, 0)
        core_copy(place).start()
        return carry

    lax.fori_loop((1 - side) * half_tiles, (2 - side) * half_tiles, out_tile, 0)
    lax.fori_loop(side * half_tiles, (1 + side) * half_tiles, out_tile, 0)

    def chip_tile(place):
        core_copy(place).wait_recv()
        rows = rows_of(place)
        chip_sum[rows, :] = (
            partial[rows, own_columns].astype(jnp.float32)
            + from_core[rows, :].astype(jnp.float32)
        ).astype(jnp.bfloat16)

    def own_tile(place):
        side_copy(place).wait_recv()
        rows = rows_of(side * half_tiles + place)
        stream[stream_rows(slot, place), own_columns] = (
            rows_in[rows, own_columns].astype(jnp.float32)
            + chip_sum[rows, :].astype(jnp.float32)
            + from_side[rows_of(place), :].astype(jnp.float32)
        ).astype(jnp.bfloat16)
        depth_copy(slot, place).start()
        half_copy(slot, place, own_columns, place).start()

    def far_tile(place):
        depth_copy(1 - slot, place).wait_recv()
        half_copy(1 - slot, place, own_columns, half_tiles + place).start()

    def to_bfloat(value):
        return value.astype(jnp.bfloat16)

    def gate_tile(which_slot, place, order):
        half_copy(which_slot, place, other_columns, order).wait_recv()
        rms_tile(stream, which_slot * half_tiles + place, 1)
        product(pre_gate, stream_rows(which_slot, place), whole_gate, 256, to_bfloat)

    come_in(G, 0, 1)
    by_y(G, 4)
    chip_tile((1 - side) * half_tiles)
    side_copy(0).start()
    by_x(G, 3)
    for place in range(1, half_tiles):
        chip_tile((1 - side) * half_tiles + place)
        side_copy(place).start()
    by_y(E, 0)
    for place in range(half_tiles):
        chip_tile(side * half_tiles + place)
    come_in(G, 1, 0)
    by_x(G, 4)
    pool_arrived(E)
    reflect(E, 1).start()
    by_y(E, 1)
    by_x(E, 1)
    own_tile(0)
    come_in(G, 0, 3)
    by_y(G, 5)
    come_in(G, 1, 2)
    by_x(G, 5)
    for place in range(1, half_tiles):
        own_tile(place)
    reflected(E, 0)
    by_y(E, 2)
    by_x(E, 2)
    far_tile(0)
    reflected(E, 1)
    by_y(E, 3)
    by_x(E, 3)
    for step in (0, 2, 4, 5):
        come_in(G, 0, step)
    for step in (1, 3, 4, 5):
        come_in(G, 1, step)
    pool_copy(W).start()
    reflect(W, 0).start()
    gate_tile(slot, 0, 0)
    gate_tile(slot, 1, 1)
    come_in(E, 0, 1)
    by_y(E, 4)
    come_in(E, 1, 0)
    by_x(E, 4)
    for place in range(1, half_tiles):
        far_tile(place)
    gate_tile(1 - slot, 0, half_tiles)
    come_in(E, 0, 3)
    by_y(E, 5)
    come_in(E, 1, 2)
    by_x(E, 5)
    by_y(W, 0)
    pool_arrived(W)
    reflect(W, 1).start()
    by_y(W, 1)
    by_x(W, 1)
    for place in range(1, half_tiles):
        gate_tile(1 - slot, place, half_tiles + place)
    for step in (0, 2, 4, 5):
        come_in(E, 0, step)
    for step in (1, 3, 4, 5):
        come_in(E, 1, step)
    shifted = lax.broadcasted_iota(jnp.int32, (tile, 256), 0)

    def taps(values, weights):
        before = jnp.where(shifted >= 1, pltpu.roll(values, 1, 0), 0.0)
        earlier = jnp.where(shifted >= 2, pltpu.roll(values, 2, 0), 0.0)
        return earlier * weights[0:1] + before * weights[1:2] + values * weights[2:3]

    def value_tile(place):
        rows = rows_of(place)

        def one(part, carry):
            columns = pl.ds(aligned(part, 256), 256)
            own = pl.ds(aligned(slot * (units // 256) + part, 256), 256)
            value = jnp.dot(
                normed[rows, :], whole_value[:, columns], preferred_element_type=jnp.float32
            )
            value = value.astype(jnp.bfloat16).astype(jnp.float32)
            gate = pre_gate[rows, columns].astype(jnp.float32)
            conv_g = taps(gate, conv_gate[:, own].astype(jnp.float32))
            conv_v = taps(value, conv_value[:, own].astype(jnp.float32))
            hidden[rows, columns] = (jax.nn.silu(conv_g) * conv_v).astype(jnp.bfloat16)
            return carry

        lax.fori_loop(0, units // 256, one, 0)

    def value_tiles(turn, carry):
        value_tile(turn)
        return carry

    lax.fori_loop(0, half_tiles, value_tiles, 0)
    reflected(W, 0)
    by_y(W, 2)
    by_x(W, 2)
    lax.fori_loop(half_tiles, tiles, value_tiles, 0)
    reflected(W, 1)
    by_y(W, 3)
    by_x(W, 3)

    given, kept = (1 - slot), slot

    def near_copy(order, block, which_side, which):
        rows = rows_of(which_side, own_rows)
        quarter_block = block % half_blocks
        return remote(
            partial.at[rows, pl.ds(aligned(block, block_width), block_width)],
            near_down.at[rows, pl.ds(aligned(quarter_block, block_width), block_width)],
            near_send.at[2 * order + which],
            near_recv.at[2 * order + which],
            partner,
        )

    def far_copy(order, block):
        columns = pl.ds(aligned(block % half_blocks, block_width), block_width)
        return remote(
            chip_sum.at[pl.ds(0, own_rows), columns],
            far_down.at[:, columns],
            far_send.at[order],
            far_recv.at[order],
            mate,
        )

    def down_block(order, block):
        columns = pl.ds(aligned(block, block_width), block_width)
        for which, which_side in enumerate((given, kept)):

            def one(part, carry):
                rows = rows_of(which_side * half_tiles + part)
                value = jnp.dot(
                    hidden[rows, :], whole_down[block], preferred_element_type=jnp.float32
                )
                partial[rows, columns] = value.astype(jnp.bfloat16)
                return carry

            lax.fori_loop(0, half_tiles, one, 0)

            @pl.when(block // half_blocks != core)
            def _():
                near_copy(order, block, which_side, which).start()

    def down_sum(order, block):
        columns = pl.ds(aligned(block, block_width), block_width)
        quarter_columns = pl.ds(aligned(block % half_blocks, block_width), block_width)

        @pl.when(block // half_blocks == core)
        def _():
            near_copy(order, block, given, 0).wait_recv()
            rows = rows_of(given, own_rows)
            chip_sum[pl.ds(0, own_rows), quarter_columns] = (
                partial[rows, columns].astype(jnp.float32)
                + near_down[rows, quarter_columns].astype(jnp.float32)
            ).astype(jnp.bfloat16)
            far_copy(order, block).start()
            near_copy(order, block, kept, 1).wait_recv()
            rows = rows_of(kept, own_rows)
            total[:, quarter_columns] = partial[rows, columns].astype(jnp.float32) + near_down[
                rows, quarter_columns
            ].astype(jnp.float32)

    def down_end(order, block):
        quarter_columns = pl.ds(aligned(block % half_blocks, block_width), block_width)

        @pl.when(block // half_blocks == core)
        def _():
            far_copy(order, block).wait_recv()
            rows = rows_of(kept, own_rows)
            strip_width = block_width // 2
            for strip in range(2):
                place = strip * plane + block % half_blocks
                summed = pl.ds(aligned(2 * (block % half_blocks) + strip, strip_width), strip_width)
                ours = pl.ds(aligned(core * 2 * plane + place, strip_width), strip_width)
                result[:, pl.ds(aligned(place, strip_width), strip_width)] = (
                    stream[rows, ours].astype(jnp.float32)
                    + total[:, summed]
                    + far_down[:, summed].astype(jnp.float32)
                ).astype(jnp.bfloat16)

    for place in range(tiles):
        core_copy(place).wait_send()
    for place in range(half_tiles):
        side_copy(place).wait_send()

    def block_at(at_level, at_cell):
        return (at_level // 2) * plane + at_cell

    cells = (cell, beside, beyond, across_diagonal)
    blocks = [block_at(at_level, at_cell) for at_cell in cells for at_level in (level, facing)]

    def run_blocks(*orders):
        for order in orders:
            down_block(order, blocks[order])
        for order in orders:
            down_sum(order, blocks[order])

    run_blocks(0, 1)
    come_in(W, 0, 1)
    by_y(W, 4)
    come_in(W, 1, 0)
    by_x(W, 4)
    come_in(W, 0, 0)
    come_in(W, 1, 1)
    run_blocks(2, 4)
    come_in(W, 0, 3)
    by_y(W, 5)
    come_in(W, 1, 2)
    by_x(W, 5)
    come_in(W, 0, 2)
    come_in(W, 1, 3)
    run_blocks(3, 5)
    come_in(W, 0, 4)
    come_in(W, 1, 4)
    run_blocks(6)
    come_in(W, 0, 5)
    come_in(W, 1, 5)
    run_blocks(7)
    for order, block in enumerate(blocks):
        down_end(order, block)

    for which in range(6):
        if which in GATING:
            for step in range(steps):
                for way in range(2):
                    ring_copy(which, step, way, step // 2).wait_send()
        else:
            for step in range(6):
                for way in range(2):
                    send_on(which, way, step).wait_send()
            for part in range(2):
                reflect(which, part).wait_send()
        pool_copy(which).wait_send()
    for place in range(half_tiles):
        depth_copy(slot, place).wait_send()
        half_copy(slot, place, own_columns, place).wait_send()
        half_copy(1 - slot, place, own_columns, half_tiles + place).wait_send()
    for order, block in enumerate(blocks):

        @pl.when(block // half_blocks != core)
        def _():
            near_copy(order, block, given, 0).wait_send()
            near_copy(order, block, kept, 1).wait_send()

        @pl.when(block // half_blocks == core)
        def _():
            far_copy(order, block).wait_send()

    token_copy(0, own_tokens, across).wait_send()
    token_copy(1, own_tokens, partner).wait_send()
    token_copy(2, token_region(1 - side, core), partner).wait_send()
    token_copy(3, gain_region(core), partner).wait_send()
    near_stats.wait_send()
    far_stats.wait_send()


def on_ring(
    fs_size,
    tokens,
    norm_gain,
    proj_u,
    proj_v,
    layer_gain,
    layer_shift,
    mix_weight,
    mix_bias,
    proj_out,
    ffn_gain,
    ffn_gate,
    ffn_value,
    conv_gate,
    conv_value,
    proj_down,
):
    own_rows, own_width = tokens.shape
    row_count, full = 2 * own_rows, 2 * own_width
    pairs = fs_size // 2
    steps = 2 * (pairs // 2) - 1
    quarter, units = proj_u.shape[1] // 2, ffn_gate.shape[1] // 2
    groups = quarter // GROUP_DIM
    tiles = row_count // SEQ_LEN
    bf16, f32 = jnp.bfloat16, jnp.float32
    pack = jnp.stack([norm_gain, ffn_gain, layer_gain, layer_shift]).astype(f32)
    vectors = jnp.concatenate([pack, jnp.zeros_like(pack)], axis=0)
    vmem, hbm = pl.BlockSpec(memory_space=pltpu.VMEM), pl.BlockSpec(memory_space=pl.ANY)
    dma = pltpu.SemaphoreType.DMA
    scratch = [
        pltpu.VMEM((full, quarter), bf16),
        pltpu.VMEM((full, quarter), bf16),
        pltpu.VMEM((pairs, quarter, 2 * proj_out.shape[1]), bf16),
        pltpu.VMEM((full, units), bf16),
        pltpu.VMEM((full, units), bf16),
        pltpu.VMEM((pairs, units, 2 * proj_down.shape[1]), bf16),
        pltpu.VMEM((row_count, full), bf16),
        pltpu.VMEM((row_count, full), bf16),
        pltpu.VMEM((8, full), f32),
        pltpu.VMEM((row_count, quarter), f32),
        pltpu.VMEM((row_count, quarter), f32),
        pltpu.VMEM((row_count, LANES), f32),
        pltpu.VMEM((8, row_count), f32),
        pltpu.VMEM((8, row_count), f32),
        pltpu.VMEM((8, row_count), f32),
        pltpu.VMEM((8, row_count), f32),
        pltpu.VMEM((groups, BLOCK, BLOCK), bf16),
        pltpu.VMEM((groups, BLOCK, LANES), f32),
        pltpu.VMEM((row_count, quarter), bf16),
        pltpu.VMEM((row_count, full), bf16),
        pltpu.VMEM((row_count, own_width), bf16),
        pltpu.VMEM((row_count, own_width), bf16),
        pltpu.VMEM((own_rows, own_width), bf16),
        pltpu.VMEM((row_count, full), bf16),
        pltpu.VMEM((row_count, units), bf16),
        pltpu.VMEM((row_count, units), bf16),
        pltpu.VMEM((own_rows, own_width), f32),
        pltpu.VMEM((row_count, own_width), bf16),
        pltpu.VMEM((own_rows, own_width), bf16),
        dma((8,)),
        dma((6,)),
        dma((6,)),
        dma((6 * steps,)),
        dma((6 * steps,)),
        dma((42,)),
        dma((42,)),
        dma((4,)),
        dma((4,)),
        dma((2,)),
        dma((2,)),
        dma((tiles,)),
        dma((tiles,)),
        dma((tiles // 2,)),
        dma((tiles // 2,)),
        dma((tiles,)),
        dma((tiles,)),
        dma((tiles // 2,)),
        dma((tiles // 2,)),
        dma((2 * pairs,)),
        dma((2 * pairs,)),
        dma((pairs,)),
        dma((pairs,)),
    ]
    return pl.pallas_call(
        functools.partial(layer_kernel, fs_size),
        out_shape=jax.ShapeDtypeStruct((own_rows, own_width), bf16),
        in_specs=[hbm, vmem, vmem, vmem, vmem, vmem] + [hbm] * 6,
        out_specs=vmem,
        scratch_shapes=scratch,
        compiler_params=pltpu.CompilerParams(
            collective_id=0, has_side_effects=True, vmem_limit_bytes=VMEM_BYTES
        ),
        name="layer",
    )(
        tokens,
        vectors,
        mix_weight,
        mix_bias,
        conv_gate,
        conv_value,
        proj_u,
        proj_v,
        proj_out,
        ffn_gate,
        ffn_value,
        proj_down,
    )


def solution(mesh):
    fs_size, tp_size = mesh.shape["fs"], mesh.shape["tp"]
    ringed = tp_size == 2 and fs_size == 16
    in_specs = (
        P("fs", "tp"),
        P("tp"),
        P("fs", "tp"),
        P("fs", "tp"),
        P("tp"),
        P("tp"),
        P("tp", None, None),
        P("tp", None),
        P("tp", "fs"),
        P("tp"),
        P("fs", "tp"),
        P("fs", "tp"),
        P(None, "tp"),
        P(None, "tp"),
        P("tp", "fs"),
    )
    return jax.shard_map(
        functools.partial(on_ring, fs_size) if ringed else on_device,
        mesh=mesh,
        in_specs=in_specs,
        out_specs=P("fs", "tp"),
        check_vma=False,
    )
```

```python
import functools

import jax
import jax.numpy as jnp
from jax import lax
from jax.experimental import pallas as pl
from jax.experimental.pallas import tpu as pltpu
from jax.sharding import PartitionSpec as P

MESH = pl.DeviceIdType.MESH
LANES = 128

GROUP_DIM = 128
BLOCK = 128
SEGMENT = 64
KERNEL = 3
SEQ_LEN = 256


EPS = 1e-06


def matmul(operand, matrix):
    return jnp.dot(operand, matrix, preferred_element_type=jnp.float32)


def local_rms(values_in, gain_row):
    values = values_in.astype(jnp.float32)
    scale_row = lax.rsqrt(jnp.mean(values * values, axis=1, keepdims=True) + EPS)
    return (values * scale_row * gain_row.astype(jnp.float32)).astype(jnp.bfloat16)


def causal_taps(values, weights):
    seq_count = values.shape[0] // SEQ_LEN
    shaped = values.reshape(seq_count, SEQ_LEN, values.shape[1])
    padded = jnp.pad(shaped, ((0, 0), (KERNEL - 1, 0), (0, 0)))
    summed = jnp.zeros(shaped.shape, jnp.float32)
    for tap_index in range(KERNEL):
        summed = summed + padded[:, tap_index : tap_index + SEQ_LEN].astype(jnp.float32) * weights[
            tap_index
        ].astype(jnp.float32)
    return summed.reshape(values.shape[0], values.shape[1])


def on_device(
    tokens,
    norm_gain,
    proj_u,
    proj_v,
    layer_gain,
    layer_shift,
    mix_weight,
    mix_bias,
    proj_out,
    ffn_gain,
    ffn_gate,
    ffn_value,
    conv_gate,
    conv_value,
    proj_down,
):
    own_width = tokens.shape[1]
    whole_tokens, whole_gain, whole_ffn_gain = (
        lax.all_gather(tokens, "tp", axis=1, tiled=True),
        lax.all_gather(norm_gain, "tp", axis=0, tiled=True),
        lax.all_gather(ffn_gain, "tp", axis=0, tiled=True),
    )
    normed = local_rms(whole_tokens, whole_gain)
    row_count = normed.shape[0]
    whole_u, whole_v = (
        lax.all_gather(proj_u, "fs", axis=0, tiled=True),
        lax.all_gather(proj_v, "fs", axis=0, tiled=True),
    )
    pre_u = matmul(normed, whole_u)
    pre_v = matmul(normed, whole_v)
    act_u = jax.nn.gelu(pre_u, approximate=False)
    act_v = jax.nn.gelu(pre_v, approximate=False)
    full_width = act_v.shape[1] * lax.axis_size("tp")
    total_sum, second = lax.psum((jnp.sum(act_v, axis=1), jnp.sum(act_v * act_v, axis=1)), "tp")
    center = total_sum / full_width
    spread = second / full_width - center * center
    mixed_in = (
        (act_v - center[:, None])
        * lax.rsqrt(spread + EPS)[:, None]
        * layer_gain.astype(jnp.float32)
        + layer_shift.astype(jnp.float32)
    ).astype(jnp.bfloat16)
    groups = mixed_in.shape[1] // GROUP_DIM
    blocks = mixed_in.reshape(row_count // BLOCK, BLOCK, groups, GROUP_DIM)
    segment = jnp.arange(BLOCK) // SEGMENT
    visible = segment[None, :] <= segment[:, None]
    masked = jnp.where(visible[None], mix_weight, jnp.zeros_like(mix_weight))
    spatial = (
        jnp.einsum("gij,njgc->nigc", masked, blocks, preferred_element_type=jnp.float32)
        + mix_bias.astype(jnp.float32).T[None, :, :, None]
    )
    gated_rows = (act_u * spatial.reshape(row_count, mixed_in.shape[1])).astype(jnp.bfloat16)
    whole_out = lax.all_gather(proj_out, "fs", axis=1, tiled=True)
    partial_value = matmul(gated_rows, whole_out)
    summed = lax.psum(partial_value.astype(jnp.bfloat16), "tp").astype(jnp.float32)
    stream_rows = (whole_tokens.astype(jnp.float32) + summed).astype(jnp.bfloat16)
    normed_two = local_rms(stream_rows, whole_ffn_gain)
    stream = lax.dynamic_slice_in_dim(stream_rows, lax.axis_index("tp") * own_width, own_width, 1)
    whole_gate, whole_value = (
        lax.all_gather(ffn_gate, "fs", axis=0, tiled=True),
        lax.all_gather(ffn_value, "fs", axis=0, tiled=True),
    )
    pre_gate = matmul(normed_two, whole_gate)
    pre_value = matmul(normed_two, whole_value)
    conv_g = causal_taps(pre_gate.astype(jnp.bfloat16), conv_gate)
    conv_v = causal_taps(pre_value.astype(jnp.bfloat16), conv_value)
    hidden = (jax.nn.silu(conv_g) * conv_v).astype(jnp.bfloat16)
    whole_down = lax.all_gather(proj_down, "fs", axis=1, tiled=True)
    partial_two = matmul(hidden, whole_down)
    return (
        stream.astype(jnp.float32)
        + lax.psum_scatter(
            partial_two.astype(jnp.bfloat16), "tp", scatter_dimension=1, tiled=True
        ).astype(jnp.float32)
    ).astype(jnp.bfloat16)


V, U, O, G, E, W = range(6)
NAMES = ("V", "U", "O", "G", "E", "W")
ORDER = (
    "yG0", "poolG", "yV0", "poolU", "xG0", "xO0", "poolV", "yO0", "poolE", "xU0", "poolO",
    "halftok", "yW0", "poolW", "mirV0", "yU0", "mirO0", "yE0", "mirG0", "xG4", "xV4", "yG1", "xG1",
    "mirV1", "xV1", "mirU0", "mirU1", "mirO1", "prep", "xE0", "yU1", "xO4", "yE1", "xV2", "xV0",
    "yO1", "yV2", "xO1", "yG2", "Nk1", "xV3", "xV5", "Nk0", "tok", "mirG1", "xU2", "yO2", "mirE0",
    "xU1", "yU3", "yU2", "xU3", "yV5", "xO5", "xO2", "yV1", "mirE1", "xU4", "yO4", "mirW1", "xO3",
    "xG2", "xU5", "yV3", "yU5", "yV4", "fwd", "Ng0", "yO5", "Ng1", "yU4", "yO3", "Vk1", "xE1",
    "Vk0", "xG5", "yE2", "Vg1", "xG3", "Vg0", "statA", "yG4", "yG3", "statB", "xE2", "yE4", "statC",
    "Uk1", "Mk1", "Ok1", "Uk0", "Mk0", "xE3", "xE4", "mirW0", "Ck1", "sidek1", "yG5", "xE5", "Ug0",
    "Ug1", "Ok0", "Ck0", "Mg1", "xW0", "yW2", "sidek0", "Og1", "Cg1", "yE5", "Sg1", "Gg1", "xW2",
    "sideg1", "Mg0", "yE3", "yW1", "yW3", "Og0", "Cg0", "sideg0", "Sg0", "xW3", "Gg0", "Eg0", "xW1",
    "Eg1", "DG4", "DG5", "DG0", "Sk1", "DG2", "SG2", "Gk1", "xW4", "SG4", "far4", "yW4", "Ek1",
    "DG6", "SG0", "yW5", "Sk0", "far2", "SG6", "xW5", "far6", "SG5", "far5", "Gk0", "Ek0", "far0",
    "DK5", "DG3", "DG1", "DK7", "SG1", "DG7", "DK2", "far1", "DK4", "SK7", "DK6", "SK4", "SG7",
    "far7", "END4", "SG3", "far3", "DK0", "SK2", "END2", "DK3", "DK1", "END7", "SK1", "END1", "SK0",
    "END0", "SK6", "END6", "SK5", "END5", "SK3", "END3",
)
BY_ROWS = (V, U, G, E)
VMEM_BYTES = 67043328


def gelu(values):
    return 0.5 * values * (1.0 + lax.erf(values * (0.5**0.5)))


def aligned(index, size):
    return pl.multiple_of(index * size, size)


def layer_kernel(
    fs_size,
    tokens,
    vectors,
    mix_weight,
    mix_bias,
    conv_gate,
    conv_value,
    proj_u,
    proj_v,
    proj_out,
    ffn_gate,
    ffn_value,
    proj_down,
    result,
    whole_v,
    whole_u,
    whole_out,
    whole_gate,
    whole_value,
    whole_down,
    rows_in,
    normed,
    gains,
    act_v,
    act_u,
    stat_cols,
    stat_own,
    stat_chip,
    stat_near,
    stat_far,
    masked,
    bias_cols,
    gated,
    partial,
    from_core,
    chip_sum,
    from_side,
    stream,
    pre_gate,
    hidden,
    total,
    given_down,
    near_down,
    far_down,
    local_sem,
    pool_send,
    pool_recv,
    flow_send,
    flow_recv,
    token_send,
    token_recv,
    stat_send,
    stat_recv,
    core_send,
    core_recv,
    side_send,
    side_recv,
    half_send,
    half_recv,
    near_send,
    near_recv,
    far_send,
    far_recv,
):
    pairs = fs_size // 2
    plane = fs_size // 4
    index, core = lax.axis_index("fs"), lax.axis_index("tp")
    level, cell = index // plane, index % plane
    side, column = cell % 2, cell // 2
    low, half = level % 2, level // 2
    slot = (low + half) % 2
    facing = 3 - level
    levels = (level, level + 1 - 2 * low, facing, facing + 1 - 2 * (facing % 2))
    beside, beyond = cell + 1 - 2 * side, cell + 2 - 4 * column
    diagonal = beside + 2 - 4 * column

    partner = (index, 1 - core)
    mate = (levels[1] * plane + cell, core)
    mirror = (facing * plane + cell, core)
    across = (level * plane + beside, core)
    over = (level * plane + beyond, core)

    own_rows, own_width = tokens.shape
    row_count, full = rows_in.shape
    tile = SEQ_LEN
    tiles = row_count // tile
    half_tiles = tiles // 2
    quarter = whole_v.shape[1]
    units = whole_gate.shape[1]
    groups = quarter // GROUP_DIM
    spread_width = 2 * 2 * quarter
    block_width = whole_out.shape[2]
    half_blocks = pairs // 2

    sources = (proj_v, proj_u, proj_out, ffn_gate, ffn_value, proj_down)
    wholes = (whole_v, whole_u, whole_out, whole_gate, whole_value, whole_down)

    def shard(which, part):
        source = sources[which]
        if which in BY_ROWS:
            width = source.shape[1] // 2
            return source.at[:, pl.ds(aligned(part, width), width)]
        height = source.shape[0] // 2
        return source.at[pl.ds(aligned(part, height), height), :]

    def piece(which, at_level, at_cell):
        whole = wholes[which]
        if which in BY_ROWS:
            depth_rows = sources[which].shape[0]
            return whole.at[pl.ds(aligned(at_level * plane + at_cell, depth_rows), depth_rows), :]
        width = sources[which].shape[1]
        block = (at_level // 2) * plane + at_cell
        return whole.at[block, :, pl.ds(aligned(at_level % 2, width), width)]

    def remote(source, target, send, recv, device):
        return pltpu.make_async_remote_copy(
            src_ref=source,
            dst_ref=target,
            send_sem=send,
            recv_sem=recv,
            device_id=device,
            device_id_type=MESH,
        )

    def own_copy(which):
        return pltpu.make_async_copy(
            shard(which, slot), piece(which, level, cell), local_sem.at[which]
        )

    def pool_copy(which):
        return remote(
            shard(which, 1 - slot),
            piece(which, level, cell),
            pool_send.at[which],
            pool_recv.at[which],
            mate,
        )

    def pool_arrived(which):
        here = piece(which, levels[1], cell)
        remote(here, here, pool_send.at[which], pool_recv.at[which], mate).wait_recv()

    def moved(which, here, slot_index, device):
        place = which * 14 + slot_index
        return remote(here, here, flow_send.at[place], flow_recv.at[place], device)

    def send_on(which, way, step):
        if step < 4:
            here = piece(which, levels[step], cell)
        else:
            here = piece(which, levels[2 * (step - 4) + way], (beyond, beside)[way])
        return moved(which, here, way * 6 + step, (across, over)[way])

    def come_in(which, way, step):
        if step < 4:
            here = piece(which, levels[step], (beside, beyond)[way])
        else:
            here = piece(which, levels[2 * (step - 4) + way], diagonal)
        moved(which, here, way * 6 + step, (across, over)[way]).wait_recv()

    def reflect(which, part):
        return moved(which, piece(which, levels[part], cell), 12 + part, mirror)

    def reflected(which, part):
        moved(which, piece(which, levels[2 + part], cell), 12 + part, mirror).wait_recv()

    def token_region(which_side, which_core):
        return rows_in.at[
            pl.ds(aligned(which_side, own_rows), own_rows),
            pl.ds(aligned(which_core, own_width), own_width),
        ]

    def gain_region(which_core):
        return gains.at[:, pl.ds(aligned(which_core, own_width), own_width)]

    def token_copy(which, region, device):
        return remote(region, region, token_send.at[which], token_recv.at[which], device)

    def rows_of(place, height=tile):
        return pl.ds(aligned(place, height), height)

    barrier = pltpu.get_barrier_semaphore()
    for device in (across, over, mate, mirror, partner):
        pl.semaphore_signal(barrier, inc=1, device_id=device, device_id_type=MESH)
    for which in (V, U, O):
        own_copy(which).start()
    tokens_in = pltpu.make_async_copy(tokens, token_region(slot, core), local_sem.at[6])
    tokens_in.start()
    vectors_in = pltpu.make_async_copy(vectors, gain_region(core), local_sem.at[7])
    vectors_in.start()
    for which in (G, E, W):
        own_copy(which).start()
    pl.semaphore_wait(barrier, 5)

    own_tokens = token_region(slot, core)
    def arrive_pool(which):
        return lambda: pool_arrived(which)

    def arrive_mirror(which, part):
        return lambda: reflected(which, part)

    def arrive_flow(which, way, step):
        return lambda: come_in(which, way, step)

    done = set()

    def once(name, wait):
        if name not in done:
            done.add(name)
            wait()

    def own_here(which):
        once(("own", which), lambda: own_copy(which).wait())

    def pool_here(which):
        once(("pool", which), arrive_pool(which))

    def mirror_here(which, part):
        once(("mirror", which, part), arrive_mirror(which, part))

    def flow_here(which, way, step):
        once(("flow", which, way, step), arrive_flow(which, way, step))

    def part_here(which, part):
        (own_here, pool_here)[part](which)

    def all_here(which):
        own_here(which)
        pool_here(which)
        for part in range(2):
            mirror_here(which, part)
        for step in range(6):
            for way in range(2):
                flow_here(which, way, step)

    def send_flow(which, way, step):
        if step < 2:
            part_here(which, step)
        elif step < 4:
            mirror_here(which, step - 2)
        else:
            flow_here(which, 1 - way, 2 * (step - 4) + way)
        send_on(which, way, step).start()

    def send_mirror(which, part):
        part_here(which, part)
        reflect(which, part).start()

    tokens_in.wait()
    token_copy(1, own_tokens, partner).start()
    vectors_in.wait()
    token_copy(3, gain_region(core), partner).start()

    head = slot * groups

    def prepare():
        above = lax.broadcasted_iota(jnp.int32, (BLOCK, BLOCK), 1)
        below = lax.broadcasted_iota(jnp.int32, (BLOCK, BLOCK), 0)
        visible = lax.div(above, SEGMENT) <= lax.div(below, SEGMENT)
        bias_rows = mix_bias[...].astype(jnp.float32)
        for group in range(groups):
            weight = mix_weight[head + group].astype(jnp.float32)
            masked[group] = jnp.where(visible, weight, 0.0).astype(jnp.bfloat16)
            lower = bias_rows[group : group + 1]
            upper = bias_rows[group + groups : group + groups + 1]
            row = jnp.where(slot == 0, lower, upper)
            bias_cols[group] = jnp.broadcast_to(row, (LANES, BLOCK)).T

    first, second = slot * half_tiles, (1 - slot) * half_tiles

    def near_tokens():
        token_copy(1, token_region(slot, 1 - core), partner).wait_recv()
        token_copy(3, gain_region(1 - core), partner).wait_recv()

    def pass_tokens():
        token_copy(0, token_region(1 - slot, core), mate).wait_recv()
        token_copy(2, token_region(1 - slot, core), partner).start()

    def last_tokens():
        token_copy(2, token_region(1 - slot, 1 - core), partner).wait_recv()

    def rms_tile(source, place, gain_index):
        step_rows = 32

        def one(part, carry):
            rows = pl.ds(aligned(place * (tile // step_rows) + part, step_rows), step_rows)
            values = source[rows, :].astype(jnp.float32)
            scale = lax.rsqrt(jnp.mean(values * values, axis=1, keepdims=True) + EPS)
            normed[rows, :] = (values * scale * gains[gain_index : gain_index + 1, :]).astype(
                jnp.bfloat16
            )
            return carry

        lax.fori_loop(0, tile // step_rows, one, 0)

    def product(target, rows, weights, width, finish):
        def one(part, carry):
            columns = pl.ds(aligned(part, width), width)
            value = jnp.dot(
                normed[rows, :], weights[:, columns], preferred_element_type=jnp.float32
            )
            target[rows, columns] = finish(value)
            return carry

        lax.fori_loop(0, weights.shape[1] // width, one, 0)

    lane = lax.broadcasted_iota(jnp.int32, (64, LANES), 1)

    def act_tile(place, weights, target, with_stats):
        rows = rows_of(place)
        product(target, rows, weights, 256, lambda value: value)

        def one(part, carry):
            some = pl.ds(aligned(place * (tile // 64) + part, 64), 64)
            value = gelu(target[some, :])
            target[some, :] = value
            if with_stats:
                sums = jnp.sum(value, axis=1, keepdims=True)
                squares = jnp.sum(value * value, axis=1, keepdims=True)
                stat_cols[some, :] = jnp.where(lane == 0, sums, jnp.where(lane == 1, squares, 0.0))
            return carry

        lax.fori_loop(0, tile // 64, one, 0)
        if with_stats:
            for part in range(tile // LANES):
                some = pl.ds(aligned(place * (tile // LANES) + part, LANES), LANES)
                stat_own[:, some] = stat_cols[some, :].T[0:8, :]

    near_stats = remote(stat_own, stat_near, stat_send.at[0], stat_recv.at[0], partner)
    far_stats = remote(stat_chip, stat_far, stat_send.at[1], stat_recv.at[1], mate)

    def sum_stats():
        near_stats.wait_recv()
        stat_chip[...] = stat_own[...] + stat_near[...]

    def mix_block(block, carry):
        rows = pl.ds(aligned(block, BLOCK), BLOCK)
        sums = stat_chip[0:2, rows] + stat_far[0:2, rows]
        center_row = sums[0:1] / spread_width
        spread_row = sums[1:2] / spread_width - center_row * center_row
        scale_row = lax.rsqrt(spread_row + EPS)
        center = jnp.broadcast_to(center_row, (LANES, BLOCK)).T
        scale = jnp.broadcast_to(scale_row, (LANES, BLOCK)).T
        for group in range(groups):
            columns = slice(group * GROUP_DIM, (group + 1) * GROUP_DIM)
            own = pl.ds(aligned(slot * groups + group, GROUP_DIM), GROUP_DIM)
            mixed = (
                (act_v[rows, columns] - center) * scale * vectors[2:3, own] + vectors[3:4, own]
            ).astype(jnp.bfloat16)
            spatial = (
                jnp.dot(masked[group], mixed, preferred_element_type=jnp.float32)
                + bias_cols[group]
            )
            gated[rows, columns] = (act_u[rows, columns] * spatial).astype(jnp.bfloat16)
        return carry

    def mix_tile(place):
        once("stats", far_stats.wait_recv)
        ratio = tile // BLOCK
        lax.fori_loop(place * ratio, (place + 1) * ratio, mix_block, 0)

    own_columns = pl.ds(aligned(core, own_width), own_width)
    other_columns = pl.ds(aligned(1 - core, own_width), own_width)

    def core_copy(place):
        rows = rows_of(place)
        return remote(
            partial.at[rows, other_columns],
            from_core.at[rows, :],
            core_send.at[place],
            core_recv.at[place],
            partner,
        )

    def side_copy(place):
        rows = rows_of(place)
        return remote(
            chip_sum.at[rows, :],
            from_side.at[rows, :],
            side_send.at[place],
            side_recv.at[place],
            mate,
        )

    def half_copy(place, columns):
        region = stream.at[rows_of(place), columns]
        return remote(region, region, half_send.at[place], half_recv.at[place], partner)

    def out_tile(place):
        rows = rows_of(place)

        def one(block, inner):
            columns = pl.ds(aligned(block, block_width), block_width)
            value = jnp.dot(gated[rows, :], whole_out[block], preferred_element_type=jnp.float32)
            partial[rows, columns] = value.astype(jnp.bfloat16)
            return inner

        lax.fori_loop(0, pairs, one, 0)
        core_copy(place).start()

    def chip_tile(place):
        core_copy(place).wait_recv()
        rows = rows_of(place)
        chip_sum[rows, :] = (
            partial[rows, own_columns].astype(jnp.float32)
            + from_core[rows, :].astype(jnp.float32)
        ).astype(jnp.bfloat16)

    strip_width = block_width // 2

    def strips():
        for strip in range(2):
            for place in range(half_blocks):
                ours = pl.ds(
                    aligned(core * 2 * plane + strip * plane + place, strip_width), strip_width
                )
                start = (2 * place + strip) * strip_width
                yield ours, slice(start, start + strip_width)

    def stream_tile(place):
        side_copy(place).wait_recv()
        rows = rows_of(place)
        for ours, summed in strips():
            stream[rows, ours] = (
                rows_in[rows, ours].astype(jnp.float32)
                + chip_sum[rows, summed].astype(jnp.float32)
                + from_side[rows, summed].astype(jnp.float32)
            ).astype(jnp.bfloat16)
        half_copy(place, own_columns).start()

    def to_bfloat(value):
        return value.astype(jnp.bfloat16)

    def gate_tile(place):
        half_copy(place, other_columns).wait_recv()
        rms_tile(stream, place, 1)
        product(pre_gate, rows_of(place), whole_gate, 256, to_bfloat)

    shifted = lax.broadcasted_iota(jnp.int32, (tile, 256), 0)

    def taps(values, weights):
        before = jnp.where(shifted >= 1, pltpu.roll(values, 1, 0), 0.0)
        earlier = jnp.where(shifted >= 2, pltpu.roll(values, 2, 0), 0.0)
        return earlier * weights[0:1] + before * weights[1:2] + values * weights[2:3]

    def value_tile(place):
        rows = rows_of(place)

        def one(part, carry):
            columns = pl.ds(aligned(part, 256), 256)
            own = pl.ds(aligned(slot * (units // 256) + part, 256), 256)
            value = jnp.dot(
                normed[rows, :], whole_value[:, columns], preferred_element_type=jnp.float32
            )
            value = value.astype(jnp.bfloat16).astype(jnp.float32)
            gate = pre_gate[rows, columns].astype(jnp.float32)
            conv_g = taps(gate, conv_gate[:, own].astype(jnp.float32))
            conv_v = taps(value, conv_value[:, own].astype(jnp.float32))
            hidden[rows, columns] = (jax.nn.silu(conv_g) * conv_v).astype(jnp.bfloat16)
            return carry

        lax.fori_loop(0, units // 256, one, 0)

    given, kept = (1 - slot), slot

    def near_copy(order, block, which_side, which):
        rows = rows_of(which_side, own_rows)
        quarter_block = block % half_blocks
        return remote(
            partial.at[rows, pl.ds(aligned(block, block_width), block_width)],
            near_down.at[rows, pl.ds(aligned(quarter_block, block_width), block_width)],
            near_send.at[2 * order + which],
            near_recv.at[2 * order + which],
            partner,
        )

    def far_copy(order, block):
        columns = pl.ds(aligned(block % half_blocks, block_width), block_width)
        return remote(
            given_down.at[:, columns],
            far_down.at[:, columns],
            far_send.at[order],
            far_recv.at[order],
            mate,
        )

    def down_block(order, which):
        block = blocks[order]
        which_side = (given, kept)[which]
        columns = pl.ds(aligned(block, block_width), block_width)

        def one(part, carry):
            rows = rows_of(which_side * half_tiles + part)
            value = jnp.dot(hidden[rows, :], whole_down[block], preferred_element_type=jnp.float32)
            partial[rows, columns] = value.astype(jnp.bfloat16)
            return carry

        lax.fori_loop(0, half_tiles, one, 0)

        @pl.when(block // half_blocks != core)
        def _():
            near_copy(order, block, which_side, which).start()

    def given_sum(order):
        block = blocks[order]
        columns = pl.ds(aligned(block, block_width), block_width)
        quarter_columns = pl.ds(aligned(block % half_blocks, block_width), block_width)

        @pl.when(block // half_blocks == core)
        def _():
            near_copy(order, block, given, 0).wait_recv()
            rows = rows_of(given, own_rows)
            given_down[:, quarter_columns] = (
                partial[rows, columns].astype(jnp.float32)
                + near_down[rows, quarter_columns].astype(jnp.float32)
            ).astype(jnp.bfloat16)

    def send_given(order):
        block = blocks[order]

        @pl.when(block // half_blocks == core)
        def _():
            far_copy(order, block).start()

    def kept_sum(order):
        block = blocks[order]
        columns = pl.ds(aligned(block, block_width), block_width)
        quarter_columns = pl.ds(aligned(block % half_blocks, block_width), block_width)

        @pl.when(block // half_blocks == core)
        def _():
            near_copy(order, block, kept, 1).wait_recv()
            rows = rows_of(kept, own_rows)
            total[:, quarter_columns] = partial[rows, columns].astype(jnp.float32) + near_down[
                rows, quarter_columns
            ].astype(jnp.float32)

    def down_end(order, block):
        quarter_columns = pl.ds(aligned(block % half_blocks, block_width), block_width)

        @pl.when(block // half_blocks == core)
        def _():
            far_copy(order, block).wait_recv()
            rows = rows_of(kept, own_rows)
            for strip in range(2):
                place = strip * plane + block % half_blocks
                summed = pl.ds(aligned(2 * (block % half_blocks) + strip, strip_width), strip_width)
                ours = pl.ds(aligned(core * 2 * plane + place, strip_width), strip_width)
                result[:, pl.ds(aligned(place, strip_width), strip_width)] = (
                    stream[rows, ours].astype(jnp.float32)
                    + total[:, summed]
                    + far_down[:, summed].astype(jnp.float32)
                ).astype(jnp.bfloat16)

    def block_at(at_level, at_cell):
        return (at_level // 2) * plane + at_cell

    cells = (cell, beside, beyond, diagonal)
    blocks = [block_at(at_level, at_cell) for at_level in (level, facing) for at_cell in cells]

    needed = (
        (("pool",),),
        (("x", 0), ("x", 1)),
        (("y", 0), ("y", 1)),
        (("x", 4), ("y", 4)),
        (("mirror", 0), ("mirror", 1)),
        (("x", 2), ("x", 3)),
        (("y", 2), ("y", 3)),
        (("x", 5), ("y", 5)),
    )

    def block_here(order):
        for kind, *rest in needed[order]:
            if kind == "pool":
                own_here(W)
                pool_here(W)
            elif kind == "mirror":
                mirror_here(W, rest[0])
            else:
                flow_here(W, ("x", "y").index(kind), rest[0])

    def share_block(order, which):
        for place in range(tiles):
            once(("core", place), core_copy(place).wait_send)
        block_here(order)
        down_block(order, which)

    tile_steps = {
        "N": lambda place: rms_tile(rows_in, place, 0),
        "V": lambda place: act_tile(place, whole_v, act_v, True),
        "U": lambda place: act_tile(place, whole_u, act_u, False),
        "M": mix_tile,
        "O": out_tile,
        "C": chip_tile,
        "side": lambda place: side_copy(place).start(),
        "S": stream_tile,
        "G": gate_tile,
        "E": value_tile,
    }
    plain_steps = {
        "prep": prepare,
        "tok": lambda: token_copy(0, own_tokens, mate).start(),
        "halftok": near_tokens,
        "fwd": pass_tokens,
        "statA": near_stats.start,
        "statB": sum_stats,
        "statC": far_stats.start,
    }
    block_steps = {
        "DG": lambda order: share_block(order, 0),
        "SG": given_sum,
        "far": send_given,
        "DK": lambda order: share_block(order, 1),
        "SK": kept_sum,
        "END": lambda order: down_end(order, blocks[order]),
    }
    uses = {"V": V, "U": U, "O": O, "G": G, "E": E}

    def run_step(name):
        stem, tail = name[:-2], name[-2:]
        if name in plain_steps:
            plain_steps[name]()
        elif stem in tile_steps and tail[0] in "kg":
            if stem in uses:
                all_here(uses[stem])
            if stem == "N" and tail[0] == "g":
                once("tokens", last_tokens)
            tile_steps[stem]((first if tail[0] == "k" else second) + int(tail[1]))
        elif name[:-1] in block_steps:
            block_steps[name[:-1]](int(name[-1]))
        elif name[:4] == "pool":
            pool_copy(NAMES.index(name[4])).start()
        elif name[:3] == "mir":
            send_mirror(NAMES.index(name[3]), int(name[4]))
        else:
            send_flow(NAMES.index(name[1]), ("x", "y").index(name[0]), int(name[2]))

    for name in ORDER:
        run_step(name)

    for place in range(tiles):
        side_copy(place).wait_send()
    for which in range(6):
        for step in range(6):
            for way in range(2):
                send_on(which, way, step).wait_send()
        for part in range(2):
            reflect(which, part).wait_send()
        pool_copy(which).wait_send()
    for place in range(tiles):
        half_copy(place, own_columns).wait_send()
    for order, block in enumerate(blocks):

        @pl.when(block // half_blocks != core)
        def _():
            near_copy(order, block, given, 0).wait_send()
            near_copy(order, block, kept, 1).wait_send()

        @pl.when(block // half_blocks == core)
        def _():
            far_copy(order, block).wait_send()

    token_copy(0, own_tokens, mate).wait_send()
    token_copy(1, own_tokens, partner).wait_send()
    token_copy(2, token_region(1 - slot, core), partner).wait_send()
    token_copy(3, gain_region(core), partner).wait_send()
    near_stats.wait_send()
    far_stats.wait_send()


def on_ring(
    fs_size,
    tokens,
    norm_gain,
    proj_u,
    proj_v,
    layer_gain,
    layer_shift,
    mix_weight,
    mix_bias,
    proj_out,
    ffn_gain,
    ffn_gate,
    ffn_value,
    conv_gate,
    conv_value,
    proj_down,
):
    own_rows, own_width = tokens.shape
    row_count, full = 2 * own_rows, 2 * own_width
    pairs = fs_size // 2
    quarter, units = proj_u.shape[1] // 2, ffn_gate.shape[1] // 2
    groups = quarter // GROUP_DIM
    tiles = row_count // SEQ_LEN
    bf16, f32 = jnp.bfloat16, jnp.float32
    pack = jnp.stack([norm_gain, ffn_gain, layer_gain, layer_shift]).astype(f32)
    vectors = jnp.concatenate([pack, jnp.zeros_like(pack)], axis=0)
    vmem, hbm = pl.BlockSpec(memory_space=pltpu.VMEM), pl.BlockSpec(memory_space=pl.ANY)
    dma = pltpu.SemaphoreType.DMA
    scratch = [
        pltpu.VMEM((full, quarter), bf16),
        pltpu.VMEM((full, quarter), bf16),
        pltpu.VMEM((pairs, quarter, 2 * proj_out.shape[1]), bf16),
        pltpu.VMEM((full, units), bf16),
        pltpu.VMEM((full, units), bf16),
        pltpu.VMEM((pairs, units, 2 * proj_down.shape[1]), bf16),
        pltpu.VMEM((row_count, full), bf16),
        pltpu.VMEM((row_count, full), bf16),
        pltpu.VMEM((8, full), f32),
        pltpu.VMEM((row_count, quarter), f32),
        pltpu.VMEM((row_count, quarter), f32),
        pltpu.VMEM((row_count, LANES), f32),
        pltpu.VMEM((8, row_count), f32),
        pltpu.VMEM((8, row_count), f32),
        pltpu.VMEM((8, row_count), f32),
        pltpu.VMEM((8, row_count), f32),
        pltpu.VMEM((groups, BLOCK, BLOCK), bf16),
        pltpu.VMEM((groups, BLOCK, LANES), f32),
        pltpu.VMEM((row_count, quarter), bf16),
        pltpu.VMEM((row_count, full), bf16),
        pltpu.VMEM((row_count, own_width), bf16),
        pltpu.VMEM((row_count, own_width), bf16),
        pltpu.VMEM((row_count, own_width), bf16),
        pltpu.VMEM((row_count, full), bf16),
        pltpu.VMEM((row_count, units), bf16),
        pltpu.VMEM((row_count, units), bf16),
        pltpu.VMEM((own_rows, own_width), f32),
        pltpu.VMEM((own_rows, own_width), bf16),
        pltpu.VMEM((row_count, own_width), bf16),
        pltpu.VMEM((own_rows, own_width), bf16),
        dma((8,)),
        dma((6,)),
        dma((6,)),
        dma((84,)),
        dma((84,)),
        dma((4,)),
        dma((4,)),
        dma((2,)),
        dma((2,)),
        dma((tiles,)),
        dma((tiles,)),
        dma((tiles,)),
        dma((tiles,)),
        dma((tiles,)),
        dma((tiles,)),
        dma((2 * pairs,)),
        dma((2 * pairs,)),
        dma((pairs,)),
        dma((pairs,)),
    ]
    return pl.pallas_call(
        functools.partial(layer_kernel, fs_size),
        out_shape=jax.ShapeDtypeStruct((own_rows, own_width), bf16),
        in_specs=[hbm, vmem, vmem, vmem, vmem, vmem] + [hbm] * 6,
        out_specs=vmem,
        scratch_shapes=scratch,
        compiler_params=pltpu.CompilerParams(
            collective_id=0, has_side_effects=True, vmem_limit_bytes=VMEM_BYTES
        ),
        name="layer",
    )(
        tokens,
        vectors,
        mix_weight,
        mix_bias,
        conv_gate,
        conv_value,
        proj_u,
        proj_v,
        proj_out,
        ffn_gate,
        ffn_value,
        proj_down,
    )


def solution(mesh):
    fs_size, tp_size = mesh.shape["fs"], mesh.shape["tp"]
    ringed = tp_size == 2 and fs_size == 16
    in_specs = (
        P("fs", "tp"),
        P("tp"),
        P("fs", "tp"),
        P("fs", "tp"),
        P("tp"),
        P("tp"),
        P("tp", None, None),
        P("tp", None),
        P("tp", "fs"),
        P("tp"),
        P("fs", "tp"),
        P("fs", "tp"),
        P(None, "tp"),
        P(None, "tp"),
        P("tp", "fs"),
    )
    return jax.shard_map(
        functools.partial(on_ring, fs_size) if ringed else on_device,
        mesh=mesh,
        in_specs=in_specs,
        out_specs=P("fs", "tp"),
        check_vma=False,
    )
```

```python
import functools

import jax
import jax.numpy as jnp
from jax import lax
from jax.experimental import pallas as pl
from jax.experimental.pallas import tpu as pltpu
from jax.sharding import PartitionSpec as P

MESH = pl.DeviceIdType.MESH
LANES = 128

GROUP_DIM = 128
BLOCK = 128
SEGMENT = 64
KERNEL = 3
SEQ_LEN = 256


EPS = 1e-06


def matmul(operand, matrix):
    return jnp.dot(operand, matrix, preferred_element_type=jnp.float32)


def local_rms(values_in, gain_row):
    values = values_in.astype(jnp.float32)
    scale_row = lax.rsqrt(jnp.mean(values * values, axis=1, keepdims=True) + EPS)
    return (values * scale_row * gain_row.astype(jnp.float32)).astype(jnp.bfloat16)


def causal_taps(values, weights):
    seq_count = values.shape[0] // SEQ_LEN
    shaped = values.reshape(seq_count, SEQ_LEN, values.shape[1])
    padded = jnp.pad(shaped, ((0, 0), (KERNEL - 1, 0), (0, 0)))
    summed = jnp.zeros(shaped.shape, jnp.float32)
    for tap_index in range(KERNEL):
        summed = summed + padded[:, tap_index : tap_index + SEQ_LEN].astype(jnp.float32) * weights[
            tap_index
        ].astype(jnp.float32)
    return summed.reshape(values.shape[0], values.shape[1])


def on_device(
    tokens,
    norm_gain,
    proj_u,
    proj_v,
    layer_gain,
    layer_shift,
    mix_weight,
    mix_bias,
    proj_out,
    ffn_gain,
    ffn_gate,
    ffn_value,
    conv_gate,
    conv_value,
    proj_down,
):
    own_width = tokens.shape[1]
    whole_tokens, whole_gain, whole_ffn_gain = (
        lax.all_gather(tokens, "tp", axis=1, tiled=True),
        lax.all_gather(norm_gain, "tp", axis=0, tiled=True),
        lax.all_gather(ffn_gain, "tp", axis=0, tiled=True),
    )
    normed = local_rms(whole_tokens, whole_gain)
    row_count = normed.shape[0]
    whole_u, whole_v = (
        lax.all_gather(proj_u, "fs", axis=0, tiled=True),
        lax.all_gather(proj_v, "fs", axis=0, tiled=True),
    )
    pre_u = matmul(normed, whole_u)
    pre_v = matmul(normed, whole_v)
    act_u = jax.nn.gelu(pre_u, approximate=False)
    act_v = jax.nn.gelu(pre_v, approximate=False)
    full_width = act_v.shape[1] * lax.axis_size("tp")
    total_sum, second = lax.psum((jnp.sum(act_v, axis=1), jnp.sum(act_v * act_v, axis=1)), "tp")
    center = total_sum / full_width
    spread = second / full_width - center * center
    mixed_in = (
        (act_v - center[:, None])
        * lax.rsqrt(spread + EPS)[:, None]
        * layer_gain.astype(jnp.float32)
        + layer_shift.astype(jnp.float32)
    ).astype(jnp.bfloat16)
    groups = mixed_in.shape[1] // GROUP_DIM
    blocks = mixed_in.reshape(row_count // BLOCK, BLOCK, groups, GROUP_DIM)
    segment = jnp.arange(BLOCK) // SEGMENT
    visible = segment[None, :] <= segment[:, None]
    masked = jnp.where(visible[None], mix_weight, jnp.zeros_like(mix_weight))
    spatial = (
        jnp.einsum("gij,njgc->nigc", masked, blocks, preferred_element_type=jnp.float32)
        + mix_bias.astype(jnp.float32).T[None, :, :, None]
    )
    gated_rows = (act_u * spatial.reshape(row_count, mixed_in.shape[1])).astype(jnp.bfloat16)
    whole_out = lax.all_gather(proj_out, "fs", axis=1, tiled=True)
    partial_value = matmul(gated_rows, whole_out)
    summed = lax.psum(partial_value.astype(jnp.bfloat16), "tp").astype(jnp.float32)
    stream_rows = (whole_tokens.astype(jnp.float32) + summed).astype(jnp.bfloat16)
    normed_two = local_rms(stream_rows, whole_ffn_gain)
    stream = lax.dynamic_slice_in_dim(stream_rows, lax.axis_index("tp") * own_width, own_width, 1)
    whole_gate, whole_value = (
        lax.all_gather(ffn_gate, "fs", axis=0, tiled=True),
        lax.all_gather(ffn_value, "fs", axis=0, tiled=True),
    )
    pre_gate = matmul(normed_two, whole_gate)
    pre_value = matmul(normed_two, whole_value)
    conv_g = causal_taps(pre_gate.astype(jnp.bfloat16), conv_gate)
    conv_v = causal_taps(pre_value.astype(jnp.bfloat16), conv_value)
    hidden = (jax.nn.silu(conv_g) * conv_v).astype(jnp.bfloat16)
    whole_down = lax.all_gather(proj_down, "fs", axis=1, tiled=True)
    partial_two = matmul(hidden, whole_down)
    return (
        stream.astype(jnp.float32)
        + lax.psum_scatter(
            partial_two.astype(jnp.bfloat16), "tp", scatter_dimension=1, tiled=True
        ).astype(jnp.float32)
    ).astype(jnp.bfloat16)


V, U, O, G, E, W = range(6)
NAMES = ("V", "U", "O", "G", "E", "W")
ORDER = (
    "poolO", "poolU", "poolE", "poolV", "yV0", "poolG", "xV0", "poolW", "xW0", "mirV0", "mirU0",
    "yU0", "xU4", "xO1", "xO0", "yW0", "mirE0", "yO1", "mirO1", "yE1", "mirU1", "prep", "mirO0",
    "xV1", "xV4", "xU1", "mirV1", "yU1", "yO0", "yG0", "yG1", "yV4", "halftok", "xU0", "xG1", "xU2",
    "yV1", "xG4", "yV2", "xE0", "xU3", "yU2", "xV5", "tok", "mirG1", "xV3", "mirW0", "xO3", "xE1",
    "xG0", "Nk0", "yO3", "mirG0", "Nk1", "yV3", "yV5", "yO2", "yU4", "xO4", "yU3", "yU5", "mirE1",
    "yE0", "yE2", "fwd", "xU5", "xV2", "Ng1", "yO5", "xO2", "yO4", "xO5", "Vk0", "yG4", "xG3",
    "Ng0", "Vg1", "xE4", "Vg0", "Vk1", "statA", "Ug1", "statB", "statC", "Uk1", "xG2", "yG2", "Mk1",
    "Ok1", "yG5", "Uk0", "xW2", "yG3", "mirW1", "xE3", "Ck1", "sidek1", "Mg1", "yE3", "Ug0", "xG5",
    "Mg0", "Og1", "Cg1", "xE2", "Mk0", "Ok0", "Ck0", "sidek0", "Sg1", "yE5", "sideg1", "xE5", "Og0",
    "Gg1", "yE4", "yW2", "xW1", "Cg0", "yW1", "Sg0", "Gg0", "Eg0", "sideg0", "xW3", "yW3", "Eg1",
    "DG0", "xW5", "xW4", "DG4", "Sk1", "SG4", "far4", "DG1", "SG1", "SG0", "far0", "Gk1", "yW4",
    "DG2", "Ek1", "DG5", "SG5", "SG2", "yW5", "Sk0", "far5", "far2", "DG6", "Gk0", "Ek0", "DK0",
    "SG6", "far6", "DG3", "DK6", "SG3", "DG7", "far3", "DK2", "SG7", "DK5", "far1", "DK4", "SK5",
    "SK2", "DK3", "far7", "END2", "SK0", "END0", "SK4", "DK7", "END4", "SK3", "END3", "SK6", "END5",
    "DK1", "SK1", "END1", "END6", "SK7", "END7",
)
BY_ROWS = (V, U, G, E)
VMEM_BYTES = 67043328


def gelu(values):
    return 0.5 * values * (1.0 + lax.erf(values * (0.5**0.5)))


def aligned(index, size):
    return pl.multiple_of(index * size, size)


def layer_kernel(
    fs_size,
    tokens,
    norm_gain,
    ffn_gain,
    layer_gain,
    layer_shift,
    mix_weight,
    mix_bias,
    conv_gate,
    conv_value,
    proj_u,
    proj_v,
    proj_out,
    ffn_gate,
    ffn_value,
    proj_down,
    result,
    whole_v,
    whole_u,
    whole_out,
    whole_gate,
    whole_value,
    whole_down,
    rows_in,
    normed,
    gains,
    act_v,
    act_u,
    stat_cols,
    stat_own,
    stat_chip,
    stat_near,
    stat_far,
    masked,
    bias_cols,
    gated,
    partial,
    from_core,
    chip_sum,
    from_side,
    stream,
    pre_gate,
    hidden,
    total,
    given_down,
    near_down,
    far_down,
    finished,
    local_sem,
    pool_send,
    pool_recv,
    flow_send,
    flow_recv,
    token_send,
    token_recv,
    stat_send,
    stat_recv,
    core_send,
    core_recv,
    side_send,
    side_recv,
    half_send,
    half_recv,
    near_send,
    near_recv,
    far_send,
    far_recv,
    out_sem,
):
    pairs = fs_size // 2
    plane = fs_size // 4
    index, core = lax.axis_index("fs"), lax.axis_index("tp")
    level, cell = index // plane, index % plane
    side, column = cell % 2, cell // 2
    low, half = level % 2, level // 2
    slot = (low + half) % 2
    facing = 3 - level
    levels = (level, level + 1 - 2 * low, facing, facing + 1 - 2 * (facing % 2))
    beside, beyond = cell + 1 - 2 * side, cell + 2 - 4 * column
    diagonal = beside + 2 - 4 * column

    partner = (index, 1 - core)
    mate = (levels[1] * plane + cell, core)
    mirror = (facing * plane + cell, core)
    across = (level * plane + beside, core)
    over = (level * plane + beyond, core)

    own_rows, own_width = tokens.shape
    row_count, full = rows_in.shape
    tile = SEQ_LEN
    tiles = row_count // tile
    half_tiles = tiles // 2
    quarter = whole_v.shape[1]
    units = whole_gate.shape[1]
    groups = quarter // GROUP_DIM
    spread_width = 2 * 2 * quarter
    block_width = whole_out.shape[2]
    half_blocks = pairs // 2

    sources = (proj_v, proj_u, proj_out, ffn_gate, ffn_value, proj_down)
    wholes = (whole_v, whole_u, whole_out, whole_gate, whole_value, whole_down)

    def shard(which, part):
        source = sources[which]
        if which in BY_ROWS:
            width = source.shape[1] // 2
            return source.at[:, pl.ds(aligned(part, width), width)]
        height = source.shape[0] // 2
        return source.at[pl.ds(aligned(part, height), height), :]

    def piece(which, at_level, at_cell):
        whole = wholes[which]
        if which in BY_ROWS:
            depth_rows = sources[which].shape[0]
            return whole.at[pl.ds(aligned(at_level * plane + at_cell, depth_rows), depth_rows), :]
        width = sources[which].shape[1]
        block = (at_level // 2) * plane + at_cell
        return whole.at[block, :, pl.ds(aligned(at_level % 2, width), width)]

    def remote(source, target, send, recv, device):
        return pltpu.make_async_remote_copy(
            src_ref=source,
            dst_ref=target,
            send_sem=send,
            recv_sem=recv,
            device_id=device,
            device_id_type=MESH,
        )

    def own_copy(which):
        return pltpu.make_async_copy(
            shard(which, slot), piece(which, level, cell), local_sem.at[which]
        )

    def pool_copy(which):
        return remote(
            shard(which, 1 - slot),
            piece(which, level, cell),
            pool_send.at[which],
            pool_recv.at[which],
            mate,
        )

    def pool_arrived(which):
        here = piece(which, levels[1], cell)
        remote(here, here, pool_send.at[which], pool_recv.at[which], mate).wait_recv()

    def moved(which, here, slot_index, device):
        place = which * 14 + slot_index
        return remote(here, here, flow_send.at[place], flow_recv.at[place], device)

    def send_on(which, way, step):
        if step < 4:
            here = piece(which, levels[step], cell)
        else:
            here = piece(which, levels[2 * (step - 4) + way], (beyond, beside)[way])
        return moved(which, here, way * 6 + step, (across, over)[way])

    def come_in(which, way, step):
        if step < 4:
            here = piece(which, levels[step], (beside, beyond)[way])
        else:
            here = piece(which, levels[2 * (step - 4) + way], diagonal)
        moved(which, here, way * 6 + step, (across, over)[way]).wait_recv()

    def reflect(which, part):
        return moved(which, piece(which, levels[part], cell), 12 + part, mirror)

    def reflected(which, part):
        moved(which, piece(which, levels[2 + part], cell), 12 + part, mirror).wait_recv()

    def token_region(which_side, which_core):
        return rows_in.at[
            pl.ds(aligned(which_side, own_rows), own_rows),
            pl.ds(aligned(which_core, own_width), own_width),
        ]

    def gain_region(which_core):
        return gains.at[:, pl.ds(aligned(which_core, own_width), own_width)]

    def token_copy(which, region, device):
        return remote(region, region, token_send.at[which], token_recv.at[which], device)

    def rows_of(place, height=tile):
        return pl.ds(aligned(place, height), height)

    barrier = pltpu.get_barrier_semaphore()
    for device in (across, over, mate, mirror, partner):
        pl.semaphore_signal(barrier, inc=1, device_id=device, device_id_type=MESH)
    for which in (V, U, O):
        own_copy(which).start()
    tokens_in = pltpu.make_async_copy(tokens, token_region(slot, core), local_sem.at[6])
    tokens_in.start()
    for which in (G, E, W):
        own_copy(which).start()
    for row, vector in enumerate((norm_gain, ffn_gain, layer_gain, layer_shift)):
        values = vector[...].astype(jnp.float32).reshape(1, own_width)
        gains[row : row + 1, pl.ds(aligned(core, own_width), own_width)] = values
    pl.semaphore_wait(barrier, 5)

    own_tokens = token_region(slot, core)
    def arrive_pool(which):
        return lambda: pool_arrived(which)

    def arrive_mirror(which, part):
        return lambda: reflected(which, part)

    def arrive_flow(which, way, step):
        return lambda: come_in(which, way, step)

    done = set()

    def once(name, wait):
        if name not in done:
            done.add(name)
            wait()

    def own_here(which):
        once(("own", which), lambda: own_copy(which).wait())

    def pool_here(which):
        once(("pool", which), arrive_pool(which))

    def mirror_here(which, part):
        once(("mirror", which, part), arrive_mirror(which, part))

    def flow_here(which, way, step):
        once(("flow", which, way, step), arrive_flow(which, way, step))

    def part_here(which, part):
        (own_here, pool_here)[part](which)

    def all_here(which):
        own_here(which)
        pool_here(which)
        for part in range(2):
            mirror_here(which, part)
        for step in range(6):
            for way in range(2):
                flow_here(which, way, step)

    def send_flow(which, way, step):
        if step < 2:
            part_here(which, step)
        elif step < 4:
            mirror_here(which, step - 2)
        else:
            flow_here(which, 1 - way, 2 * (step - 4) + way)
        send_on(which, way, step).start()

    def send_mirror(which, part):
        part_here(which, part)
        reflect(which, part).start()

    tokens_in.wait()
    token_copy(1, own_tokens, partner).start()
    token_copy(3, gain_region(core), partner).start()

    head = slot * groups

    def prepare():
        above = lax.broadcasted_iota(jnp.int32, (BLOCK, BLOCK), 1)
        below = lax.broadcasted_iota(jnp.int32, (BLOCK, BLOCK), 0)
        visible = lax.div(above, SEGMENT) <= lax.div(below, SEGMENT)
        bias_rows = mix_bias[...].astype(jnp.float32)
        for group in range(groups):
            weight = mix_weight[head + group].astype(jnp.float32)
            masked[group] = jnp.where(visible, weight, 0.0).astype(jnp.bfloat16)
            lower = bias_rows[group : group + 1]
            upper = bias_rows[group + groups : group + groups + 1]
            row = jnp.where(slot == 0, lower, upper)
            bias_cols[group] = jnp.broadcast_to(row, (LANES, BLOCK)).T

    first, second = slot * half_tiles, (1 - slot) * half_tiles

    def near_tokens():
        token_copy(1, token_region(slot, 1 - core), partner).wait_recv()
        token_copy(3, gain_region(1 - core), partner).wait_recv()

    def pass_tokens():
        token_copy(0, token_region(1 - slot, core), mate).wait_recv()
        token_copy(2, token_region(1 - slot, core), partner).start()

    def last_tokens():
        token_copy(2, token_region(1 - slot, 1 - core), partner).wait_recv()

    def rms_tile(source, place, gain_index):
        step_rows = 32

        def one(part, carry):
            rows = pl.ds(aligned(place * (tile // step_rows) + part, step_rows), step_rows)
            values = source[rows, :].astype(jnp.float32)
            scale = lax.rsqrt(jnp.mean(values * values, axis=1, keepdims=True) + EPS)
            normed[rows, :] = (values * scale * gains[gain_index : gain_index + 1, :]).astype(
                jnp.bfloat16
            )
            return carry

        lax.fori_loop(0, tile // step_rows, one, 0)

    def product(target, rows, weights, width, finish):
        def one(part, carry):
            columns = pl.ds(aligned(part, width), width)
            value = jnp.dot(
                normed[rows, :], weights[:, columns], preferred_element_type=jnp.float32
            )
            target[rows, columns] = finish(value)
            return carry

        lax.fori_loop(0, weights.shape[1] // width, one, 0)

    lane = lax.broadcasted_iota(jnp.int32, (64, LANES), 1)

    def act_tile(place, weights, target, with_stats):
        rows = rows_of(place)
        product(target, rows, weights, 256, lambda value: value)

        def one(part, carry):
            some = pl.ds(aligned(place * (tile // 64) + part, 64), 64)
            value = gelu(target[some, :])
            target[some, :] = value
            if with_stats:
                sums = jnp.sum(value, axis=1, keepdims=True)
                squares = jnp.sum(value * value, axis=1, keepdims=True)
                stat_cols[some, :] = jnp.where(lane == 0, sums, jnp.where(lane == 1, squares, 0.0))
            return carry

        lax.fori_loop(0, tile // 64, one, 0)
        if with_stats:
            for part in range(tile // LANES):
                some = pl.ds(aligned(place * (tile // LANES) + part, LANES), LANES)
                stat_own[:, some] = stat_cols[some, :].T[0:8, :]

    near_stats = remote(stat_own, stat_near, stat_send.at[0], stat_recv.at[0], partner)
    far_stats = remote(stat_chip, stat_far, stat_send.at[1], stat_recv.at[1], mate)

    def sum_stats():
        near_stats.wait_recv()
        stat_chip[...] = stat_own[...] + stat_near[...]

    def mix_block(block, carry):
        rows = pl.ds(aligned(block, BLOCK), BLOCK)
        sums = stat_chip[0:2, rows] + stat_far[0:2, rows]
        center_row = sums[0:1] / spread_width
        spread_row = sums[1:2] / spread_width - center_row * center_row
        scale_row = lax.rsqrt(spread_row + EPS)
        center = jnp.broadcast_to(center_row, (LANES, BLOCK)).T
        scale = jnp.broadcast_to(scale_row, (LANES, BLOCK)).T
        for group in range(groups):
            columns = slice(group * GROUP_DIM, (group + 1) * GROUP_DIM)
            own = pl.ds(aligned((core * 2 + slot) * groups + group, GROUP_DIM), GROUP_DIM)
            mixed = (
                (act_v[rows, columns] - center) * scale * gains[2:3, own] + gains[3:4, own]
            ).astype(jnp.bfloat16)
            spatial = (
                jnp.dot(masked[group], mixed, preferred_element_type=jnp.float32)
                + bias_cols[group]
            )
            gated[rows, columns] = (act_u[rows, columns] * spatial).astype(jnp.bfloat16)
        return carry

    def mix_tile(place):
        once("stats", far_stats.wait_recv)
        ratio = tile // BLOCK
        lax.fori_loop(place * ratio, (place + 1) * ratio, mix_block, 0)

    own_columns = pl.ds(aligned(core, own_width), own_width)
    other_columns = pl.ds(aligned(1 - core, own_width), own_width)

    def core_copy(place):
        rows = rows_of(place)
        return remote(
            partial.at[rows, other_columns],
            from_core.at[rows, :],
            core_send.at[place],
            core_recv.at[place],
            partner,
        )

    def side_copy(place):
        rows = rows_of(place)
        return remote(
            chip_sum.at[rows, :],
            from_side.at[rows, :],
            side_send.at[place],
            side_recv.at[place],
            mate,
        )

    def half_copy(place, columns):
        region = stream.at[rows_of(place), columns]
        return remote(region, region, half_send.at[place], half_recv.at[place], partner)

    def out_tile(place):
        rows = rows_of(place)

        def one(block, inner):
            columns = pl.ds(aligned(block, block_width), block_width)
            value = jnp.dot(gated[rows, :], whole_out[block], preferred_element_type=jnp.float32)
            partial[rows, columns] = value.astype(jnp.bfloat16)
            return inner

        lax.fori_loop(0, pairs, one, 0)
        core_copy(place).start()

    def chip_tile(place):
        core_copy(place).wait_recv()
        rows = rows_of(place)
        chip_sum[rows, :] = (
            partial[rows, own_columns].astype(jnp.float32)
            + from_core[rows, :].astype(jnp.float32)
        ).astype(jnp.bfloat16)

    strip_width = block_width // 2

    def strips():
        for strip in range(2):
            for place in range(half_blocks):
                ours = pl.ds(
                    aligned(core * 2 * plane + strip * plane + place, strip_width), strip_width
                )
                start = (2 * place + strip) * strip_width
                yield ours, slice(start, start + strip_width)

    def stream_tile(place):
        side_copy(place).wait_recv()
        rows = rows_of(place)
        for ours, summed in strips():
            stream[rows, ours] = (
                rows_in[rows, ours].astype(jnp.float32)
                + chip_sum[rows, summed].astype(jnp.float32)
                + from_side[rows, summed].astype(jnp.float32)
            ).astype(jnp.bfloat16)
        half_copy(place, own_columns).start()

    def to_bfloat(value):
        return value.astype(jnp.bfloat16)

    def gate_tile(place):
        half_copy(place, other_columns).wait_recv()
        rms_tile(stream, place, 1)
        product(pre_gate, rows_of(place), whole_gate, 256, to_bfloat)

    shifted = lax.broadcasted_iota(jnp.int32, (tile, 256), 0)

    def taps(values, weights):
        before = jnp.where(shifted >= 1, pltpu.roll(values, 1, 0), 0.0)
        earlier = jnp.where(shifted >= 2, pltpu.roll(values, 2, 0), 0.0)
        return earlier * weights[0:1] + before * weights[1:2] + values * weights[2:3]

    def value_tile(place):
        rows = rows_of(place)

        def one(part, carry):
            columns = pl.ds(aligned(part, 256), 256)
            own = pl.ds(aligned(slot * (units // 256) + part, 256), 256)
            value = jnp.dot(
                normed[rows, :], whole_value[:, columns], preferred_element_type=jnp.float32
            )
            value = value.astype(jnp.bfloat16).astype(jnp.float32)
            gate = pre_gate[rows, columns].astype(jnp.float32)
            conv_g = taps(gate, conv_gate[:, own].astype(jnp.float32))
            conv_v = taps(value, conv_value[:, own].astype(jnp.float32))
            hidden[rows, columns] = (jax.nn.silu(conv_g) * conv_v).astype(jnp.bfloat16)
            return carry

        lax.fori_loop(0, units // 256, one, 0)

    given, kept = (1 - slot), slot

    def near_copy(order, block, which_side, which):
        rows = rows_of(which_side, own_rows)
        quarter_block = block % half_blocks
        return remote(
            partial.at[rows, pl.ds(aligned(block, block_width), block_width)],
            near_down.at[rows, pl.ds(aligned(quarter_block, block_width), block_width)],
            near_send.at[2 * order + which],
            near_recv.at[2 * order + which],
            partner,
        )

    def far_copy(order, block):
        columns = pl.ds(aligned(block % half_blocks, block_width), block_width)
        return remote(
            given_down.at[:, columns],
            far_down.at[:, columns],
            far_send.at[order],
            far_recv.at[order],
            mate,
        )

    def down_block(order, which):
        block = blocks[order]
        which_side = (given, kept)[which]
        columns = pl.ds(aligned(block, block_width), block_width)

        def one(part, carry):
            rows = rows_of(which_side * half_tiles + part)
            value = jnp.dot(hidden[rows, :], whole_down[block], preferred_element_type=jnp.float32)
            partial[rows, columns] = value.astype(jnp.bfloat16)
            return carry

        lax.fori_loop(0, half_tiles, one, 0)

        @pl.when(block // half_blocks != core)
        def _():
            near_copy(order, block, which_side, which).start()

    def given_sum(order):
        block = blocks[order]
        columns = pl.ds(aligned(block, block_width), block_width)
        quarter_columns = pl.ds(aligned(block % half_blocks, block_width), block_width)

        @pl.when(block // half_blocks == core)
        def _():
            near_copy(order, block, given, 0).wait_recv()
            rows = rows_of(given, own_rows)
            given_down[:, quarter_columns] = (
                partial[rows, columns].astype(jnp.float32)
                + near_down[rows, quarter_columns].astype(jnp.float32)
            ).astype(jnp.bfloat16)

    def send_given(order):
        block = blocks[order]

        @pl.when(block // half_blocks == core)
        def _():
            far_copy(order, block).start()

    def kept_sum(order):
        block = blocks[order]
        columns = pl.ds(aligned(block, block_width), block_width)
        quarter_columns = pl.ds(aligned(block % half_blocks, block_width), block_width)

        @pl.when(block // half_blocks == core)
        def _():
            near_copy(order, block, kept, 1).wait_recv()
            rows = rows_of(kept, own_rows)
            total[:, quarter_columns] = partial[rows, columns].astype(jnp.float32) + near_down[
                rows, quarter_columns
            ].astype(jnp.float32)

    def strip_out(order, strip, block):
        columns = pl.ds(
            aligned(strip * plane + block % half_blocks, block_width // 2), block_width // 2
        )
        return pltpu.make_async_copy(
            finished.at[:, columns], result.at[:, columns], out_sem.at[2 * order + strip]
        )

    def down_end(order, block):
        quarter_columns = pl.ds(aligned(block % half_blocks, block_width), block_width)

        @pl.when(block // half_blocks == core)
        def _():
            far_copy(order, block).wait_recv()
            rows = rows_of(kept, own_rows)
            for strip in range(2):
                place = strip * plane + block % half_blocks
                summed = pl.ds(aligned(2 * (block % half_blocks) + strip, strip_width), strip_width)
                ours = pl.ds(aligned(core * 2 * plane + place, strip_width), strip_width)
                finished[:, pl.ds(aligned(place, strip_width), strip_width)] = (
                    stream[rows, ours].astype(jnp.float32)
                    + total[:, summed]
                    + far_down[:, summed].astype(jnp.float32)
                ).astype(jnp.bfloat16)
                strip_out(order, strip, block).start()

    def block_at(at_level, at_cell):
        return (at_level // 2) * plane + at_cell

    cells = (cell, beside, beyond, diagonal)
    blocks = [block_at(at_level, at_cell) for at_level in (level, facing) for at_cell in cells]

    needed = (
        (("pool",),),
        (("x", 0), ("x", 1)),
        (("y", 0), ("y", 1)),
        (("x", 4), ("y", 4)),
        (("mirror", 0), ("mirror", 1)),
        (("x", 2), ("x", 3)),
        (("y", 2), ("y", 3)),
        (("x", 5), ("y", 5)),
    )

    def block_here(order):
        for kind, *rest in needed[order]:
            if kind == "pool":
                own_here(W)
                pool_here(W)
            elif kind == "mirror":
                mirror_here(W, rest[0])
            else:
                flow_here(W, ("x", "y").index(kind), rest[0])

    def core_sent(place):
        core_copy(place).wait_send()

    def share_block(order, which):
        for place in range(tiles):
            once(("core", place), functools.partial(core_sent, place))
        block_here(order)
        down_block(order, which)

    tile_steps = {
        "N": lambda place: rms_tile(rows_in, place, 0),
        "V": lambda place: act_tile(place, whole_v, act_v, True),
        "U": lambda place: act_tile(place, whole_u, act_u, False),
        "M": mix_tile,
        "O": out_tile,
        "C": chip_tile,
        "side": lambda place: side_copy(place).start(),
        "S": stream_tile,
        "G": gate_tile,
        "E": value_tile,
    }
    plain_steps = {
        "prep": prepare,
        "tok": lambda: token_copy(0, own_tokens, mate).start(),
        "halftok": near_tokens,
        "fwd": pass_tokens,
        "statA": near_stats.start,
        "statB": sum_stats,
        "statC": far_stats.start,
    }
    block_steps = {
        "DG": lambda order: share_block(order, 0),
        "SG": given_sum,
        "far": send_given,
        "DK": lambda order: share_block(order, 1),
        "SK": kept_sum,
        "END": lambda order: down_end(order, blocks[order]),
    }
    uses = {"V": V, "U": U, "O": O, "G": G, "E": E}

    def run_step(name):
        stem, tail = name[:-2], name[-2:]
        if name in plain_steps:
            plain_steps[name]()
        elif stem in tile_steps and tail[0] in "kg":
            if stem in uses:
                all_here(uses[stem])
            if stem == "N" and tail[0] == "g":
                once("tokens", last_tokens)
            tile_steps[stem]((first if tail[0] == "k" else second) + int(tail[1]))
        elif name[:-1] in block_steps:
            block_steps[name[:-1]](int(name[-1]))
        elif name[:4] == "pool":
            pool_copy(NAMES.index(name[4])).start()
        elif name[:3] == "mir":
            send_mirror(NAMES.index(name[3]), int(name[4]))
        else:
            send_flow(NAMES.index(name[1]), ("x", "y").index(name[0]), int(name[2]))

    for name in ORDER:
        run_step(name)

    for place in range(tiles):
        side_copy(place).wait_send()
    for which in range(6):
        for step in range(6):
            for way in range(2):
                send_on(which, way, step).wait_send()
        for part in range(2):
            reflect(which, part).wait_send()
        pool_copy(which).wait_send()
    for place in range(tiles):
        half_copy(place, own_columns).wait_send()
    for order, block in enumerate(blocks):

        @pl.when(block // half_blocks != core)
        def _():
            near_copy(order, block, given, 0).wait_send()
            near_copy(order, block, kept, 1).wait_send()

        @pl.when(block // half_blocks == core)
        def _():
            far_copy(order, block).wait_send()
            for strip in range(2):
                strip_out(order, strip, block).wait()

    token_copy(0, own_tokens, mate).wait_send()
    token_copy(1, own_tokens, partner).wait_send()
    token_copy(2, token_region(1 - slot, core), partner).wait_send()
    token_copy(3, gain_region(core), partner).wait_send()
    near_stats.wait_send()
    far_stats.wait_send()


def on_ring(
    fs_size,
    tokens,
    norm_gain,
    proj_u,
    proj_v,
    layer_gain,
    layer_shift,
    mix_weight,
    mix_bias,
    proj_out,
    ffn_gain,
    ffn_gate,
    ffn_value,
    conv_gate,
    conv_value,
    proj_down,
):
    own_rows, own_width = tokens.shape
    row_count, full = 2 * own_rows, 2 * own_width
    pairs = fs_size // 2
    quarter, units = proj_u.shape[1] // 2, ffn_gate.shape[1] // 2
    groups = quarter // GROUP_DIM
    tiles = row_count // SEQ_LEN
    bf16, f32 = jnp.bfloat16, jnp.float32
    vmem, hbm = pl.BlockSpec(memory_space=pltpu.VMEM), pl.BlockSpec(memory_space=pl.ANY)
    dma = pltpu.SemaphoreType.DMA
    scratch = [
        pltpu.VMEM((full, quarter), bf16),
        pltpu.VMEM((full, quarter), bf16),
        pltpu.VMEM((pairs, quarter, 2 * proj_out.shape[1]), bf16),
        pltpu.VMEM((full, units), bf16),
        pltpu.VMEM((full, units), bf16),
        pltpu.VMEM((pairs, units, 2 * proj_down.shape[1]), bf16),
        pltpu.VMEM((row_count, full), bf16),
        pltpu.VMEM((row_count, full), bf16),
        pltpu.VMEM((8, full), f32),
        pltpu.VMEM((row_count, quarter), f32),
        pltpu.VMEM((row_count, quarter), f32),
        pltpu.VMEM((row_count, LANES), f32),
        pltpu.VMEM((8, row_count), f32),
        pltpu.VMEM((8, row_count), f32),
        pltpu.VMEM((8, row_count), f32),
        pltpu.VMEM((8, row_count), f32),
        pltpu.VMEM((groups, BLOCK, BLOCK), bf16),
        pltpu.VMEM((groups, BLOCK, LANES), f32),
        pltpu.VMEM((row_count, quarter), bf16),
        pltpu.VMEM((row_count, full), bf16),
        pltpu.VMEM((row_count, own_width), bf16),
        pltpu.VMEM((row_count, own_width), bf16),
        pltpu.VMEM((row_count, own_width), bf16),
        pltpu.VMEM((row_count, full), bf16),
        pltpu.VMEM((row_count, units), bf16),
        pltpu.VMEM((row_count, units), bf16),
        pltpu.VMEM((own_rows, own_width), f32),
        pltpu.VMEM((own_rows, own_width), bf16),
        pltpu.VMEM((row_count, own_width), bf16),
        pltpu.VMEM((own_rows, own_width), bf16),
        pltpu.VMEM((own_rows, own_width), bf16),
        dma((8,)),
        dma((6,)),
        dma((6,)),
        dma((84,)),
        dma((84,)),
        dma((4,)),
        dma((4,)),
        dma((2,)),
        dma((2,)),
        dma((tiles,)),
        dma((tiles,)),
        dma((tiles,)),
        dma((tiles,)),
        dma((tiles,)),
        dma((tiles,)),
        dma((2 * pairs,)),
        dma((2 * pairs,)),
        dma((pairs,)),
        dma((pairs,)),
        dma((2 * pairs,)),
    ]
    return pl.pallas_call(
        functools.partial(layer_kernel, fs_size),
        out_shape=jax.ShapeDtypeStruct((own_rows, own_width), bf16),
        in_specs=[hbm] + [vmem] * 8 + [hbm] * 6,
        out_specs=hbm,
        scratch_shapes=scratch,
        compiler_params=pltpu.CompilerParams(
            collective_id=0, has_side_effects=True, vmem_limit_bytes=VMEM_BYTES
        ),
        name="layer",
    )(
        tokens,
        norm_gain,
        ffn_gain,
        layer_gain,
        layer_shift,
        mix_weight,
        mix_bias,
        conv_gate,
        conv_value,
        proj_u,
        proj_v,
        proj_out,
        ffn_gate,
        ffn_value,
        proj_down,
    )


def solution(mesh):
    fs_size, tp_size = mesh.shape["fs"], mesh.shape["tp"]
    ringed = tp_size == 2 and fs_size == 16
    in_specs = (
        P("fs", "tp"),
        P("tp"),
        P("fs", "tp"),
        P("fs", "tp"),
        P("tp"),
        P("tp"),
        P("tp", None, None),
        P("tp", None),
        P("tp", "fs"),
        P("tp"),
        P("fs", "tp"),
        P("fs", "tp"),
        P(None, "tp"),
        P(None, "tp"),
        P("tp", "fs"),
    )
    return jax.shard_map(
        functools.partial(on_ring, fs_size) if ringed else on_device,
        mesh=mesh,
        in_specs=in_specs,
        out_specs=P("fs", "tp"),
        check_vma=False,
    )
```

```python
import functools

import jax
import jax.numpy as jnp
from jax import lax
from jax.experimental import pallas as pl
from jax.experimental.pallas import tpu as pltpu
from jax.sharding import PartitionSpec as P

MESH = pl.DeviceIdType.MESH
LANES = 128

GROUP_DIM = 128
BLOCK = 128
SEGMENT = 64
KERNEL = 3
SEQ_LEN = 256


EPS = 1e-06


def matmul(operand, matrix):
    return jnp.dot(operand, matrix, preferred_element_type=jnp.float32)


def local_rms(values_in, gain_row):
    values = values_in.astype(jnp.float32)
    scale_row = lax.rsqrt(jnp.mean(values * values, axis=1, keepdims=True) + EPS)
    return (values * scale_row * gain_row.astype(jnp.float32)).astype(jnp.bfloat16)


def causal_taps(values, weights):
    seq_count = values.shape[0] // SEQ_LEN
    shaped = values.reshape(seq_count, SEQ_LEN, values.shape[1])
    padded = jnp.pad(shaped, ((0, 0), (KERNEL - 1, 0), (0, 0)))
    summed = jnp.zeros(shaped.shape, jnp.float32)
    for tap_index in range(KERNEL):
        summed = summed + padded[:, tap_index : tap_index + SEQ_LEN].astype(jnp.float32) * weights[
            tap_index
        ].astype(jnp.float32)
    return summed.reshape(values.shape[0], values.shape[1])


def on_device(
    tokens,
    norm_gain,
    proj_u,
    proj_v,
    layer_gain,
    layer_shift,
    mix_weight,
    mix_bias,
    proj_out,
    ffn_gain,
    ffn_gate,
    ffn_value,
    conv_gate,
    conv_value,
    proj_down,
):
    own_width = tokens.shape[1]
    whole_tokens, whole_gain, whole_ffn_gain = (
        lax.all_gather(tokens, "tp", axis=1, tiled=True),
        lax.all_gather(norm_gain, "tp", axis=0, tiled=True),
        lax.all_gather(ffn_gain, "tp", axis=0, tiled=True),
    )
    normed = local_rms(whole_tokens, whole_gain)
    row_count = normed.shape[0]
    whole_u, whole_v = (
        lax.all_gather(proj_u, "fs", axis=0, tiled=True),
        lax.all_gather(proj_v, "fs", axis=0, tiled=True),
    )
    pre_u = matmul(normed, whole_u)
    pre_v = matmul(normed, whole_v)
    act_u = jax.nn.gelu(pre_u, approximate=False)
    act_v = jax.nn.gelu(pre_v, approximate=False)
    full_width = act_v.shape[1] * lax.axis_size("tp")
    total_sum, second = lax.psum((jnp.sum(act_v, axis=1), jnp.sum(act_v * act_v, axis=1)), "tp")
    center = total_sum / full_width
    spread = second / full_width - center * center
    mixed_in = (
        (act_v - center[:, None])
        * lax.rsqrt(spread + EPS)[:, None]
        * layer_gain.astype(jnp.float32)
        + layer_shift.astype(jnp.float32)
    ).astype(jnp.bfloat16)
    groups = mixed_in.shape[1] // GROUP_DIM
    blocks = mixed_in.reshape(row_count // BLOCK, BLOCK, groups, GROUP_DIM)
    segment = jnp.arange(BLOCK) // SEGMENT
    visible = segment[None, :] <= segment[:, None]
    masked = jnp.where(visible[None], mix_weight, jnp.zeros_like(mix_weight))
    spatial = (
        jnp.einsum("gij,njgc->nigc", masked, blocks, preferred_element_type=jnp.float32)
        + mix_bias.astype(jnp.float32).T[None, :, :, None]
    )
    gated_rows = (act_u * spatial.reshape(row_count, mixed_in.shape[1])).astype(jnp.bfloat16)
    whole_out = lax.all_gather(proj_out, "fs", axis=1, tiled=True)
    partial_value = matmul(gated_rows, whole_out)
    summed = lax.psum(partial_value.astype(jnp.bfloat16), "tp").astype(jnp.float32)
    stream_rows = (whole_tokens.astype(jnp.float32) + summed).astype(jnp.bfloat16)
    normed_two = local_rms(stream_rows, whole_ffn_gain)
    stream = lax.dynamic_slice_in_dim(stream_rows, lax.axis_index("tp") * own_width, own_width, 1)
    whole_gate, whole_value = (
        lax.all_gather(ffn_gate, "fs", axis=0, tiled=True),
        lax.all_gather(ffn_value, "fs", axis=0, tiled=True),
    )
    pre_gate = matmul(normed_two, whole_gate)
    pre_value = matmul(normed_two, whole_value)
    conv_g = causal_taps(pre_gate.astype(jnp.bfloat16), conv_gate)
    conv_v = causal_taps(pre_value.astype(jnp.bfloat16), conv_value)
    hidden = (jax.nn.silu(conv_g) * conv_v).astype(jnp.bfloat16)
    whole_down = lax.all_gather(proj_down, "fs", axis=1, tiled=True)
    partial_two = matmul(hidden, whole_down)
    return (
        stream.astype(jnp.float32)
        + lax.psum_scatter(
            partial_two.astype(jnp.bfloat16), "tp", scatter_dimension=1, tiled=True
        ).astype(jnp.float32)
    ).astype(jnp.bfloat16)


V, U, O, G, E, W = range(6)
NAMES = ("V", "U", "O", "G", "E", "W")
ORDER = (
    "yV0", "xG0", "xO0", "yE0", "yG0", "yW0", "poolU", "mirU0", "mirU1", "xU1", "poolV", "xE4",
    "mirV1", "xV0", "mirV0", "crsV", "poolG", "xV1", "crsU", "crsO", "yU2", "halftok", "poolO",
    "mirO0", "xU2", "yU0", "yO0", "yV3", "yU4", "xV3", "prep", "Nk0", "crsG", "yV1", "mirO1", "xV4",
    "xV2", "yU1", "mirE0", "xO4", "xU5", "Nk1", "yV5", "yU3", "yV2", "xU3", "xG1", "poolE", "mirE1",
    "tok", "poolW", "xU0", "yO1", "yG4", "xV5", "xO3", "mirG0", "xU4", "xO1", "yV4", "yO2", "mirG1",
    "xG4", "yU5", "xE1", "yG1", "fwd", "Vk1", "xO2", "yO3", "Ng1", "crsE", "Ug1", "yO5", "xE2",
    "Uk0", "Uk1", "Vg1", "Vk0", "xO5", "Ng0", "yO4", "Vg0", "statA", "statB", "statC", "xG2", "yE4",
    "Mk0", "yG2", "crsW", "yE1", "xG3", "mirW0", "Ug0", "Mg0", "Mk1", "Ok1", "Ck1", "sidek1", "xE0",
    "Og0", "yG3", "Cg0", "sideg0", "yE3", "yG5", "Mg1", "Og1", "yE2", "xG5", "xW1", "Cg1", "Ok0",
    "xE3", "yE5", "Ck0", "Sg1", "sidek0", "yW1", "xW0", "xE5", "Sk0", "Gk0", "yW4", "yW2", "mirW1",
    "Gg1", "xW4", "sideg1", "Sg0", "xW2", "Gg0", "Eg0", "Eg1", "DG2", "DG1", "DG0", "SG0", "SG2",
    "far0", "Sk1", "xW3", "DG3", "SG1", "far1", "xW5", "DG4", "far2", "yW3", "Gk1", "yW5", "SG4",
    "far4", "SG3", "far3", "Ek0", "Ek1", "DK2", "DK1", "DG6", "DG5", "SG6", "far6", "DK0", "SK1",
    "DG7", "SG5", "far5", "DK4", "DK3", "SK2", "END1", "SG7", "far7", "DK5", "SK3", "END3", "DK7",
    "DK6", "SK0", "END0", "SK5", "END5", "SK4", "END4", "END2", "SK6", "END6", "SK7", "END7",
)
BY_ROWS = (V, U, G, E)
VMEM_BYTES = 67043328


def gelu(values):
    return 0.5 * values * (1.0 + lax.erf(values * (0.5**0.5)))


def aligned(index, size):
    return index * size if isinstance(index, int) else pl.multiple_of(index * size, size)


def unit_shares(total):
    outer = (3 * total // 8) // 256 * 256
    return outer, total - outer


def run_layer(
    fs_size,
    inner,
    tokens,
    norm_gain,
    ffn_gain,
    layer_gain,
    layer_shift,
    mix_weight,
    mix_bias,
    conv_gate,
    conv_value,
    proj_u,
    proj_v,
    proj_out,
    ffn_gate,
    ffn_value,
    proj_down,
    result,
    whole_v,
    whole_u,
    whole_out,
    whole_gate,
    whole_value,
    whole_down,
    rows_in,
    normed,
    gains,
    act_v,
    act_u,
    stat_cols,
    stat_own,
    stat_chip,
    stat_near,
    stat_far,
    masked,
    bias_cols,
    gated,
    partial,
    from_core,
    chip_sum,
    from_side,
    stream,
    pre_gate,
    total,
    given_down,
    near_down,
    far_down,
    finished,
    local_sem,
    pool_send,
    pool_recv,
    flow_send,
    flow_recv,
    token_send,
    token_recv,
    stat_send,
    stat_recv,
    core_send,
    core_recv,
    side_send,
    side_recv,
    half_send,
    half_recv,
    near_send,
    near_recv,
    far_send,
    far_recv,
    out_sem,
    cross_send,
):
    pairs = fs_size // 2
    plane = fs_size // 4
    index, core = lax.axis_index("fs"), lax.axis_index("tp")
    level, cell = index // plane, index % plane
    side, column = cell % 2, cell // 2
    low, half = level % 2, level // 2
    slot = int(inner)
    facing = 3 - level
    levels = (level, level + 1 - 2 * low, facing, facing + 1 - 2 * (facing % 2))
    beside, beyond = cell + 1 - 2 * side, cell + 2 - 4 * column
    diagonal = beside + 2 - 4 * column

    partner = (index, 1 - core)
    mate = (levels[1] * plane + cell, core)
    mirror = (facing * plane + cell, core)
    across = (level * plane + beside, core)
    over = (level * plane + beyond, core)
    crossed = (levels[3] * plane + cell, core)

    barrier = pltpu.get_barrier_semaphore()
    for device in (across, over, mate, mirror, crossed, partner):
        pl.semaphore_signal(barrier, inc=1, device_id=device, device_id_type=MESH)
    own_rows, own_width = tokens.shape
    row_count, full = rows_in.shape
    tile = SEQ_LEN
    tiles = row_count // tile
    half_tiles = tiles // 2
    quarter = whole_v.shape[1]
    shares = unit_shares(ffn_gate.shape[1])
    starts = (0, shares[0])
    units = shares[slot]
    relieved = (G, E, W) if inner else ()
    groups = quarter // GROUP_DIM
    spread_width = 2 * 2 * quarter
    block_width = whole_out.shape[2]
    half_blocks = pairs // 2

    sources = (proj_v, proj_u, proj_out, ffn_gate, ffn_value, proj_down)
    wholes = (whole_v, whole_u, whole_out, whole_gate, whole_value, whole_down)

    def shard(which, part):
        source = sources[which]
        if which in (G, E):
            return source.at[:, pl.ds(starts[part], shares[part])]
        if which == W:
            return source.at[pl.ds(starts[part], shares[part]), :]
        if which in BY_ROWS:
            width = source.shape[1] // 2
            return source.at[:, pl.ds(part * width, width)]
        height = source.shape[0] // 2
        return source.at[pl.ds(part * height, height), :]

    def piece(which, at_level, at_cell, part=slot):
        whole = wholes[which]
        if which in BY_ROWS:
            width = shares[part] if which in (G, E) else whole.shape[1]
            depth_rows = sources[which].shape[0]
            place = aligned(at_level * plane + at_cell, depth_rows)
            return whole.at[pl.ds(place, depth_rows), pl.ds(0, width)]
        height = shares[part] if which == W else whole.shape[1]
        width = sources[which].shape[1]
        block = (at_level // 2) * plane + at_cell
        return whole.at[block, pl.ds(0, height), pl.ds(aligned(at_level % 2, width), width)]

    def remote(source, target, send, recv, device):
        return pltpu.make_async_remote_copy(
            src_ref=source,
            dst_ref=target,
            send_sem=send,
            recv_sem=recv,
            device_id=device,
            device_id_type=MESH,
        )

    def own_copy(which):
        return pltpu.make_async_copy(
            shard(which, slot), piece(which, level, cell), local_sem.at[which]
        )

    def pool_copy(which):
        return remote(
            shard(which, 1 - slot),
            piece(which, level, cell, 1 - slot),
            pool_send.at[which],
            pool_recv.at[which],
            mate,
        )

    def pool_arrived(which):
        here = piece(which, levels[1], cell)
        remote(here, here, pool_send.at[which], pool_recv.at[which], mate).wait_recv()

    def moved(which, here, slot_index, device):
        place = which * 14 + slot_index
        return remote(here, here, flow_send.at[place], flow_recv.at[place], device)

    def send_on(which, way, step):
        device = (across, over)[way]
        if step < 4:
            here = piece(which, levels[step], cell)
        elif step == 5 and which in relieved:
            here, device = piece(which, levels[way], diagonal), mirror
        else:
            here = piece(which, levels[2 * (step - 4) + way], (beyond, beside)[way])
        return moved(which, here, way * 6 + step, device)

    def come_in(which, way, step):
        device = (across, over)[way]
        if step < 4:
            here = piece(which, levels[step], (beside, beyond)[way])
        else:
            here = piece(which, levels[2 * (step - 4) + way], diagonal)
        if step == 5 and which in relieved:
            device = mirror
        moved(which, here, way * 6 + step, device).wait_recv()

    def reflect(which, part):
        return moved(which, piece(which, levels[part], cell), 12 + part, mirror)

    def reflected(which, part):
        moved(which, piece(which, levels[2 + part], cell), 12 + part, mirror).wait_recv()

    def token_region(which_side, which_core):
        return rows_in.at[
            pl.ds(aligned(which_side, own_rows), own_rows),
            pl.ds(aligned(which_core, own_width), own_width),
        ]

    def gain_region(which_core):
        return gains.at[:, pl.ds(aligned(which_core, own_width), own_width)]

    def token_copy(which, region, device):
        return remote(region, region, token_send.at[which], token_recv.at[which], device)

    def rows_of(place, height=tile):
        return pl.ds(aligned(place, height), height)

    for which in (V, U, O):
        own_copy(which).start()
    tokens_in = pltpu.make_async_copy(tokens, token_region(slot, core), local_sem.at[6])
    tokens_in.start()
    for which in (G, E, W):
        own_copy(which).start()
    for row, vector in enumerate((norm_gain, ffn_gain, layer_gain, layer_shift)):
        values = vector[...].astype(jnp.float32).reshape(1, own_width)
        gains[row : row + 1, pl.ds(aligned(core, own_width), own_width)] = values
    pl.semaphore_wait(pltpu.get_barrier_semaphore(), 6)

    own_tokens = token_region(slot, core)
    def arrive_pool(which):
        return lambda: pool_arrived(which)

    def arrive_mirror(which, part):
        return lambda: reflected(which, part)

    def arrive_flow(which, way, step):
        return lambda: come_in(which, way, step)

    done = set()

    def once(name, wait):
        if name not in done:
            done.add(name)
            wait()

    def own_here(which):
        once(("own", which), lambda: own_copy(which).wait())

    def pool_here(which):
        once(("pool", which), arrive_pool(which))

    def mirror_here(which, part):
        once(("mirror", which, part), arrive_mirror(which, part))

    def flow_here(which, way, step):
        once(("flow", which, way, step), arrive_flow(which, way, step))

    def part_here(which, part):
        (own_here, pool_here)[part](which)

    def all_here(which):
        own_here(which)
        pool_here(which)
        for part in range(2):
            mirror_here(which, part)
        for step in range(6):
            for way in range(2):
                flow_here(which, way, step)

    def send_flow(which, way, step):
        if step < 2:
            part_here(which, step)
        elif step < 4:
            mirror_here(which, step - 2)
        else:
            if step == 5 and which in relieved:
                flow_here(which, way, 4)
            else:
                flow_here(which, 1 - way, 2 * (step - 4) + way)
        send_on(which, way, step).start()

    def cross_copy(which):
        return remote(
            shard(which, 1 - slot),
            piece(which, level, cell, 1 - slot),
            cross_send.at[which],
            flow_recv.at[which * 14 + 13],
            crossed,
        )

    def send_mirror(which, part):
        if part == 0 or inner:
            part_here(which, part)
            reflect(which, part).start()

    def send_cross(which):
        if inner:
            cross_copy(which).start()

    tokens_in.wait()
    token_copy(1, own_tokens, partner).start()
    token_copy(3, gain_region(core), partner).start()

    head = slot * groups

    def prepare():
        above = lax.broadcasted_iota(jnp.int32, (BLOCK, BLOCK), 1)
        below = lax.broadcasted_iota(jnp.int32, (BLOCK, BLOCK), 0)
        visible = lax.div(above, SEGMENT) <= lax.div(below, SEGMENT)
        bias_rows = mix_bias[...].astype(jnp.float32)
        for group in range(groups):
            weight = mix_weight[head + group].astype(jnp.float32)
            masked[group] = jnp.where(visible, weight, 0.0).astype(jnp.bfloat16)
            lower = bias_rows[group : group + 1]
            upper = bias_rows[group + groups : group + groups + 1]
            row = upper if inner else lower
            bias_cols[group] = jnp.broadcast_to(row, (LANES, BLOCK)).T

    first, second = slot * half_tiles, (1 - slot) * half_tiles

    def near_tokens():
        token_copy(1, token_region(slot, 1 - core), partner).wait_recv()
        token_copy(3, gain_region(1 - core), partner).wait_recv()

    def pass_tokens():
        token_copy(0, token_region(1 - slot, core), mate).wait_recv()
        token_copy(2, token_region(1 - slot, core), partner).start()

    def last_tokens():
        token_copy(2, token_region(1 - slot, 1 - core), partner).wait_recv()

    def rms_tile(source, place, gain_index):
        step_rows = 32

        def one(part, carry):
            rows = pl.ds(aligned(place * (tile // step_rows) + part, step_rows), step_rows)
            values = source[rows, :].astype(jnp.float32)
            scale = lax.rsqrt(jnp.mean(values * values, axis=1, keepdims=True) + EPS)
            normed[rows, :] = (values * scale * gains[gain_index : gain_index + 1, :]).astype(
                jnp.bfloat16
            )
            return carry

        lax.fori_loop(0, tile // step_rows, one, 0)

    def product(target, rows, weights, width, count, finish):
        def one(part, carry):
            columns = pl.ds(aligned(part, width), width)
            value = jnp.dot(
                normed[rows, :], weights[:, columns], preferred_element_type=jnp.float32
            )
            target[rows, columns] = finish(value)
            return carry

        lax.fori_loop(0, count, one, 0)

    lane = lax.broadcasted_iota(jnp.int32, (64, LANES), 1)

    def act_tile(place, weights, target, with_stats):
        rows = rows_of(place)
        product(target, rows, weights, 256, quarter // 256, lambda value: value)

        def one(part, carry):
            some = pl.ds(aligned(place * (tile // 64) + part, 64), 64)
            value = gelu(target[some, :])
            target[some, :] = value
            if with_stats:
                sums = jnp.sum(value, axis=1, keepdims=True)
                squares = jnp.sum(value * value, axis=1, keepdims=True)
                stat_cols[some, :] = jnp.where(lane == 0, sums, jnp.where(lane == 1, squares, 0.0))
            return carry

        lax.fori_loop(0, tile // 64, one, 0)
        if with_stats:
            for part in range(tile // LANES):
                some = pl.ds(aligned(place * (tile // LANES) + part, LANES), LANES)
                stat_own[:, some] = stat_cols[some, :].T[0:8, :]

    near_stats = remote(stat_own, stat_near, stat_send.at[0], stat_recv.at[0], partner)
    far_stats = remote(stat_chip, stat_far, stat_send.at[1], stat_recv.at[1], mate)

    def sum_stats():
        near_stats.wait_recv()
        stat_chip[...] = stat_own[...] + stat_near[...]

    def mix_block(block, carry):
        rows = pl.ds(aligned(block, BLOCK), BLOCK)
        sums = stat_chip[0:2, rows] + stat_far[0:2, rows]
        center_row = sums[0:1] / spread_width
        spread_row = sums[1:2] / spread_width - center_row * center_row
        scale_row = lax.rsqrt(spread_row + EPS)
        center = jnp.broadcast_to(center_row, (LANES, BLOCK)).T
        scale = jnp.broadcast_to(scale_row, (LANES, BLOCK)).T
        for group in range(groups):
            columns = slice(group * GROUP_DIM, (group + 1) * GROUP_DIM)
            own = pl.ds(aligned((core * 2 + slot) * groups + group, GROUP_DIM), GROUP_DIM)
            mixed = (
                (act_v[rows, columns] - center) * scale * gains[2:3, own] + gains[3:4, own]
            ).astype(jnp.bfloat16)
            spatial = (
                jnp.dot(masked[group], mixed, preferred_element_type=jnp.float32)
                + bias_cols[group]
            )
            gated[rows, columns] = (act_u[rows, columns] * spatial).astype(jnp.bfloat16)
        return carry

    def mix_tile(place):
        once("stats", far_stats.wait_recv)
        ratio = tile // BLOCK
        lax.fori_loop(place * ratio, (place + 1) * ratio, mix_block, 0)

    own_columns = pl.ds(aligned(core, own_width), own_width)
    other_columns = pl.ds(aligned(1 - core, own_width), own_width)

    def core_copy(place):
        rows = rows_of(place)
        return remote(
            partial.at[rows, other_columns],
            from_core.at[rows, :],
            core_send.at[place],
            core_recv.at[place],
            partner,
        )

    def side_copy(place):
        rows = rows_of(place)
        return remote(
            chip_sum.at[rows, :],
            from_side.at[rows, :],
            side_send.at[place],
            side_recv.at[place],
            mate,
        )

    def half_copy(place, columns):
        region = stream.at[rows_of(place), columns]
        return remote(region, region, half_send.at[place], half_recv.at[place], partner)

    def out_tile(place):
        rows = rows_of(place)

        def one(block, inner):
            columns = pl.ds(aligned(block, block_width), block_width)
            value = jnp.dot(gated[rows, :], whole_out[block], preferred_element_type=jnp.float32)
            partial[rows, columns] = value.astype(jnp.bfloat16)
            return inner

        lax.fori_loop(0, pairs, one, 0)
        core_copy(place).start()

    def chip_tile(place):
        core_copy(place).wait_recv()
        rows = rows_of(place)
        chip_sum[rows, :] = (
            partial[rows, own_columns].astype(jnp.float32)
            + from_core[rows, :].astype(jnp.float32)
        ).astype(jnp.bfloat16)

    strip_width = block_width // 2

    def strips():
        for strip in range(2):
            for place in range(half_blocks):
                ours = pl.ds(
                    aligned(core * 2 * plane + strip * plane + place, strip_width), strip_width
                )
                start = (2 * place + strip) * strip_width
                yield ours, slice(start, start + strip_width)

    def stream_tile(place):
        side_copy(place).wait_recv()
        rows = rows_of(place)
        for ours, summed in strips():
            stream[rows, ours] = (
                rows_in[rows, ours].astype(jnp.float32)
                + chip_sum[rows, summed].astype(jnp.float32)
                + from_side[rows, summed].astype(jnp.float32)
            ).astype(jnp.bfloat16)
        half_copy(place, own_columns).start()

    def to_bfloat(value):
        return value.astype(jnp.bfloat16)

    def gate_tile(place):
        half_copy(place, other_columns).wait_recv()
        rms_tile(stream, place, 1)
        product(pre_gate, rows_of(place), whole_gate, 256, units // 256, to_bfloat)

    shifted = lax.broadcasted_iota(jnp.int32, (tile, 256), 0)

    def taps(values, weights):
        before = jnp.where(shifted >= 1, pltpu.roll(values, 1, 0), 0.0)
        earlier = jnp.where(shifted >= 2, pltpu.roll(values, 2, 0), 0.0)
        return earlier * weights[0:1] + before * weights[1:2] + values * weights[2:3]

    def value_tile(place):
        rows = rows_of(place)

        def one(part, carry):
            columns = pl.ds(aligned(part, 256), 256)
            own = pl.ds(aligned(starts[slot] // 256 + part, 256), 256)
            value = jnp.dot(
                normed[rows, :], whole_value[:, columns], preferred_element_type=jnp.float32
            )
            value = value.astype(jnp.bfloat16).astype(jnp.float32)
            gate = pre_gate[rows, columns].astype(jnp.float32)
            conv_g = taps(gate, conv_gate[:, own].astype(jnp.float32))
            conv_v = taps(value, conv_value[:, own].astype(jnp.float32))
            pre_gate[rows, columns] = (jax.nn.silu(conv_g) * conv_v).astype(jnp.bfloat16)
            return carry

        lax.fori_loop(0, units // 256, one, 0)

    given, kept = (1 - slot), slot

    def near_copy(order, block, which_side, which):
        rows = rows_of(which_side, own_rows)
        quarter_block = block % half_blocks
        return remote(
            partial.at[rows, pl.ds(aligned(block, block_width), block_width)],
            near_down.at[rows, pl.ds(aligned(quarter_block, block_width), block_width)],
            near_send.at[2 * order + which],
            near_recv.at[2 * order + which],
            partner,
        )

    def far_copy(order, block):
        columns = pl.ds(aligned(block % half_blocks, block_width), block_width)
        return remote(
            given_down.at[:, columns],
            far_down.at[:, columns],
            far_send.at[order],
            far_recv.at[order],
            mate,
        )

    def down_block(order, which):
        block = blocks[order]
        which_side = (given, kept)[which]
        columns = pl.ds(aligned(block, block_width), block_width)

        def one(part, carry):
            rows = rows_of(which_side * half_tiles + part)
            value = jnp.dot(
                pre_gate[rows, pl.ds(0, units)],
                whole_down[block, pl.ds(0, units), :],
                preferred_element_type=jnp.float32,
            )
            partial[rows, columns] = value.astype(jnp.bfloat16)
            return carry

        lax.fori_loop(0, half_tiles, one, 0)

        @pl.when(block // half_blocks != core)
        def _():
            near_copy(order, block, which_side, which).start()

    def given_sum(order):
        block = blocks[order]
        columns = pl.ds(aligned(block, block_width), block_width)
        quarter_columns = pl.ds(aligned(block % half_blocks, block_width), block_width)

        @pl.when(block // half_blocks == core)
        def _():
            near_copy(order, block, given, 0).wait_recv()
            rows = rows_of(given, own_rows)
            given_down[:, quarter_columns] = (
                partial[rows, columns].astype(jnp.float32)
                + near_down[rows, quarter_columns].astype(jnp.float32)
            ).astype(jnp.bfloat16)

    def send_given(order):
        block = blocks[order]

        @pl.when(block // half_blocks == core)
        def _():
            far_copy(order, block).start()

    def kept_sum(order):
        block = blocks[order]
        columns = pl.ds(aligned(block, block_width), block_width)
        quarter_columns = pl.ds(aligned(block % half_blocks, block_width), block_width)

        @pl.when(block // half_blocks == core)
        def _():
            near_copy(order, block, kept, 1).wait_recv()
            rows = rows_of(kept, own_rows)
            total[:, quarter_columns] = partial[rows, columns].astype(jnp.float32) + near_down[
                rows, quarter_columns
            ].astype(jnp.float32)

    def strip_out(order, strip, block):
        columns = pl.ds(
            aligned(strip * plane + block % half_blocks, block_width // 2), block_width // 2
        )
        return pltpu.make_async_copy(
            finished.at[:, columns], result.at[:, columns], out_sem.at[2 * order + strip]
        )

    def down_end(order, block):
        quarter_columns = pl.ds(aligned(block % half_blocks, block_width), block_width)

        @pl.when(block // half_blocks == core)
        def _():
            far_copy(order, block).wait_recv()
            rows = rows_of(kept, own_rows)
            for strip in range(2):
                place = strip * plane + block % half_blocks
                summed = pl.ds(aligned(2 * (block % half_blocks) + strip, strip_width), strip_width)
                ours = pl.ds(aligned(core * 2 * plane + place, strip_width), strip_width)
                finished[:, pl.ds(aligned(place, strip_width), strip_width)] = (
                    stream[rows, ours].astype(jnp.float32)
                    + total[:, summed]
                    + far_down[:, summed].astype(jnp.float32)
                ).astype(jnp.bfloat16)
                strip_out(order, strip, block).start()

    def block_at(at_level, at_cell):
        return (at_level // 2) * plane + at_cell

    cells = (cell, beside, beyond, diagonal)
    blocks = [block_at(at_level, at_cell) for at_level in (level, facing) for at_cell in cells]

    needed = (
        (("pool",),),
        (("x", 0), ("x", 1)),
        (("y", 0), ("y", 1)),
        (("x", 4), ("y", 4)),
        (("mirror", 0), ("mirror", 1)),
        (("x", 2), ("x", 3)),
        (("y", 2), ("y", 3)),
        (("x", 5), ("y", 5)),
    )

    def block_here(order):
        for kind, *rest in needed[order]:
            if kind == "pool":
                own_here(W)
                pool_here(W)
            elif kind == "mirror":
                mirror_here(W, rest[0])
            else:
                flow_here(W, ("x", "y").index(kind), rest[0])

    def core_sent(place):
        core_copy(place).wait_send()

    def share_block(order, which):
        for place in range(tiles):
            once(("core", place), functools.partial(core_sent, place))
        block_here(order)
        down_block(order, which)

    tile_steps = {
        "N": lambda place: rms_tile(rows_in, place, 0),
        "V": lambda place: act_tile(place, whole_v, act_v, True),
        "U": lambda place: act_tile(place, whole_u, act_u, False),
        "M": mix_tile,
        "O": out_tile,
        "C": chip_tile,
        "side": lambda place: side_copy(place).start(),
        "S": stream_tile,
        "G": gate_tile,
        "E": value_tile,
    }
    plain_steps = {
        "prep": prepare,
        "tok": lambda: token_copy(0, own_tokens, mate).start(),
        "halftok": near_tokens,
        "fwd": pass_tokens,
        "statA": near_stats.start,
        "statB": sum_stats,
        "statC": far_stats.start,
    }
    block_steps = {
        "DG": lambda order: share_block(order, 0),
        "SG": given_sum,
        "far": send_given,
        "DK": lambda order: share_block(order, 1),
        "SK": kept_sum,
        "END": lambda order: down_end(order, blocks[order]),
    }
    uses = {"V": V, "U": U, "O": O, "G": G, "E": E}

    def run_step(name):
        stem, tail = name[:-2], name[-2:]
        if name in plain_steps:
            plain_steps[name]()
        elif stem in tile_steps and tail[0] in "kg":
            if stem in uses:
                all_here(uses[stem])
            if stem == "N" and tail[0] == "g":
                once("tokens", last_tokens)
            tile_steps[stem]((first if tail[0] == "k" else second) + int(tail[1]))
        elif name[:-1] in block_steps:
            block_steps[name[:-1]](int(name[-1]))
        elif name[:4] == "pool":
            pool_copy(NAMES.index(name[4])).start()
        elif name[:3] == "crs":
            send_cross(NAMES.index(name[3]))
        elif name[:3] == "mir":
            send_mirror(NAMES.index(name[3]), int(name[4]))
        else:
            send_flow(NAMES.index(name[1]), ("x", "y").index(name[0]), int(name[2]))

    for name in ORDER:
        run_step(name)

    for place in range(tiles):
        side_copy(place).wait_send()
    for which in range(6):
        for step in range(6):
            for way in range(2):
                send_on(which, way, step).wait_send()
        for part in range(2 if inner else 1):
            reflect(which, part).wait_send()
        if inner:
            cross_copy(which).wait_send()
        pool_copy(which).wait_send()
    for place in range(tiles):
        half_copy(place, own_columns).wait_send()
    for order, block in enumerate(blocks):

        @pl.when(block // half_blocks != core)
        def _():
            near_copy(order, block, given, 0).wait_send()
            near_copy(order, block, kept, 1).wait_send()

        @pl.when(block // half_blocks == core)
        def _():
            far_copy(order, block).wait_send()
            for strip in range(2):
                strip_out(order, strip, block).wait()

    token_copy(0, own_tokens, mate).wait_send()
    token_copy(1, own_tokens, partner).wait_send()
    token_copy(2, token_region(1 - slot, core), partner).wait_send()
    token_copy(3, gain_region(core), partner).wait_send()
    near_stats.wait_send()
    far_stats.wait_send()


def layer_kernel(fs_size, *refs):
    level = lax.axis_index("fs") // (fs_size // 4)
    middle = (level + level // 2) % 2

    @pl.when(middle == 0)
    def _():
        run_layer(fs_size, False, *refs)

    @pl.when(middle == 1)
    def _():
        run_layer(fs_size, True, *refs)


def on_ring(
    fs_size,
    tokens,
    norm_gain,
    proj_u,
    proj_v,
    layer_gain,
    layer_shift,
    mix_weight,
    mix_bias,
    proj_out,
    ffn_gain,
    ffn_gate,
    ffn_value,
    conv_gate,
    conv_value,
    proj_down,
):
    own_rows, own_width = tokens.shape
    row_count, full = 2 * own_rows, 2 * own_width
    pairs = fs_size // 2
    quarter, units = proj_u.shape[1] // 2, max(unit_shares(ffn_gate.shape[1]))
    groups = quarter // GROUP_DIM
    tiles = row_count // SEQ_LEN
    bf16, f32 = jnp.bfloat16, jnp.float32
    vmem, hbm = pl.BlockSpec(memory_space=pltpu.VMEM), pl.BlockSpec(memory_space=pl.ANY)
    dma = pltpu.SemaphoreType.DMA
    scratch = [
        pltpu.VMEM((full, quarter), bf16),
        pltpu.VMEM((full, quarter), bf16),
        pltpu.VMEM((pairs, quarter, 2 * proj_out.shape[1]), bf16),
        pltpu.VMEM((full, units), bf16),
        pltpu.VMEM((full, units), bf16),
        pltpu.VMEM((pairs, units, 2 * proj_down.shape[1]), bf16),
        pltpu.VMEM((row_count, full), bf16),
        pltpu.VMEM((row_count, full), bf16),
        pltpu.VMEM((8, full), f32),
        pltpu.VMEM((row_count, quarter), f32),
        pltpu.VMEM((row_count, quarter), f32),
        pltpu.VMEM((row_count, LANES), f32),
        pltpu.VMEM((8, row_count), f32),
        pltpu.VMEM((8, row_count), f32),
        pltpu.VMEM((8, row_count), f32),
        pltpu.VMEM((8, row_count), f32),
        pltpu.VMEM((groups, BLOCK, BLOCK), bf16),
        pltpu.VMEM((groups, BLOCK, LANES), f32),
        pltpu.VMEM((row_count, quarter), bf16),
        pltpu.VMEM((row_count, full), bf16),
        pltpu.VMEM((row_count, own_width), bf16),
        pltpu.VMEM((row_count, own_width), bf16),
        pltpu.VMEM((row_count, own_width), bf16),
        pltpu.VMEM((row_count, full), bf16),
        pltpu.VMEM((row_count, units), bf16),
        pltpu.VMEM((own_rows, own_width), f32),
        pltpu.VMEM((own_rows, own_width), bf16),
        pltpu.VMEM((row_count, own_width), bf16),
        pltpu.VMEM((own_rows, own_width), bf16),
        pltpu.VMEM((own_rows, own_width), bf16),
        dma((8,)),
        dma((6,)),
        dma((6,)),
        dma((84,)),
        dma((84,)),
        dma((4,)),
        dma((4,)),
        dma((2,)),
        dma((2,)),
        dma((tiles,)),
        dma((tiles,)),
        dma((tiles,)),
        dma((tiles,)),
        dma((tiles,)),
        dma((tiles,)),
        dma((2 * pairs,)),
        dma((2 * pairs,)),
        dma((pairs,)),
        dma((pairs,)),
        dma((2 * pairs,)),
        dma((6,)),
    ]
    return pl.pallas_call(
        functools.partial(layer_kernel, fs_size),
        out_shape=jax.ShapeDtypeStruct((own_rows, own_width), bf16),
        in_specs=[hbm] + [vmem] * 8 + [hbm] * 6,
        out_specs=hbm,
        scratch_shapes=scratch,
        compiler_params=pltpu.CompilerParams(
            collective_id=0, has_side_effects=True, vmem_limit_bytes=VMEM_BYTES
        ),
        name="layer",
    )(
        tokens,
        norm_gain,
        ffn_gain,
        layer_gain,
        layer_shift,
        mix_weight,
        mix_bias,
        conv_gate,
        conv_value,
        proj_u,
        proj_v,
        proj_out,
        ffn_gate,
        ffn_value,
        proj_down,
    )


def solution(mesh):
    fs_size, tp_size = mesh.shape["fs"], mesh.shape["tp"]
    ringed = tp_size == 2 and fs_size == 16
    in_specs = (
        P("fs", "tp"),
        P("tp"),
        P("fs", "tp"),
        P("fs", "tp"),
        P("tp"),
        P("tp"),
        P("tp", None, None),
        P("tp", None),
        P("tp", "fs"),
        P("tp"),
        P("fs", "tp"),
        P("fs", "tp"),
        P(None, "tp"),
        P(None, "tp"),
        P("tp", "fs"),
    )
    return jax.shard_map(
        functools.partial(on_ring, fs_size) if ringed else on_device,
        mesh=mesh,
        in_specs=in_specs,
        out_specs=P("fs", "tp"),
        check_vma=False,
    )
```

```python
import functools

import jax
import jax.numpy as jnp
from jax import lax
from jax.experimental import pallas as pl
from jax.experimental.pallas import tpu as pltpu
from jax.sharding import PartitionSpec as P

MESH = pl.DeviceIdType.MESH
LANES = 128

GROUP_DIM = 128
BLOCK = 128
SEGMENT = 64
KERNEL = 3
SEQ_LEN = 256


EPS = 1e-06


def matmul(operand, matrix):
    return jnp.dot(operand, matrix, preferred_element_type=jnp.float32)


def local_rms(values_in, gain_row):
    values = values_in.astype(jnp.float32)
    scale_row = lax.rsqrt(jnp.mean(values * values, axis=1, keepdims=True) + EPS)
    return (values * scale_row * gain_row.astype(jnp.float32)).astype(jnp.bfloat16)


def causal_taps(values, weights):
    seq_count = values.shape[0] // SEQ_LEN
    shaped = values.reshape(seq_count, SEQ_LEN, values.shape[1])
    padded = jnp.pad(shaped, ((0, 0), (KERNEL - 1, 0), (0, 0)))
    summed = jnp.zeros(shaped.shape, jnp.float32)
    for tap_index in range(KERNEL):
        summed = summed + padded[:, tap_index : tap_index + SEQ_LEN].astype(jnp.float32) * weights[
            tap_index
        ].astype(jnp.float32)
    return summed.reshape(values.shape[0], values.shape[1])


def on_device(
    tokens,
    norm_gain,
    proj_u,
    proj_v,
    layer_gain,
    layer_shift,
    mix_weight,
    mix_bias,
    proj_out,
    ffn_gain,
    ffn_gate,
    ffn_value,
    conv_gate,
    conv_value,
    proj_down,
):
    own_width = tokens.shape[1]
    whole_tokens, whole_gain, whole_ffn_gain = (
        lax.all_gather(tokens, "tp", axis=1, tiled=True),
        lax.all_gather(norm_gain, "tp", axis=0, tiled=True),
        lax.all_gather(ffn_gain, "tp", axis=0, tiled=True),
    )
    normed = local_rms(whole_tokens, whole_gain)
    row_count = normed.shape[0]
    whole_u, whole_v = (
        lax.all_gather(proj_u, "fs", axis=0, tiled=True),
        lax.all_gather(proj_v, "fs", axis=0, tiled=True),
    )
    pre_u = matmul(normed, whole_u)
    pre_v = matmul(normed, whole_v)
    act_u = jax.nn.gelu(pre_u, approximate=False)
    act_v = jax.nn.gelu(pre_v, approximate=False)
    full_width = act_v.shape[1] * lax.axis_size("tp")
    total_sum, second = lax.psum((jnp.sum(act_v, axis=1), jnp.sum(act_v * act_v, axis=1)), "tp")
    center = total_sum / full_width
    spread = second / full_width - center * center
    mixed_in = (
        (act_v - center[:, None])
        * lax.rsqrt(spread + EPS)[:, None]
        * layer_gain.astype(jnp.float32)
        + layer_shift.astype(jnp.float32)
    ).astype(jnp.bfloat16)
    groups = mixed_in.shape[1] // GROUP_DIM
    blocks = mixed_in.reshape(row_count // BLOCK, BLOCK, groups, GROUP_DIM)
    segment = jnp.arange(BLOCK) // SEGMENT
    visible = segment[None, :] <= segment[:, None]
    masked = jnp.where(visible[None], mix_weight, jnp.zeros_like(mix_weight))
    spatial = (
        jnp.einsum("gij,njgc->nigc", masked, blocks, preferred_element_type=jnp.float32)
        + mix_bias.astype(jnp.float32).T[None, :, :, None]
    )
    gated_rows = (act_u * spatial.reshape(row_count, mixed_in.shape[1])).astype(jnp.bfloat16)
    whole_out = lax.all_gather(proj_out, "fs", axis=1, tiled=True)
    partial_value = matmul(gated_rows, whole_out)
    summed = lax.psum(partial_value.astype(jnp.bfloat16), "tp").astype(jnp.float32)
    stream_rows = (whole_tokens.astype(jnp.float32) + summed).astype(jnp.bfloat16)
    normed_two = local_rms(stream_rows, whole_ffn_gain)
    stream = lax.dynamic_slice_in_dim(stream_rows, lax.axis_index("tp") * own_width, own_width, 1)
    whole_gate, whole_value = (
        lax.all_gather(ffn_gate, "fs", axis=0, tiled=True),
        lax.all_gather(ffn_value, "fs", axis=0, tiled=True),
    )
    pre_gate = matmul(normed_two, whole_gate)
    pre_value = matmul(normed_two, whole_value)
    conv_g = causal_taps(pre_gate.astype(jnp.bfloat16), conv_gate)
    conv_v = causal_taps(pre_value.astype(jnp.bfloat16), conv_value)
    hidden = (jax.nn.silu(conv_g) * conv_v).astype(jnp.bfloat16)
    whole_down = lax.all_gather(proj_down, "fs", axis=1, tiled=True)
    partial_two = matmul(hidden, whole_down)
    return (
        stream.astype(jnp.float32)
        + lax.psum_scatter(
            partial_two.astype(jnp.bfloat16), "tp", scatter_dimension=1, tiled=True
        ).astype(jnp.float32)
    ).astype(jnp.bfloat16)


V, U, O, G, E, W = range(6)
NAMES = ("V", "U", "O", "G", "E", "W")
ORDER = (
    "yV0", "yU0", "yO0", "yG0", "poolO", "mirU0", "xG0", "xU0", "yO1", "mirO1", "xO1", "poolU",
    "crsO", "mirU1", "xE0", "poolV", "mirV0", "xU4", "xV4", "xU1", "mirV1", "yW0", "yE0", "poolG",
    "mirO0", "crsV", "crsU", "xO3", "poolE", "crsE", "crsG", "yV2", "xV1", "yO2", "yV3", "xV3",
    "yO5", "xU3", "yG1", "mirG0", "prep", "xO4", "xG1", "mirE1", "yV4", "xO0", "yU3", "yV5",
    "halftok", "yU1", "Nk0", "yU2", "Nk1", "xV2", "yV1", "xE1", "yO3", "xO5", "tok", "xV5", "xV0",
    "poolW", "yE4", "mirG1", "xG4", "yO4", "yU5", "yU4", "mirW0", "xU2", "fwd", "Vk0", "Ng1", "xO2",
    "xU5", "yG2", "Vg1", "Ng0", "Vg0", "Vk1", "statA", "xW1", "statB", "yG4", "statC", "xE4", "xG2",
    "Ug1", "yG3", "crsW", "mirE0", "Mg1", "Og1", "Cg1", "xG5", "sideg1", "Uk1", "Mk1", "Ok1", "Ck1",
    "Ug0", "Mg0", "Og0", "sidek1", "xG3", "Uk0", "yE2", "yE1", "yG5", "xE3", "xE2", "xE5", "Mk0",
    "Ok0", "Ck0", "sidek0", "yE5", "Cg0", "sideg0", "yE3", "yW4", "Sk1", "Gk1", "mirW1", "xW4",
    "yW1", "Sg1", "Gg1", "Sg0", "Gg0", "xW0", "yW2", "Eg1", "Eg0", "DG0", "xW3", "xW5", "Sk0",
    "DG4", "SG0", "far0", "DG3", "yW3", "SG4", "far4", "Gk0", "yW5", "DG2", "DG1", "SG3", "far3",
    "Ek0", "xW2", "SG1", "far1", "Ek1", "DK1", "DK3", "SG2", "far2", "DG7", "DK4", "SK1", "END1",
    "SG7", "far7", "DK7", "DG6", "SK3", "SK7", "DK2", "SG6", "far6", "DG5", "DK0", "SK2", "END3",
    "SG5", "far5", "END2", "DK5", "SK4", "END4", "SK0", "DK6", "END7", "SK6", "END6", "SK5", "END0",
    "END5",
)
BY_ROWS = (V, U, G, E)
VMEM_BYTES = 67043328


def gelu(values):
    return 0.5 * values * (1.0 + lax.erf(values * (0.5**0.5)))


def aligned(index, size):
    return index * size if isinstance(index, int) else pl.multiple_of(index * size, size)


def unit_shares(total):
    outer = (3 * total // 8) // 256 * 256
    return outer, total - outer


def run_layer(
    fs_size,
    inner,
    tokens,
    norm_gain,
    ffn_gain,
    layer_gain,
    layer_shift,
    mix_weight,
    mix_bias,
    conv_gate,
    conv_value,
    proj_u,
    proj_v,
    proj_out,
    ffn_gate,
    ffn_value,
    proj_down,
    result,
    whole_v,
    whole_u,
    whole_out,
    whole_gate,
    whole_value,
    whole_down,
    rows_in,
    normed,
    gains,
    act_v,
    act_u,
    stat_cols,
    stat_own,
    stat_chip,
    stat_near,
    stat_far,
    masked,
    bias_cols,
    gated,
    partial,
    from_core,
    chip_sum,
    from_side,
    stream,
    pre_gate,
    total,
    given_down,
    near_down,
    far_down,
    finished,
    local_sem,
    pool_send,
    pool_recv,
    flow_send,
    flow_recv,
    token_send,
    token_recv,
    stat_send,
    stat_recv,
    core_send,
    core_recv,
    side_send,
    side_recv,
    half_send,
    half_recv,
    near_send,
    near_recv,
    far_send,
    far_recv,
    out_sem,
    cross_send,
):
    pairs = fs_size // 2
    plane = fs_size // 4
    index, core = lax.axis_index("fs"), lax.axis_index("tp")
    level, cell = index // plane, index % plane
    side, column = cell % 2, cell // 2
    low, half = level % 2, level // 2
    slot = int(inner)
    facing = 3 - level
    levels = (level, level + 1 - 2 * low, facing, facing + 1 - 2 * (facing % 2))
    beside, beyond = cell + 1 - 2 * side, cell + 2 - 4 * column
    diagonal = beside + 2 - 4 * column

    partner = (index, 1 - core)
    mate = (levels[1] * plane + cell, core)
    mirror = (facing * plane + cell, core)
    across = (level * plane + beside, core)
    over = (level * plane + beyond, core)
    crossed = (levels[3] * plane + cell, core)

    barrier = pltpu.get_barrier_semaphore()
    for device in (across, over, mate, mirror, crossed, partner):
        pl.semaphore_signal(barrier, inc=1, device_id=device, device_id_type=MESH)
    own_rows, own_width = tokens.shape
    row_count, full = rows_in.shape
    tile = SEQ_LEN
    tiles = row_count // tile
    half_tiles = tiles // 2
    quarter = whole_v.shape[1]
    shares = unit_shares(ffn_gate.shape[1])
    starts = (0, shares[0])
    units = shares[slot]
    relieved = (G, E, W) if inner else ()
    groups = quarter // GROUP_DIM
    spread_width = 2 * 2 * quarter
    block_width = whole_out.shape[2]
    half_blocks = pairs // 2

    sources = (proj_v, proj_u, proj_out, ffn_gate, ffn_value, proj_down)
    wholes = (whole_v, whole_u, whole_out, whole_gate, whole_value, whole_down)

    def shard(which, part):
        source = sources[which]
        if which in (G, E):
            return source.at[:, pl.ds(starts[part], shares[part])]
        if which == W:
            return source.at[pl.ds(starts[part], shares[part]), :]
        if which in BY_ROWS:
            width = source.shape[1] // 2
            return source.at[:, pl.ds(part * width, width)]
        height = source.shape[0] // 2
        return source.at[pl.ds(part * height, height), :]

    def piece(which, at_level, at_cell, part=slot):
        whole = wholes[which]
        if which in BY_ROWS:
            width = shares[part] if which in (G, E) else whole.shape[1]
            depth_rows = sources[which].shape[0]
            place = aligned(at_level * plane + at_cell, depth_rows)
            return whole.at[pl.ds(place, depth_rows), pl.ds(0, width)]
        height = shares[part] if which == W else whole.shape[1]
        width = sources[which].shape[1]
        block = (at_level // 2) * plane + at_cell
        return whole.at[block, pl.ds(0, height), pl.ds(aligned(at_level % 2, width), width)]

    def remote(source, target, send, recv, device):
        return pltpu.make_async_remote_copy(
            src_ref=source,
            dst_ref=target,
            send_sem=send,
            recv_sem=recv,
            device_id=device,
            device_id_type=MESH,
        )

    def own_copy(which):
        return pltpu.make_async_copy(
            shard(which, slot), piece(which, level, cell), local_sem.at[which]
        )

    def pool_copy(which):
        return remote(
            shard(which, 1 - slot),
            piece(which, level, cell, 1 - slot),
            pool_send.at[which],
            pool_recv.at[which],
            mate,
        )

    def pool_arrived(which):
        here = piece(which, levels[1], cell)
        remote(here, here, pool_send.at[which], pool_recv.at[which], mate).wait_recv()

    def moved(which, here, slot_index, device):
        place = which * 14 + slot_index
        return remote(here, here, flow_send.at[place], flow_recv.at[place], device)

    def send_on(which, way, step):
        device = (across, over)[way]
        if step < 4:
            here = piece(which, levels[step], cell)
        elif step == 5 and which in relieved:
            here, device = piece(which, levels[way], diagonal), mirror
        else:
            here = piece(which, levels[2 * (step - 4) + way], (beyond, beside)[way])
        return moved(which, here, way * 6 + step, device)

    def come_in(which, way, step):
        device = (across, over)[way]
        if step < 4:
            here = piece(which, levels[step], (beside, beyond)[way])
        else:
            here = piece(which, levels[2 * (step - 4) + way], diagonal)
        if step == 5 and which in relieved:
            device = mirror
        moved(which, here, way * 6 + step, device).wait_recv()

    def reflect(which, part):
        return moved(which, piece(which, levels[part], cell), 12 + part, mirror)

    def reflected(which, part):
        moved(which, piece(which, levels[2 + part], cell), 12 + part, mirror).wait_recv()

    def token_region(which_side, which_core):
        return rows_in.at[
            pl.ds(aligned(which_side, own_rows), own_rows),
            pl.ds(aligned(which_core, own_width), own_width),
        ]

    def gain_region(which_core):
        return gains.at[:, pl.ds(aligned(which_core, own_width), own_width)]

    def token_copy(which, region, device):
        return remote(region, region, token_send.at[which], token_recv.at[which], device)

    def rows_of(place, height=tile):
        return pl.ds(aligned(place, height), height)

    for which in (V, U, O):
        own_copy(which).start()
    tokens_in = pltpu.make_async_copy(tokens, token_region(slot, core), local_sem.at[6])
    tokens_in.start()
    for which in (G, E, W):
        own_copy(which).start()
    for row, vector in enumerate((norm_gain, ffn_gain, layer_gain, layer_shift)):
        values = vector[...].astype(jnp.float32).reshape(1, own_width)
        gains[row : row + 1, pl.ds(aligned(core, own_width), own_width)] = values
    pl.semaphore_wait(pltpu.get_barrier_semaphore(), 6)

    own_tokens = token_region(slot, core)
    def arrive_pool(which):
        return lambda: pool_arrived(which)

    def arrive_mirror(which, part):
        return lambda: reflected(which, part)

    def arrive_flow(which, way, step):
        return lambda: come_in(which, way, step)

    done = set()

    def once(name, wait):
        if name not in done:
            done.add(name)
            wait()

    def own_here(which):
        once(("own", which), lambda: own_copy(which).wait())

    def pool_here(which):
        once(("pool", which), arrive_pool(which))

    def mirror_here(which, part):
        once(("mirror", which, part), arrive_mirror(which, part))

    def flow_here(which, way, step):
        once(("flow", which, way, step), arrive_flow(which, way, step))

    def part_here(which, part):
        (own_here, pool_here)[part](which)

    def all_here(which):
        own_here(which)
        pool_here(which)
        for part in range(2):
            mirror_here(which, part)
        for step in range(6):
            for way in range(2):
                flow_here(which, way, step)

    def send_flow(which, way, step):
        if step < 2:
            part_here(which, step)
        elif step < 4:
            mirror_here(which, step - 2)
        else:
            if step == 5 and which in relieved:
                flow_here(which, way, 4)
            else:
                flow_here(which, 1 - way, 2 * (step - 4) + way)
        send_on(which, way, step).start()

    def cross_copy(which):
        return remote(
            shard(which, 1 - slot),
            piece(which, level, cell, 1 - slot),
            cross_send.at[which],
            flow_recv.at[which * 14 + 13],
            crossed,
        )

    def send_mirror(which, part):
        if part == 0 or inner:
            part_here(which, part)
            reflect(which, part).start()

    def send_cross(which):
        if inner:
            cross_copy(which).start()

    tokens_in.wait()
    token_copy(1, own_tokens, partner).start()
    token_copy(3, gain_region(core), partner).start()

    head = slot * groups

    def prepare():
        above = lax.broadcasted_iota(jnp.int32, (BLOCK, BLOCK), 1)
        below = lax.broadcasted_iota(jnp.int32, (BLOCK, BLOCK), 0)
        visible = lax.div(above, SEGMENT) <= lax.div(below, SEGMENT)
        bias_rows = mix_bias[...].astype(jnp.float32)
        for group in range(groups):
            weight = mix_weight[head + group].astype(jnp.float32)
            masked[group] = jnp.where(visible, weight, 0.0).astype(jnp.bfloat16)
            lower = bias_rows[group : group + 1]
            upper = bias_rows[group + groups : group + groups + 1]
            row = upper if inner else lower
            bias_cols[group] = jnp.broadcast_to(row, (LANES, BLOCK)).T

    first, second = slot * half_tiles, (1 - slot) * half_tiles

    def near_tokens():
        token_copy(1, token_region(slot, 1 - core), partner).wait_recv()
        token_copy(3, gain_region(1 - core), partner).wait_recv()

    def pass_tokens():
        token_copy(0, token_region(1 - slot, core), mate).wait_recv()
        token_copy(2, token_region(1 - slot, core), partner).start()

    def last_tokens():
        token_copy(2, token_region(1 - slot, 1 - core), partner).wait_recv()

    def rms_tile(source, place, gain_index):
        step_rows = 32

        def one(part, carry):
            rows = pl.ds(aligned(place * (tile // step_rows) + part, step_rows), step_rows)
            values = source[rows, :].astype(jnp.float32)
            scale = lax.rsqrt(jnp.mean(values * values, axis=1, keepdims=True) + EPS)
            normed[rows, :] = (values * scale * gains[gain_index : gain_index + 1, :]).astype(
                jnp.bfloat16
            )
            return carry

        lax.fori_loop(0, tile // step_rows, one, 0)

    def product(target, rows, weights, width, count, finish):
        def one(part, carry):
            columns = pl.ds(aligned(part, width), width)
            value = jnp.dot(
                normed[rows, :], weights[:, columns], preferred_element_type=jnp.float32
            )
            target[rows, columns] = finish(value)
            return carry

        lax.fori_loop(0, count, one, 0)

    lane = lax.broadcasted_iota(jnp.int32, (64, LANES), 1)

    def act_tile(place, weights, target, with_stats):
        rows = rows_of(place)
        product(target, rows, weights, 256, quarter // 256, lambda value: value)

        def one(part, carry):
            some = pl.ds(aligned(place * (tile // 64) + part, 64), 64)
            value = gelu(target[some, :])
            target[some, :] = value
            if with_stats:
                sums = jnp.sum(value, axis=1, keepdims=True)
                squares = jnp.sum(value * value, axis=1, keepdims=True)
                stat_cols[some, :] = jnp.where(lane == 0, sums, jnp.where(lane == 1, squares, 0.0))
            return carry

        lax.fori_loop(0, tile // 64, one, 0)
        if with_stats:
            for part in range(tile // LANES):
                some = pl.ds(aligned(place * (tile // LANES) + part, LANES), LANES)
                stat_own[:, some] = stat_cols[some, :].T[0:8, :]

    near_stats = remote(stat_own, stat_near, stat_send.at[0], stat_recv.at[0], partner)
    far_stats = remote(stat_chip, stat_far, stat_send.at[1], stat_recv.at[1], mate)

    def sum_stats():
        near_stats.wait_recv()
        stat_chip[...] = stat_own[...] + stat_near[...]

    def mix_block(block, carry):
        rows = pl.ds(aligned(block, BLOCK), BLOCK)
        sums = stat_chip[0:2, rows] + stat_far[0:2, rows]
        center_row = sums[0:1] / spread_width
        spread_row = sums[1:2] / spread_width - center_row * center_row
        scale_row = lax.rsqrt(spread_row + EPS)
        center = jnp.broadcast_to(center_row, (LANES, BLOCK)).T
        scale = jnp.broadcast_to(scale_row, (LANES, BLOCK)).T
        for group in range(groups):
            columns = slice(group * GROUP_DIM, (group + 1) * GROUP_DIM)
            own = pl.ds(aligned((core * 2 + slot) * groups + group, GROUP_DIM), GROUP_DIM)
            mixed = (
                (act_v[rows, columns] - center) * scale * gains[2:3, own] + gains[3:4, own]
            ).astype(jnp.bfloat16)
            spatial = (
                jnp.dot(masked[group], mixed, preferred_element_type=jnp.float32)
                + bias_cols[group]
            )
            gated[rows, columns] = (act_u[rows, columns] * spatial).astype(jnp.bfloat16)
        return carry

    def mix_tile(place):
        once("stats", far_stats.wait_recv)
        ratio = tile // BLOCK
        lax.fori_loop(place * ratio, (place + 1) * ratio, mix_block, 0)

    own_columns = pl.ds(aligned(core, own_width), own_width)
    other_columns = pl.ds(aligned(1 - core, own_width), own_width)

    def core_copy(place):
        rows = rows_of(place)
        return remote(
            partial.at[rows, other_columns],
            from_core.at[rows, :],
            core_send.at[place],
            core_recv.at[place],
            partner,
        )

    def side_copy(place):
        rows = rows_of(place)
        return remote(
            chip_sum.at[rows, :],
            from_side.at[rows, :],
            side_send.at[place],
            side_recv.at[place],
            mate,
        )

    def half_copy(place, columns):
        region = stream.at[rows_of(place), columns]
        return remote(region, region, half_send.at[place], half_recv.at[place], partner)

    def out_tile(place):
        rows = rows_of(place)

        def one(block, inner):
            columns = pl.ds(aligned(block, block_width), block_width)
            value = jnp.dot(gated[rows, :], whole_out[block], preferred_element_type=jnp.float32)
            partial[rows, columns] = value.astype(jnp.bfloat16)
            return inner

        lax.fori_loop(0, pairs, one, 0)
        core_copy(place).start()

    def chip_tile(place):
        core_copy(place).wait_recv()
        rows = rows_of(place)
        chip_sum[rows, :] = (
            partial[rows, own_columns].astype(jnp.float32)
            + from_core[rows, :].astype(jnp.float32)
        ).astype(jnp.bfloat16)

    strip_width = block_width // 2

    def strips():
        for strip in range(2):
            for place in range(half_blocks):
                ours = pl.ds(
                    aligned(core * 2 * plane + strip * plane + place, strip_width), strip_width
                )
                start = (2 * place + strip) * strip_width
                yield ours, slice(start, start + strip_width)

    def stream_tile(place):
        side_copy(place).wait_recv()
        rows = rows_of(place)
        for ours, summed in strips():
            stream[rows, ours] = (
                rows_in[rows, ours].astype(jnp.float32)
                + chip_sum[rows, summed].astype(jnp.float32)
                + from_side[rows, summed].astype(jnp.float32)
            ).astype(jnp.bfloat16)
        half_copy(place, own_columns).start()

    def to_bfloat(value):
        return value.astype(jnp.bfloat16)

    def gate_tile(place):
        half_copy(place, other_columns).wait_recv()
        rms_tile(stream, place, 1)
        product(pre_gate, rows_of(place), whole_gate, 256, units // 256, to_bfloat)

    shifted = lax.broadcasted_iota(jnp.int32, (tile, 256), 0)

    def taps(values, weights):
        before = jnp.where(shifted >= 1, pltpu.roll(values, 1, 0), 0.0)
        earlier = jnp.where(shifted >= 2, pltpu.roll(values, 2, 0), 0.0)
        return earlier * weights[0:1] + before * weights[1:2] + values * weights[2:3]

    def value_tile(place):
        rows = rows_of(place)

        def one(part, carry):
            columns = pl.ds(aligned(part, 256), 256)
            own = pl.ds(aligned(starts[slot] // 256 + part, 256), 256)
            value = jnp.dot(
                normed[rows, :], whole_value[:, columns], preferred_element_type=jnp.float32
            )
            value = value.astype(jnp.bfloat16).astype(jnp.float32)
            gate = pre_gate[rows, columns].astype(jnp.float32)
            conv_g = taps(gate, conv_gate[:, own].astype(jnp.float32))
            conv_v = taps(value, conv_value[:, own].astype(jnp.float32))
            pre_gate[rows, columns] = (jax.nn.silu(conv_g) * conv_v).astype(jnp.bfloat16)
            return carry

        lax.fori_loop(0, units // 256, one, 0)

    given, kept = (1 - slot), slot

    def near_copy(order, block, which_side, which):
        rows = rows_of(which_side, own_rows)
        quarter_block = block % half_blocks
        return remote(
            partial.at[rows, pl.ds(aligned(block, block_width), block_width)],
            near_down.at[rows, pl.ds(aligned(quarter_block, block_width), block_width)],
            near_send.at[2 * order + which],
            near_recv.at[2 * order + which],
            partner,
        )

    def far_copy(order, block):
        columns = pl.ds(aligned(block % half_blocks, block_width), block_width)
        return remote(
            given_down.at[:, columns],
            far_down.at[:, columns],
            far_send.at[order],
            far_recv.at[order],
            mate,
        )

    def down_block(order, which):
        block = blocks[order]
        which_side = (given, kept)[which]
        columns = pl.ds(aligned(block, block_width), block_width)

        def one(part, carry):
            rows = rows_of(which_side * half_tiles + part)
            value = jnp.dot(
                pre_gate[rows, pl.ds(0, units)],
                whole_down[block, pl.ds(0, units), :],
                preferred_element_type=jnp.float32,
            )
            partial[rows, columns] = value.astype(jnp.bfloat16)
            return carry

        lax.fori_loop(0, half_tiles, one, 0)

        @pl.when(block // half_blocks != core)
        def _():
            near_copy(order, block, which_side, which).start()

    def given_sum(order):
        block = blocks[order]
        columns = pl.ds(aligned(block, block_width), block_width)
        quarter_columns = pl.ds(aligned(block % half_blocks, block_width), block_width)

        @pl.when(block // half_blocks == core)
        def _():
            near_copy(order, block, given, 0).wait_recv()
            rows = rows_of(given, own_rows)
            given_down[:, quarter_columns] = (
                partial[rows, columns].astype(jnp.float32)
                + near_down[rows, quarter_columns].astype(jnp.float32)
            ).astype(jnp.bfloat16)

    def send_given(order):
        block = blocks[order]

        @pl.when(block // half_blocks == core)
        def _():
            far_copy(order, block).start()

    def kept_sum(order):
        block = blocks[order]
        columns = pl.ds(aligned(block, block_width), block_width)
        quarter_columns = pl.ds(aligned(block % half_blocks, block_width), block_width)

        @pl.when(block // half_blocks == core)
        def _():
            near_copy(order, block, kept, 1).wait_recv()
            rows = rows_of(kept, own_rows)
            total[:, quarter_columns] = partial[rows, columns].astype(jnp.float32) + near_down[
                rows, quarter_columns
            ].astype(jnp.float32)

    def strip_out(order, strip, block):
        columns = pl.ds(
            aligned(strip * plane + block % half_blocks, block_width // 2), block_width // 2
        )
        return pltpu.make_async_copy(
            finished.at[:, columns], result.at[:, columns], out_sem.at[2 * order + strip]
        )

    def down_end(order, block):
        quarter_columns = pl.ds(aligned(block % half_blocks, block_width), block_width)

        @pl.when(block // half_blocks == core)
        def _():
            far_copy(order, block).wait_recv()
            rows = rows_of(kept, own_rows)
            for strip in range(2):
                place = strip * plane + block % half_blocks
                summed = pl.ds(aligned(2 * (block % half_blocks) + strip, strip_width), strip_width)
                ours = pl.ds(aligned(core * 2 * plane + place, strip_width), strip_width)
                finished[:, pl.ds(aligned(place, strip_width), strip_width)] = (
                    stream[rows, ours].astype(jnp.float32)
                    + total[:, summed]
                    + far_down[:, summed].astype(jnp.float32)
                ).astype(jnp.bfloat16)
                strip_out(order, strip, block).start()

    def block_at(at_level, at_cell):
        return (at_level // 2) * plane + at_cell

    cells = (cell, beside, beyond, diagonal)
    blocks = [block_at(at_level, at_cell) for at_level in (level, facing) for at_cell in cells]

    needed = (
        (("pool",),),
        (("x", 0), ("x", 1)),
        (("y", 0), ("y", 1)),
        (("x", 4), ("y", 4)),
        (("mirror", 0), ("mirror", 1)),
        (("x", 2), ("x", 3)),
        (("y", 2), ("y", 3)),
        (("x", 5), ("y", 5)),
    )

    def block_here(order):
        for kind, *rest in needed[order]:
            if kind == "pool":
                own_here(W)
                pool_here(W)
            elif kind == "mirror":
                mirror_here(W, rest[0])
            else:
                flow_here(W, ("x", "y").index(kind), rest[0])

    def core_sent(place):
        core_copy(place).wait_send()

    def share_block(order, which):
        for place in range(tiles):
            once(("core", place), functools.partial(core_sent, place))
        block_here(order)
        down_block(order, which)

    tile_steps = {
        "N": lambda place: rms_tile(rows_in, place, 0),
        "V": lambda place: act_tile(place, whole_v, act_v, True),
        "U": lambda place: act_tile(place, whole_u, act_u, False),
        "M": mix_tile,
        "O": out_tile,
        "C": chip_tile,
        "side": lambda place: side_copy(place).start(),
        "S": stream_tile,
        "G": gate_tile,
        "E": value_tile,
    }
    plain_steps = {
        "prep": prepare,
        "tok": lambda: token_copy(0, own_tokens, mate).start(),
        "halftok": near_tokens,
        "fwd": pass_tokens,
        "statA": near_stats.start,
        "statB": sum_stats,
        "statC": far_stats.start,
    }
    block_steps = {
        "DG": lambda order: share_block(order, 0),
        "SG": given_sum,
        "far": send_given,
        "DK": lambda order: share_block(order, 1),
        "SK": kept_sum,
        "END": lambda order: down_end(order, blocks[order]),
    }
    uses = {"V": V, "U": U, "O": O, "G": G, "E": E}

    def run_step(name):
        stem, tail = name[:-2], name[-2:]
        if name in plain_steps:
            plain_steps[name]()
        elif stem in tile_steps and tail[0] in "kg":
            if stem in uses:
                all_here(uses[stem])
            if stem == "N" and tail[0] == "g":
                once("tokens", last_tokens)
            tile_steps[stem]((first if tail[0] == "k" else second) + int(tail[1]))
        elif name[:-1] in block_steps:
            block_steps[name[:-1]](int(name[-1]))
        elif name[:4] == "pool":
            pool_copy(NAMES.index(name[4])).start()
        elif name[:3] == "crs":
            send_cross(NAMES.index(name[3]))
        elif name[:3] == "mir":
            send_mirror(NAMES.index(name[3]), int(name[4]))
        else:
            send_flow(NAMES.index(name[1]), ("x", "y").index(name[0]), int(name[2]))

    for name in ORDER:
        run_step(name)

    for place in range(tiles):
        side_copy(place).wait_send()
    for which in range(6):
        for step in range(6):
            for way in range(2):
                send_on(which, way, step).wait_send()
        for part in range(2 if inner else 1):
            reflect(which, part).wait_send()
        if inner:
            cross_copy(which).wait_send()
        pool_copy(which).wait_send()
    for place in range(tiles):
        half_copy(place, own_columns).wait_send()
    for order, block in enumerate(blocks):

        @pl.when(block // half_blocks != core)
        def _():
            near_copy(order, block, given, 0).wait_send()
            near_copy(order, block, kept, 1).wait_send()

        @pl.when(block // half_blocks == core)
        def _():
            far_copy(order, block).wait_send()
            for strip in range(2):
                strip_out(order, strip, block).wait()

    token_copy(0, own_tokens, mate).wait_send()
    token_copy(1, own_tokens, partner).wait_send()
    token_copy(2, token_region(1 - slot, core), partner).wait_send()
    token_copy(3, gain_region(core), partner).wait_send()
    near_stats.wait_send()
    far_stats.wait_send()


def layer_kernel(fs_size, *refs):
    level = lax.axis_index("fs") // (fs_size // 4)
    middle = (level + level // 2) % 2

    @pl.when(middle == 0)
    def _():
        run_layer(fs_size, False, *refs)

    @pl.when(middle == 1)
    def _():
        run_layer(fs_size, True, *refs)


def on_ring(
    fs_size,
    tokens,
    norm_gain,
    proj_u,
    proj_v,
    layer_gain,
    layer_shift,
    mix_weight,
    mix_bias,
    proj_out,
    ffn_gain,
    ffn_gate,
    ffn_value,
    conv_gate,
    conv_value,
    proj_down,
):
    own_rows, own_width = tokens.shape
    row_count, full = 2 * own_rows, 2 * own_width
    pairs = fs_size // 2
    quarter, units = proj_u.shape[1] // 2, max(unit_shares(ffn_gate.shape[1]))
    groups = quarter // GROUP_DIM
    tiles = row_count // SEQ_LEN
    bf16, f32 = jnp.bfloat16, jnp.float32
    vmem, hbm = pl.BlockSpec(memory_space=pltpu.VMEM), pl.BlockSpec(memory_space=pl.ANY)
    dma = pltpu.SemaphoreType.DMA
    scratch = [
        pltpu.VMEM((full, quarter), bf16),
        pltpu.VMEM((full, quarter), bf16),
        pltpu.VMEM((pairs, quarter, 2 * proj_out.shape[1]), bf16),
        pltpu.VMEM((full, units), bf16),
        pltpu.VMEM((full, units), bf16),
        pltpu.VMEM((pairs, units, 2 * proj_down.shape[1]), bf16),
        pltpu.VMEM((row_count, full), bf16),
        pltpu.VMEM((row_count, full), bf16),
        pltpu.VMEM((8, full), f32),
        pltpu.VMEM((row_count, quarter), f32),
        pltpu.VMEM((row_count, quarter), f32),
        pltpu.VMEM((row_count, LANES), f32),
        pltpu.VMEM((8, row_count), f32),
        pltpu.VMEM((8, row_count), f32),
        pltpu.VMEM((8, row_count), f32),
        pltpu.VMEM((8, row_count), f32),
        pltpu.VMEM((groups, BLOCK, BLOCK), bf16),
        pltpu.VMEM((groups, BLOCK, LANES), f32),
        pltpu.VMEM((row_count, quarter), bf16),
        pltpu.VMEM((row_count, full), bf16),
        pltpu.VMEM((row_count, own_width), bf16),
        pltpu.VMEM((row_count, own_width), bf16),
        pltpu.VMEM((row_count, own_width), bf16),
        pltpu.VMEM((row_count, full), bf16),
        pltpu.VMEM((row_count, units), bf16),
        pltpu.VMEM((own_rows, own_width), f32),
        pltpu.VMEM((own_rows, own_width), bf16),
        pltpu.VMEM((row_count, own_width), bf16),
        pltpu.VMEM((own_rows, own_width), bf16),
        pltpu.VMEM((own_rows, own_width), bf16),
        dma((8,)),
        dma((6,)),
        dma((6,)),
        dma((84,)),
        dma((84,)),
        dma((4,)),
        dma((4,)),
        dma((2,)),
        dma((2,)),
        dma((tiles,)),
        dma((tiles,)),
        dma((tiles,)),
        dma((tiles,)),
        dma((tiles,)),
        dma((tiles,)),
        dma((2 * pairs,)),
        dma((2 * pairs,)),
        dma((pairs,)),
        dma((pairs,)),
        dma((2 * pairs,)),
        dma((6,)),
    ]
    return pl.pallas_call(
        functools.partial(layer_kernel, fs_size),
        out_shape=jax.ShapeDtypeStruct((own_rows, own_width), bf16),
        in_specs=[hbm] + [vmem] * 8 + [hbm] * 6,
        out_specs=hbm,
        scratch_shapes=scratch,
        compiler_params=pltpu.CompilerParams(
            collective_id=0, has_side_effects=True, vmem_limit_bytes=VMEM_BYTES
        ),
        name="layer",
    )(
        tokens,
        norm_gain,
        ffn_gain,
        layer_gain,
        layer_shift,
        mix_weight,
        mix_bias,
        conv_gate,
        conv_value,
        proj_u,
        proj_v,
        proj_out,
        ffn_gate,
        ffn_value,
        proj_down,
    )


def solution(mesh):
    fs_size, tp_size = mesh.shape["fs"], mesh.shape["tp"]
    ringed = tp_size == 2 and fs_size == 16
    in_specs = (
        P("fs", "tp"),
        P("tp"),
        P("fs", "tp"),
        P("fs", "tp"),
        P("tp"),
        P("tp"),
        P("tp", None, None),
        P("tp", None),
        P("tp", "fs"),
        P("tp"),
        P("fs", "tp"),
        P("fs", "tp"),
        P(None, "tp"),
        P(None, "tp"),
        P("tp", "fs"),
    )
    return jax.shard_map(
        functools.partial(on_ring, fs_size) if ringed else on_device,
        mesh=mesh,
        in_specs=in_specs,
        out_specs=P("fs", "tp"),
        check_vma=False,
    )
```
